32 devices in a mesh: sp: 4 (over y, x), tp: 8 (over z, core).
Axes of the slice: x: 2, y: 2, z: 4, core: 2. Of those that a mesh axis runs over, the one named last changes fastest.
Arguments:
- prompt: bfloat16 [2, 8, 2, 4, 128, 2048], P(None, 'tp', None, 'sp'), may hold values from -60 to 60
- new_token: bfloat16 [2, 2048], replicated, may hold values from -20 to 20
- query_proj_matrix: bfloat16 [2048, 1024], P(None, 'tp'), may hold values from -1 to 1
- key_weight: bfloat16 [2048, 1024], P(None, 'tp'), may hold values from -1 to 1
- value_weight: bfloat16 [2048, 1024], P(None, 'tp'), may hold values from -0.125 to 0.125
- map_balance: float32 [8], replicated, may hold values from 0.3 to 0.8
- head_gain: float32 [128], replicated, may hold values from 0.1 to 1.9
Outputs:
- key_cache: bfloat16 [4, 8, 512, 1024], P('sp', 'tp')
- value_cache: bfloat16 [4, 8, 512, 1024], P('sp', 'tp')
- read: float32 [2, 1024], replicated
The draws below stay inside these ranges and needn't reach their ends.
All inputs are finite; a program needn't handle non-finite values.
Results may differ from the reference program's by a relative error of at most 0.004.
The reference program's roundings to bfloat16 on the way (of `queries`) count: a program that leaves them out, or rounds other values in their place, can miss the bound.
Values may be sent and summed in bfloat16 or wider, within the bound.
A program may use at most 64 MiB of HBM per device.

```python
import math
import jax
import jax.numpy as jnp
from jax import lax

D = 2048
HEADS = 8
MAP_HEAD_SIZE = 64
VD = 128
SEQS = 2
KW = 1024
VW = 1024
GROUP = 2
SUB = 128
TILES = 8
SPAN = 512
LEN = 8192
N_SP = 4


def shared_query(key):
    base = jax.random.normal(jax.random.fold_in(key, 11), (D, KW), jnp.float32)
    return jnp.clip(base, -6.0, 6.0) / math.sqrt(D)


def shared_new(key):
    base = jnp.clip(jax.random.normal(jax.random.fold_in(key, 13), (SEQS, D), jnp.float32), -6.0, 6.0) * 1.3
    return base


def draw_query_proj_matrix(key, part):
    return shared_query(key).astype(jnp.bfloat16)


def draw_key_weight(key, part):
    base = jax.random.normal(jax.random.fold_in(key, 12), (D, KW), jnp.float32)
    own = jnp.clip(base, -6.0, 6.0) / math.sqrt(D)
    matrix = own
    return matrix.astype(jnp.bfloat16)


def draw_new_token(key, part):
    return shared_new(key).astype(jnp.bfloat16)


def draw_prompt(key, part):
    base = jax.random.normal(jax.random.fold_in(key, 14), (SEQS, LEN, D), jnp.float32)
    base = jnp.clip(base, -6.0, 6.0) * 1.3
    return base.reshape(SEQS, TILES, GROUP, N_SP, SUB, D).astype(jnp.bfloat16)


def block_levels(rng, shape, pieces, smallest, top_value):
    loudness = 1.0
    for axis_at, blocks in pieces:
        draws = jax.random.uniform(jax.random.fold_in(jax.random.fold_in(rng, 6), axis_at), (blocks,), jnp.float32, smallest / len(pieces), top_value / len(pieces))
        loudness = loudness * jnp.repeat(jnp.exp(draws), shape[axis_at] // blocks).reshape((-1,) + (1,) * (len(shape) - 1 - axis_at))
    return loudness


def normal_values(stream_key, dims, spread, reach, pieces=(), held_as=jnp.bfloat16):
    result = spread * jax.random.normal(stream_key, dims, jnp.float32)
    if pieces:
        result = result * block_levels(stream_key, dims, pieces, -0.22, 0.18)
    return jnp.clip(result, -reach, reach).astype(held_as)


def setup_inputs(seed: int = 0) -> dict:
    splits = jax.random.split(jax.random.key(seed), 8)
    return {
        "prompt": draw_prompt(jax.random.fold_in(splits[7], 71), 0),
        "new_token": draw_new_token(jax.random.fold_in(splits[7], 71), 0),
        "query_proj_matrix": draw_query_proj_matrix(jax.random.fold_in(splits[7], 71), 0),
        "key_weight": draw_key_weight(jax.random.fold_in(splits[7], 71), 0),
        "value_weight": normal_values(splits[4], (D, VW), D ** -0.5, 0.125, ((1, 8),)),
        "map_balance": jnp.clip(jax.random.uniform(splits[5], (HEADS,), jnp.float32, 0.3, 0.8), 0.3, 0.8),
        "head_gain": jnp.clip(1.0 + 0.18 * jax.random.normal(splits[6], (VD,), jnp.float32), 0.1, 1.9),
    }


norm_eps = 1e-06

def project(inputs, weight_matrix):
    return jnp.dot(inputs, weight_matrix, preferred_element_type=jnp.float32).astype(jnp.bfloat16)

def relayout(rows, width):
    shaped = rows.reshape(SEQS, TILES, GROUP, SPAN, width)
    return jnp.transpose(shaped, (0, 2, 1, 3, 4)).reshape(SEQS * GROUP, TILES, SPAN, width)

def reference(prompt, new_token, query_proj_matrix, key_weight, value_weight, map_balance, head_gain):

    def cache_rows(sequence):
        flat_rows = sequence.reshape(LEN, D)
        return (project(flat_rows, key_weight), project(flat_rows, value_weight))
    flat_keys, flat_values = lax.map(cache_rows, prompt)
    queries = project(new_token, query_proj_matrix)
    new_keys = project(new_token, key_weight)
    new_values = project(new_token, value_weight)

    def read_one(inputs):
        seq_keys, seq_values, own_query, own_key, own_value = inputs
        every_key_row = jnp.concatenate([seq_keys, own_key[None, :]], axis=0)
        every_key_row = every_key_row.astype(jnp.float32).reshape(LEN + 1, HEADS, 2, MAP_HEAD_SIZE)
        all_values = jnp.concatenate([seq_values, own_value[None, :]], axis=0)
        all_values = all_values.astype(jnp.float32).reshape(LEN + 1, HEADS, VD)
        query_matrix_rows = own_query.astype(jnp.float32).reshape(HEADS, 2, MAP_HEAD_SIZE)
        logit_scores = jnp.einsum('rkx,vrkx->rkv', query_matrix_rows, every_key_row) * MAP_HEAD_SIZE ** (-0.5)
        probs = jax.nn.softmax(logit_scores, axis=-1)
        heads_out = jnp.einsum('hmj,jhe->hme', probs, all_values)
        blended = heads_out[:, 0] - map_balance[:, None] * heads_out[:, 1]
        normed = blended * lax.rsqrt(lax.optimization_barrier(jnp.mean(blended * blended, axis=-1, keepdims=True)) + norm_eps) * head_gain
        return normed.reshape(HEADS * VD)
    read = lax.map(read_one, (flat_keys, flat_values, queries, new_keys, new_values))
    return (relayout(flat_keys, KW), relayout(flat_values, VW), read)
```

```python
import functools

import jax
import jax.numpy as jnp
from jax import lax
from jax.experimental import pallas as pl
from jax.experimental.pallas import tpu as pltpu
from jax.sharding import PartitionSpec as P

HEADS = 8
MAP_HEAD_SIZE = 64
VD = 128


norm_eps = 1e-06
far_below = -1e30


def joined(part, axis, combine):
    gathered = jax.tree.map(lambda a: lax.all_gather(a, axis), part)

    def take(source):
        return jax.tree.map(lambda a: lax.dynamic_index_in_dim(a, source, 0, False), gathered)

    return lax.fori_loop(
        1, lax.axis_size(axis), lambda source, state: combine(state, take(source)), take(0)
    )


def fill_cols(source, w_piece):
    product = jnp.dot(source, w_piece, preferred_element_type=jnp.float32).astype(jnp.bfloat16)
    return product


def local_new(new_token, query_proj_matrix, key_weight, value_weight):
    return (
        jnp.dot(new_token, query_proj_matrix, preferred_element_type=jnp.float32).astype(
            jnp.bfloat16
        ),
        jnp.dot(new_token, key_weight, preferred_element_type=jnp.float32).astype(jnp.bfloat16),
        jnp.dot(new_token, value_weight, preferred_element_type=jnp.float32).astype(jnp.bfloat16),
    )


def partial_read(query_matrix_rows, key_rows, value_rows):
    logit_scores = jnp.einsum(
        "bhmd,bjhmd->bhmj", query_matrix_rows, key_rows, preferred_element_type=jnp.float32
    ) * MAP_HEAD_SIZE ** (-0.5)
    peak = jnp.max(logit_scores, axis=-1)
    weights_exp = jnp.exp(logit_scores - peak[..., None])
    totals = jnp.sum(weights_exp, axis=-1)
    weighted = jnp.einsum("bhmj,bjhe->bhme", weights_exp, value_rows.astype(jnp.float32))
    return (peak, totals, weighted)


def combine(first, second):
    peak_a, totals_a, weighted_a = first
    peak_b, totals_b, weighted_b = second
    peak = jnp.maximum(peak_a, peak_b)
    factor_a = jnp.exp(peak_a - peak)
    factor_b = jnp.exp(peak_b - peak)
    return (
        peak,
        totals_a * factor_a + totals_b * factor_b,
        weighted_a * factor_a[..., None] + weighted_b * factor_b[..., None],
    )


def shards(prompt, new_token, query_proj_matrix, key_weight, value_weight, map_balance, head_gain):
    seq_count, _, span_count, _, piece_rows, model_width = prompt.shape
    token_rows = prompt.reshape(seq_count * span_count * piece_rows, model_width)
    tp_count = lax.axis_size("tp")
    key_width = key_weight.shape[1] * tp_count
    value_width = value_weight.shape[1] * tp_count
    key_piece = lax.all_gather(key_weight, "tp", axis=1, tiled=True)
    value_piece = lax.all_gather(value_weight, "tp", axis=1, tiled=True)
    key_rows = fill_cols(token_rows, key_piece)
    value_rows = fill_cols(token_rows, value_piece)
    own_columns = local_new(new_token, query_proj_matrix, key_weight, value_weight)
    queries, new_keys, new_values = (
        lax.all_gather(own_columns[0], "tp", axis=1, tiled=True),
        lax.all_gather(own_columns[1], "tp", axis=1, tiled=True),
        lax.all_gather(own_columns[2], "tp", axis=1, tiled=True),
    )
    slot_count = seq_count * span_count
    cached_keys, cached_values = (
        lax.all_to_all(
            key_rows.reshape(slot_count, piece_rows, key_width),
            "sp",
            split_axis=0,
            concat_axis=1,
            tiled=True,
        ),
        lax.all_to_all(
            value_rows.reshape(slot_count, piece_rows, value_width),
            "sp",
            split_axis=0,
            concat_axis=1,
            tiled=True,
        ),
    )
    block_rows = cached_keys.shape[1]
    key_cache = cached_keys.reshape(1, 1, block_rows, key_width)
    value_cache = cached_values.reshape(1, 1, block_rows, value_width)
    all_queries = queries.reshape(seq_count, HEADS, 2, MAP_HEAD_SIZE)
    own_seq = lax.axis_index("sp") // span_count
    own_query = lax.dynamic_slice_in_dim(all_queries, own_seq, 1, 0)
    peak, totals, weighted = partial_read(
        own_query,
        cached_keys.reshape(1, block_rows, HEADS, 2, MAP_HEAD_SIZE),
        cached_values.reshape(1, block_rows, HEADS, VD),
    )
    chosen = jnp.arange(seq_count) == own_seq
    chosen_rows = chosen[:, None, None]
    spread = (
        jnp.where(chosen_rows, peak, far_below),
        jnp.where(chosen_rows, totals, 0.0),
        jnp.where(chosen_rows[..., None], weighted, 0.0),
    )
    merged = joined(spread, ("sp", "tp"), combine)
    own_keys = new_keys.reshape(seq_count, HEADS, 2, MAP_HEAD_SIZE)
    own_score = jnp.einsum(
        "bhmd,bhmd->bhm", all_queries, own_keys, preferred_element_type=jnp.float32
    ) * MAP_HEAD_SIZE ** (-0.5)
    own_values = new_values.astype(jnp.float32).reshape(seq_count, HEADS, VD)
    own_weighted = jnp.broadcast_to(own_values[:, :, None, :], (seq_count, HEADS, 2, VD))
    own_state = (own_score, jnp.ones_like(own_score), own_weighted)
    _, totals, weighted = combine(merged, own_state)
    heads_out = weighted / totals[..., None]
    blended = heads_out[:, :, 0] - map_balance[None, :, None] * heads_out[:, :, 1]
    normed = (
        blended
        * lax.rsqrt(jnp.mean(blended * blended, axis=-1, keepdims=True) + norm_eps)
        * head_gain
    )
    return (key_cache, value_cache, normed.reshape(seq_count, HEADS * VD))


MESH = pl.DeviceIdType.MESH
CORES = 2
PIECES = 2


def merged(states):
    peak = functools.reduce(jnp.maximum, [a[1] for a in states])
    factors = [jnp.exp(a[1] - peak) for a in states]
    weighted = functools.reduce(jnp.add, [a[0] * f for a, f in zip(states, factors)])
    total = functools.reduce(jnp.add, [a[2] * f for a, f in zip(states, factors)])
    return weighted, peak, total


def pack(ref, state):
    weighted, peak, total = state
    rows = weighted.shape[0]
    lane = lax.broadcasted_iota(jnp.int32, weighted.shape, 1)
    ref[:rows] = weighted
    ref[rows:] = jnp.where(lane < VD // 2, peak, total)


def unpack(ref):
    rows = ref.shape[0] // 2
    tail = ref[rows:]
    return ref[:rows], tail[:, :1], tail[:, VD // 2 : VD // 2 + 1]


def step_kernel(
    dims,
    prompt, token_hbm, wq_hbm, wk_hbm, wv_hbm, balance_hbm, gain_hbm,
    kv, read,
    xbuf, wbuf, kvbuf, wq, token, balance, gain, qbuf, pbuf, pstat, stbuf, finbuf,
    loc, line_send, prim_recv, xy_send, sec_recv, sib_send, sib_recv,
    out_send, out_recv, pk_send, pk_recv, st_send, st_recv, fin_send, fin_recv,
):
    sp_count, tp_count, seq_count = dims
    _, _, depth, wide = wbuf.shape
    cols = wide // CORES
    chips = tp_count // CORES
    rows = xbuf.shape[1]
    state_rows = CORES * 2 * seq_count
    s = lax.axis_index("sp")
    t = lax.axis_index("tp")
    z = t // CORES
    c = t % CORES
    sib = z * CORES + (1 - c)
    xs = s + 1 - 2 * (s % 2)
    ys = (s + 2) % 4
    diag = 3 - s
    prim = (s + s // 2) % 2
    sec = 1 - prim
    half = depth // 2
    step = half // PIECES
    part_rows = step // 2

    def lanes_of(core):
        return pl.ds(pl.multiple_of(core * cols, cols), cols)

    lanes, sib_lanes = lanes_of(c), lanes_of(1 - c)

    loads = [
        pltpu.make_async_copy(wk_hbm, wbuf.at[0, z, :, lanes], loc.at[0]),
        pltpu.make_async_copy(wv_hbm, wbuf.at[1, z, :, lanes], loc.at[1]),
        pltpu.make_async_copy(prompt, xbuf, loc.at[2]),
        pltpu.make_async_copy(token_hbm, token, loc.at[3]),
        pltpu.make_async_copy(wq_hbm, wq, loc.at[4]),
        pltpu.make_async_copy(balance_hbm, balance, loc.at[5]),
        pltpu.make_async_copy(gain_hbm, gain, loc.at[6]),
    ]
    for a in loads:
        a.start()

    peers = [(s, (t + d) % tp_count) for d in range(1, tp_count)]
    z_peers = [(s, (t + d * CORES) % tp_count) for d in range(1, chips)]
    plane_peers = [((s + d) % sp_count, t) for d in range(1, sp_count)]
    cross_peers = [((s + d) % sp_count, sib) for d in range(1, sp_count)]
    barrier = pltpu.get_barrier_semaphore()
    greeted = peers + plane_peers + cross_peers
    for p in greeted:
        pl.semaphore_signal(barrier, inc=1, device_id=p, device_id_type=MESH)
    pl.semaphore_wait(barrier, len(greeted))

    def remote(src, dst, send, recv, dev):
        return pltpu.make_async_remote_copy(
            src_ref=src, dst_ref=dst, send_sem=send, recv_sem=recv, device_id=dev, device_id_type=MESH
        )

    def push(view, send, recv, dev):
        remote(view, view, send, recv, dev).start()

    def got(view, recv):
        remote(view, view, xy_send, recv, (s, sib)).wait_recv()

    def gone(view, send):
        remote(view, view, send, loc.at[0], (s, sib)).wait_send()

    def span(start, size):
        return pl.ds(pl.multiple_of(start, size), size)

    def piece_of(m, zz, p):
        return wbuf.at[m, zz, span(prim * half + p * step, step), lanes]

    def line(direction, m, zz, p):
        view = piece_of(m, zz, p)
        push(view, line_send.at[(direction + 1) // 2], prim_recv.at[m, zz, p], (s, t + direction * CORES))

    def has_next(direction):
        return (z > 0) if direction < 0 else (z < chips - 1)

    for m in range(2):
        loads[m].wait()
        for direction in (-1, 1):
            @pl.when(has_next(direction))
            def _(direction=direction, m=m):
                for p in range(PIECES):
                    line(direction, m, z, p)
        push(wbuf.at[m, z, :, lanes], sib_send, sib_recv.at[m, z], (s, sib))

    loads[3].wait()
    loads[4].wait()
    vector = token[...]
    me_q = jnp.dot(vector, wq[...], preferred_element_type=jnp.float32)
    me_k = jnp.dot(vector, wbuf[0, z, :, lanes], preferred_element_type=jnp.float32)
    me_v = jnp.dot(vector, wbuf[1, z, :, lanes], preferred_element_type=jnp.float32)
    for i, value in enumerate((me_q, me_k, me_v)):
        value = value.astype(jnp.bfloat16).astype(jnp.float32)
        qbuf[t, i * seq_count : (i + 1) * seq_count, :] = value[:seq_count]

    near = jnp.minimum(z, chips - 1 - z)
    inside = near > 0

    def source(j):
        j = j + 1
        paired = j <= 2 * near
        dist = jnp.where(paired, (j + 1) // 2, j - near)
        from_left = jnp.where(paired, j % 2 == 1, z > near)
        return jnp.where(from_left, z - dist, z + dist), from_left

    def event(e):
        both = jnp.logical_and(inside, e < 8)
        j = jnp.where(both, e % 2, e // 4)
        m = jnp.where(both, e // 4, (e // 2) % 2)
        p = jnp.where(both, (e // 2) % 2, e % 2)
        return j, m, p

    def group(g):
        both = jnp.logical_and(inside, g < 4)
        return jnp.where(both, g % 2, g // 2), jnp.where(both, g // 2, g % 2)

    def arrive(e):
        j, m, p = event(e)
        zz, from_left = source(j)
        view = piece_of(m, zz, p)
        got(view, prim_recv.at[m, zz, p])
        on_right = jnp.logical_and(from_left, z < chips - 1)
        on_left = jnp.logical_and(jnp.logical_not(from_left), z > 0)
        pl.when(on_right)(lambda: line(1, m, zz, p))
        pl.when(on_left)(lambda: line(-1, m, zz, p))
        for h, to in enumerate((xs, ys)):
            part = wbuf.at[m, zz, span(prim * half + p * step + h * part_rows, part_rows), lanes]
            push(part, xy_send, sec_recv.at[m, zz], (to, t))
        push(view, sib_send, sib_recv.at[m, zz], (s, sib))

    def arrive_secondary(g):
        j, m = group(g)
        zz, _ = source(j)
        view = wbuf.at[m, zz, span(sec * half, half), lanes]
        got(view, sec_recv.at[m, zz])
        push(view, sib_send, sib_recv.at[m, zz], (s, sib))

    def columns_of(zz):
        return pl.ds(pl.multiple_of(zz * wide, wide), wide)

    def multiply(m, zz):
        got(wbuf.at[m, zz, :, sib_lanes], sib_recv.at[m, zz])
        columns = columns_of(zz)

        def some(i, _):
            at = pl.ds(2 * i, 2)
            product = jnp.dot(
                xbuf[at].reshape(-1, depth), wbuf[m, zz], preferred_element_type=jnp.float32
            ).astype(jnp.bfloat16)
            kvbuf[m, at, :, columns] = product.reshape(2, rows, wide)
            return 0

        lax.fori_loop(0, sp_count // 2, some, 0)
        kv[m, span(s * rows, rows), columns] = kvbuf[m, s, :, columns]

    def send_results(m, zz):
        columns = columns_of(zz)
        for p in (diag, xs, ys):
            remote(
                kvbuf.at[m, p, :, columns], kv.at[m, span(s * rows, rows), columns],
                out_send, out_recv, (p, t),
            ).start()

    scale = MAP_HEAD_SIZE ** (-0.5)
    row = lax.broadcasted_iota(jnp.int32, (state_rows, 1), 0)
    row_map = row // (CORES * seq_count)
    row_seq = (row // CORES) % seq_count
    row_head = row % CORES

    def by_seq(new, first):
        values = jnp.zeros((state_rows, new.shape[1]), jnp.float32)
        for b in range(seq_count):
            values = jnp.where(row_seq == b, new[first + b : first + b + 1], values)
        return values

    def by_head(values):
        return functools.reduce(
            jnp.add,
            [jnp.where(row_head == i, values[:, i * VD : (i + 1) * VD], 0.0) for i in range(CORES)],
        )

    def new_rows(zz):
        return jnp.concatenate([qbuf[zz * CORES + i] for i in range(CORES)], axis=1)

    def query_of(new):
        lane = lax.broadcasted_iota(jnp.int32, (state_rows, wide), 1)
        mine = lane // MAP_HEAD_SIZE == row_head * 2 + row_map
        return jnp.where(mine, by_seq(new, 0), 0.0)

    def score(j, zz):
        query = query_of(new_rows(zz)).astype(jnp.bfloat16)
        keys = kvbuf[0, :, :, columns_of(zz)].reshape(-1, wide)
        scores = lax.dot_general(
            query, keys, (((1,), (1,)), ((), ())), preferred_element_type=jnp.float32
        ) * scale
        at = lax.broadcasted_iota(jnp.int32, scores.shape, 1)
        mine = at // (scores.shape[1] // seq_count) == row_seq
        peak = jnp.max(jnp.where(mine, scores, far_below), axis=1, keepdims=True)
        raised = jnp.where(mine, jnp.exp(scores - peak), 0.0)
        total = jnp.sum(raised, axis=1, keepdims=True)
        high = raised.astype(jnp.bfloat16)
        low = (raised - high.astype(jnp.float32)).astype(jnp.bfloat16)
        pbuf[j, :state_rows] = high
        pbuf[j, state_rows:] = low
        pstat[j, 0] = jnp.broadcast_to(peak, (state_rows, VD))
        pstat[j, 1] = jnp.broadcast_to(total, (state_rows, VD))

    def weigh(j, zz):
        values = kvbuf[1, :, :, columns_of(zz)].reshape(-1, wide)
        both = jnp.dot(pbuf[j], values, preferred_element_type=jnp.float32)
        return by_head(both[:state_rows] + both[state_rows:]), pstat[j, 0][:, :1], pstat[j, 1][:, :1]

    def send_state(zz):
        view = stbuf.at[z, zz]
        for p in z_peers:
            push(view, st_send, st_recv.at[zz], p)

    mine_at = chips - 1
    loads[2].wait()
    multiply(0, z)
    for p in peers:
        push(qbuf.at[t], pk_send, pk_recv.at[t], p)
    send_results(0, z)
    multiply(1, z)
    got(qbuf.at[sib], pk_recv.at[sib])
    score(mine_at, z)
    send_results(1, z)
    new = new_rows(z)
    own_score = jnp.sum(query_of(new) * by_seq(new, seq_count), axis=1, keepdims=True) * scale
    holder = jnp.logical_and(s == 0, c == 0)
    own = (
        jnp.where(holder, by_head(by_seq(new, 2 * seq_count)), 0.0),
        jnp.where(holder, own_score, far_below),
        jnp.where(holder, jnp.ones_like(own_score), 0.0),
    )
    pack(stbuf.at[z, z], merged([weigh(mine_at, z), own]))

    def finish(g):
        j, m = group(g)
        zz, _ = source(j)
        multiply(m, zz)

        @pl.when(m == 0)
        def _():
            for i in range(CORES):
                got(qbuf.at[zz * CORES + i], pk_recv.at[zz * CORES + i])
            score(j, zz)
            send_results(m, zz)

        @pl.when(m == 1)
        def _():
            pack(stbuf.at[z, zz], weigh(j, zz))
            send_results(m, zz)
            send_state(zz)

    arrive(0)
    send_state(z)
    arrive(1)
    groups = 2 * (chips - 1)

    def work(g, _):
        arrive(2 * g)
        arrive_secondary(g - 1)
        arrive(2 * g + 1)
        finish(g - 1)
        return 0

    lax.fori_loop(1, groups, work, 0)

    me = s * CORES + c
    ends = (0, chips - 1)
    middle = tuple(range(1, chips - 1))

    def join_z(k, blocks):
        for i, zz in enumerate(blocks):
            got(stbuf.at[pl.ds(0, chips - 1), zz], st_recv.at[zz])
            pack(finbuf.at[k, me, i], merged([unpack(stbuf.at[a, zz]) for a in range(chips)]))
        for p in plane_peers + cross_peers + [(s, sib)]:
            push(finbuf.at[k, me], fin_send, fin_recv.at[k], p)

    join_z(0, middle)
    arrive_secondary(groups - 1)
    finish(groups - 1)
    join_z(1, ends)

    loads[5].wait()
    loads[6].wait()
    others = sp_count * CORES - 1
    fold = state_rows // 2
    for k, blocks in ((0, middle), (1, ends)):
        got(finbuf.at[k, pl.ds(0, others)], fin_recv.at[k])
        for i, zz in enumerate(blocks):
            weighted, _, total = merged([unpack(finbuf.at[k, a, i]) for a in range(others + 1)])
            heads_out = weighted / total
            lane = lax.broadcasted_iota(jnp.int32, (fold, HEADS), 1)
            chosen = lane == zz * CORES + lax.broadcasted_iota(jnp.int32, (fold, HEADS), 0) % CORES
            second = jnp.sum(jnp.where(chosen, balance[...], 0.0), axis=1, keepdims=True)
            blended = heads_out[:fold] - second * heads_out[fold:]
            normed = (
                blended
                * lax.rsqrt(jnp.mean(blended * blended, axis=1, keepdims=True) + norm_eps)
                * gain[...]
            )
            for b in range(seq_count):
                for h in range(CORES):
                    r = b * CORES + h
                    read[b : b + 1, (zz * CORES + h) * VD : (zz * CORES + h + 1) * VD] = normed[r : r + 1]

    others_rows = pl.ds(0, sp_count - 1)
    got(kvbuf.at[:, others_rows], out_recv)
    gone(kvbuf.at[:, others_rows], out_send)
    gone(wbuf.at[0, pl.ds(0, chips - 1), :, lanes], xy_send)
    gone(wbuf.at[:, :, :, lanes], sib_send)
    gone(qbuf.at[pl.ds(0, tp_count - 1)], pk_send)
    gone(stbuf.at[pl.ds(0, chips - 1)], st_send)
    gone(finbuf.at[:, pl.ds(0, others)], fin_send)
    for direction, count in ((-1, chips - z), (1, z + 1)):
        for n in range(1, chips):
            @pl.when(jnp.logical_and(has_next(direction), count == n))
            def _(direction=direction, n=n):
                gone(
                    wbuf.at[:, pl.ds(0, n), pl.ds(0, half), lanes],
                    line_send.at[(direction + 1) // 2],
                )


def store_kernel(kv, read, keys_out, values_out, read_out, sem):
    copies = [
        pltpu.make_async_copy(kv.at[0], keys_out, sem.at[0]),
        pltpu.make_async_copy(kv.at[1], values_out, sem.at[1]),
        pltpu.make_async_copy(read, read_out, sem.at[2]),
    ]
    for a in copies:
        a.start()
    for a in copies:
        a.wait()


def fused(prompt, new_token, query_proj_matrix, key_weight, value_weight, map_balance, head_gain):
    seq_count, _, span_count, _, piece_rows, width = prompt.shape
    sp_count, tp_count = lax.axis_size("sp"), lax.axis_size("tp")
    cols = key_weight.shape[1]
    slots = seq_count * span_count
    chips = tp_count // CORES
    key_width = cols * tp_count
    block_rows = sp_count * piece_rows
    state_rows = CORES * 2 * seq_count
    any_space = pl.BlockSpec(memory_space=pltpu.HBM)
    vmem = pl.BlockSpec(memory_space=pltpu.VMEM)
    dma = pltpu.SemaphoreType.DMA
    kv, read = pl.pallas_call(
        functools.partial(step_kernel, (sp_count, tp_count, seq_count)),
        out_shape=[
            pltpu.VMEM((2, block_rows, key_width), jnp.bfloat16),
            pltpu.VMEM((seq_count, HEADS * VD), jnp.float32),
        ],
        in_specs=[any_space] * 7,
        out_specs=[vmem, vmem],
        scratch_shapes=[
            pltpu.VMEM((slots, piece_rows, width), jnp.bfloat16),
            pltpu.VMEM((2, chips, width, CORES * cols), jnp.bfloat16),
            pltpu.VMEM((2, slots, piece_rows, key_width), jnp.bfloat16),
            pltpu.VMEM((width, cols), jnp.bfloat16),
            pltpu.VMEM((seq_count, width), jnp.bfloat16),
            pltpu.VMEM((1, HEADS), jnp.float32),
            pltpu.VMEM((1, VD), jnp.float32),
            pltpu.VMEM((tp_count, 8, cols), jnp.float32),
            pltpu.VMEM((chips, 2 * state_rows, slots * piece_rows), jnp.bfloat16),
            pltpu.VMEM((chips, 2, state_rows, VD), jnp.float32),
            pltpu.VMEM((chips, chips, 2 * state_rows, VD), jnp.float32),
            pltpu.VMEM((2, sp_count * CORES, 2, 2 * state_rows, VD), jnp.float32),
            dma((7,)), dma((2,)), dma((2, chips, PIECES)), dma(()), dma((2, chips)),
            dma(()), dma((2, chips)),
            dma(()), dma(()), dma(()), dma((tp_count,)), dma(()), dma((chips,)), dma(()), dma((2,)),
        ],
        compiler_params=pltpu.CompilerParams(
            collective_id=0, has_side_effects=True, vmem_limit_bytes=61 * 1024 * 1024 + 800 * 1024
        ),
    )(
        prompt.reshape(slots, piece_rows, width),
        new_token, query_proj_matrix, key_weight, value_weight,
        map_balance[None, :], head_gain[None, :],
    )
    keys, values, read = pl.pallas_call(
        store_kernel,
        out_shape=[
            jax.ShapeDtypeStruct((block_rows, key_width), jnp.bfloat16),
            jax.ShapeDtypeStruct((block_rows, key_width), jnp.bfloat16),
            jax.ShapeDtypeStruct(read.shape, jnp.float32),
        ],
        in_specs=[vmem, vmem],
        out_specs=[any_space] * 3,
        scratch_shapes=[dma((3,))],
        compiler_params=pltpu.CompilerParams(vmem_limit_bytes=1024 * 1024),
    )(kv, read)
    shape = (1, 1, block_rows, key_width)
    return keys.reshape(shape), values.reshape(shape), read


def fits(mesh, key_weight, value_weight, prompt):
    tp_count, sp_count = mesh.shape["tp"], mesh.shape["sp"]
    seq_count, _, span_count = prompt.shape[:3]
    cols = key_weight.shape[1] // tp_count
    return (
        sp_count == 4
        and seq_count * span_count == sp_count
        and tp_count % CORES == 0
        and tp_count == 4 * CORES
        and cols == VD
        and 3 * seq_count <= 8
        and key_weight.shape == value_weight.shape
    )


def solution(mesh):
    in_specs = (
        P(None, "tp", None, "sp", None, None),
        P(),
        P(None, "tp"),
        P(None, "tp"),
        P(None, "tp"),
        P(),
        P(),
    )
    out_specs = (P("sp", "tp", None, None), P("sp", "tp", None, None), P())

    def step(prompt, new_token, query_proj_matrix, key_weight, value_weight, map_balance, head_gain):
        body = fused if fits(mesh, key_weight, value_weight, prompt) else shards
        mapped = jax.shard_map(
            body, mesh=mesh, in_specs=in_specs, out_specs=out_specs, check_vma=False
        )
        return mapped(
            prompt, new_token, query_proj_matrix, key_weight, value_weight, map_balance, head_gain
        )

    return step
```

```python
import functools

import jax
import jax.numpy as jnp
from jax import lax
from jax.experimental import pallas as pl
from jax.experimental.pallas import tpu as pltpu
from jax.sharding import PartitionSpec as P

HEADS = 8
MAP_HEAD_SIZE = 64
VD = 128


norm_eps = 1e-06
far_below = -1e30


def joined(part, axis, combine):
    gathered = jax.tree.map(lambda a: lax.all_gather(a, axis), part)

    def take(source):
        return jax.tree.map(lambda a: lax.dynamic_index_in_dim(a, source, 0, False), gathered)

    return lax.fori_loop(
        1, lax.axis_size(axis), lambda source, state: combine(state, take(source)), take(0)
    )


def fill_cols(source, w_piece):
    product = jnp.dot(source, w_piece, preferred_element_type=jnp.float32).astype(jnp.bfloat16)
    return product


def local_new(new_token, query_proj_matrix, key_weight, value_weight):
    return (
        jnp.dot(new_token, query_proj_matrix, preferred_element_type=jnp.float32).astype(
            jnp.bfloat16
        ),
        jnp.dot(new_token, key_weight, preferred_element_type=jnp.float32).astype(jnp.bfloat16),
        jnp.dot(new_token, value_weight, preferred_element_type=jnp.float32).astype(jnp.bfloat16),
    )


def partial_read(query_matrix_rows, key_rows, value_rows):
    logit_scores = jnp.einsum(
        "bhmd,bjhmd->bhmj", query_matrix_rows, key_rows, preferred_element_type=jnp.float32
    ) * MAP_HEAD_SIZE ** (-0.5)
    peak = jnp.max(logit_scores, axis=-1)
    weights_exp = jnp.exp(logit_scores - peak[..., None])
    totals = jnp.sum(weights_exp, axis=-1)
    weighted = jnp.einsum("bhmj,bjhe->bhme", weights_exp, value_rows.astype(jnp.float32))
    return (peak, totals, weighted)


def combine(first, second):
    peak_a, totals_a, weighted_a = first
    peak_b, totals_b, weighted_b = second
    peak = jnp.maximum(peak_a, peak_b)
    factor_a = jnp.exp(peak_a - peak)
    factor_b = jnp.exp(peak_b - peak)
    return (
        peak,
        totals_a * factor_a + totals_b * factor_b,
        weighted_a * factor_a[..., None] + weighted_b * factor_b[..., None],
    )


def shards(prompt, new_token, query_proj_matrix, key_weight, value_weight, map_balance, head_gain):
    seq_count, _, span_count, _, piece_rows, model_width = prompt.shape
    token_rows = prompt.reshape(seq_count * span_count * piece_rows, model_width)
    tp_count = lax.axis_size("tp")
    key_width = key_weight.shape[1] * tp_count
    value_width = value_weight.shape[1] * tp_count
    key_piece = lax.all_gather(key_weight, "tp", axis=1, tiled=True)
    value_piece = lax.all_gather(value_weight, "tp", axis=1, tiled=True)
    key_rows = fill_cols(token_rows, key_piece)
    value_rows = fill_cols(token_rows, value_piece)
    own_columns = local_new(new_token, query_proj_matrix, key_weight, value_weight)
    queries, new_keys, new_values = (
        lax.all_gather(own_columns[0], "tp", axis=1, tiled=True),
        lax.all_gather(own_columns[1], "tp", axis=1, tiled=True),
        lax.all_gather(own_columns[2], "tp", axis=1, tiled=True),
    )
    slot_count = seq_count * span_count
    cached_keys, cached_values = (
        lax.all_to_all(
            key_rows.reshape(slot_count, piece_rows, key_width),
            "sp",
            split_axis=0,
            concat_axis=1,
            tiled=True,
        ),
        lax.all_to_all(
            value_rows.reshape(slot_count, piece_rows, value_width),
            "sp",
            split_axis=0,
            concat_axis=1,
            tiled=True,
        ),
    )
    block_rows = cached_keys.shape[1]
    key_cache = cached_keys.reshape(1, 1, block_rows, key_width)
    value_cache = cached_values.reshape(1, 1, block_rows, value_width)
    all_queries = queries.reshape(seq_count, HEADS, 2, MAP_HEAD_SIZE)
    own_seq = lax.axis_index("sp") // span_count
    own_query = lax.dynamic_slice_in_dim(all_queries, own_seq, 1, 0)
    peak, totals, weighted = partial_read(
        own_query,
        cached_keys.reshape(1, block_rows, HEADS, 2, MAP_HEAD_SIZE),
        cached_values.reshape(1, block_rows, HEADS, VD),
    )
    chosen = jnp.arange(seq_count) == own_seq
    chosen_rows = chosen[:, None, None]
    spread = (
        jnp.where(chosen_rows, peak, far_below),
        jnp.where(chosen_rows, totals, 0.0),
        jnp.where(chosen_rows[..., None], weighted, 0.0),
    )
    merged = joined(spread, ("sp", "tp"), combine)
    own_keys = new_keys.reshape(seq_count, HEADS, 2, MAP_HEAD_SIZE)
    own_score = jnp.einsum(
        "bhmd,bhmd->bhm", all_queries, own_keys, preferred_element_type=jnp.float32
    ) * MAP_HEAD_SIZE ** (-0.5)
    own_values = new_values.astype(jnp.float32).reshape(seq_count, HEADS, VD)
    own_weighted = jnp.broadcast_to(own_values[:, :, None, :], (seq_count, HEADS, 2, VD))
    own_state = (own_score, jnp.ones_like(own_score), own_weighted)
    _, totals, weighted = combine(merged, own_state)
    heads_out = weighted / totals[..., None]
    blended = heads_out[:, :, 0] - map_balance[None, :, None] * heads_out[:, :, 1]
    normed = (
        blended
        * lax.rsqrt(jnp.mean(blended * blended, axis=-1, keepdims=True) + norm_eps)
        * head_gain
    )
    return (key_cache, value_cache, normed.reshape(seq_count, HEADS * VD))


MESH = pl.DeviceIdType.MESH
CORES = 2
PIECES = 2


def merged(states):
    peak = functools.reduce(jnp.maximum, [a[1] for a in states])
    factors = [jnp.exp(a[1] - peak) for a in states]
    weighted = functools.reduce(jnp.add, [a[0] * f for a, f in zip(states, factors)])
    total = functools.reduce(jnp.add, [a[2] * f for a, f in zip(states, factors)])
    return weighted, peak, total


def pack(ref, at, stat_at, state):
    weighted, peak, total = state
    rows = weighted.shape[0]
    lane = lax.broadcasted_iota(jnp.int32, weighted.shape, 1)
    row = lax.broadcasted_iota(jnp.int32, weighted.shape, 0)
    stats = jnp.where(lane == row, peak, jnp.where(lane == row + rows, total, 0.0))
    ref[at : at + rows] = weighted
    ref[stat_at : stat_at + 1] = jnp.sum(stats, axis=0, keepdims=True)


def unpack(ref, at, stat_at, rows):
    weighted = ref[at : at + rows]
    lane = lax.broadcasted_iota(jnp.int32, weighted.shape, 1)
    row = lax.broadcasted_iota(jnp.int32, weighted.shape, 0)
    stats = ref[stat_at : stat_at + 1]
    peak = jnp.sum(jnp.where(lane == row, stats, 0.0), axis=1, keepdims=True)
    total = jnp.sum(jnp.where(lane == row + rows, stats, 0.0), axis=1, keepdims=True)
    return weighted, peak, total


def step_kernel(
    dims,
    prompt, token_hbm, wq_hbm, wk_hbm, wv_hbm,
    kv, finbuf,
    xbuf, wbuf, kvbuf, wq, token, qbuf, pbuf, pstat, stbuf,
    loc, far_send, far_recv, line_send, prim_recv, xy_send, sec_recv, sib_send, sib_recv,
    out_send, out_recv, pk_send, pk_recv, st_send, st_recv, fin_send, fin_recv,
):
    sp_count, tp_count, seq_count = dims
    _, _, depth, wide = wbuf.shape
    cols = wide // CORES
    chips = tp_count // CORES
    rows = xbuf.shape[1]
    state_rows = CORES * 2 * seq_count
    s = lax.axis_index("sp")
    t = lax.axis_index("tp")
    z = t // CORES
    c = t % CORES
    sib = z * CORES + (1 - c)
    xs = s + 1 - 2 * (s % 2)
    ys = (s + 2) % 4
    diag = 3 - s
    prim = (s + s // 2) % 2
    sec = 1 - prim
    half = depth // 2
    step = half // PIECES
    part_rows = step // 2

    def lanes_of(core):
        return pl.ds(pl.multiple_of(core * cols, cols), cols)

    lanes, sib_lanes = lanes_of(c), lanes_of(1 - c)

    loads = [
        pltpu.make_async_copy(wk_hbm, wbuf.at[0, z, :, lanes], loc.at[0]),
        pltpu.make_async_copy(wv_hbm, wbuf.at[1, z, :, lanes], loc.at[1]),
        pltpu.make_async_copy(prompt.at[xs], xbuf.at[0], loc.at[2]),
        pltpu.make_async_copy(prompt.at[ys], xbuf.at[1], loc.at[3]),
        pltpu.make_async_copy(token_hbm, token, loc.at[4]),
        pltpu.make_async_copy(wq_hbm, wq, loc.at[5]),
        pltpu.make_async_copy(prompt.at[s], xbuf.at[2], loc.at[6]),
    ]
    for a in loads:
        a.start()

    peers = [(s, (t + d) % tp_count) for d in range(1, tp_count)]
    z_peers = [(s, (t + d * CORES) % tp_count) for d in range(1, chips)]
    plane_peers = [((s + d) % sp_count, t) for d in range(1, sp_count)]
    cross_peers = [((s + d) % sp_count, sib) for d in range(1, sp_count)]
    barrier = pltpu.get_barrier_semaphore()
    greeted = peers + plane_peers + cross_peers
    for p in greeted:
        pl.semaphore_signal(barrier, inc=1, device_id=p, device_id_type=MESH)
    pl.semaphore_wait(barrier, len(greeted))

    def remote(src, dst, send, recv, dev):
        return pltpu.make_async_remote_copy(
            src_ref=src, dst_ref=dst, send_sem=send, recv_sem=recv, device_id=dev, device_id_type=MESH
        )

    def push(view, send, recv, dev):
        remote(view, view, send, recv, dev).start()

    def got(view, recv):
        remote(view, view, xy_send, recv, (s, sib)).wait_recv()

    def gone(view, send):
        remote(view, view, send, loc.at[0], (s, sib)).wait_send()

    def span(start, size):
        return pl.ds(pl.multiple_of(start, size), size)

    def piece_of(m, zz, p):
        return wbuf.at[m, zz, span(prim * half + p * step, step), lanes]

    def line(direction, m, zz, p):
        view = piece_of(m, zz, p)
        push(view, line_send.at[(direction + 1) // 2], prim_recv.at[m, zz, p], (s, t + direction * CORES))

    def has_next(direction):
        return (z > 0) if direction < 0 else (z < chips - 1)

    far_prompt = remote(prompt.at[diag], xbuf.at[3], far_send, far_recv, (diag, t))
    far_prompt.start()
    for m in range(2):
        loads[m].wait()
        for direction in (-1, 1):
            @pl.when(has_next(direction))
            def _(direction=direction, m=m):
                for p in range(PIECES):
                    line(direction, m, z, p)
        push(wbuf.at[m, z, :, lanes], sib_send, sib_recv.at[m, z], (s, sib))

    near = jnp.minimum(z, chips - 1 - z)
    inside = near > 0

    def source(j):
        j = j + 1
        paired = j <= 2 * near
        dist = jnp.where(paired, (j + 1) // 2, j - near)
        from_left = jnp.where(paired, j % 2 == 1, z > near)
        return jnp.where(from_left, z - dist, z + dist), from_left

    def event(e):
        both = jnp.logical_and(inside, e < 8)
        j = jnp.where(both, e % 2, e // 4)
        m = jnp.where(both, e // 4, (e // 2) % 2)
        p = jnp.where(both, (e // 2) % 2, e % 2)
        return j, m, p

    def group(g):
        both = jnp.logical_and(inside, g < 4)
        return jnp.where(both, g % 2, g // 2), jnp.where(both, g // 2, g % 2)

    def arrive(e):
        j, m, p = event(e)
        zz, from_left = source(j)
        view = piece_of(m, zz, p)
        got(view, prim_recv.at[m, zz, p])
        on_right = jnp.logical_and(from_left, z < chips - 1)
        on_left = jnp.logical_and(jnp.logical_not(from_left), z > 0)
        pl.when(on_right)(lambda: line(1, m, zz, p))
        pl.when(on_left)(lambda: line(-1, m, zz, p))
        for h, to in enumerate((xs, ys)):
            part = wbuf.at[m, zz, span(prim * half + p * step + h * part_rows, part_rows), lanes]
            push(part, xy_send, sec_recv.at[m, zz], (to, t))
        push(view, sib_send, sib_recv.at[m, zz], (s, sib))

    def arrive_secondary(g):
        j, m = group(g)
        zz, _ = source(j)
        view = wbuf.at[m, zz, span(sec * half, half), lanes]
        got(view, sec_recv.at[m, zz])
        push(view, sib_send, sib_recv.at[m, zz], (s, sib))

    def columns_of(zz):
        return pl.ds(pl.multiple_of(zz * wide, wide), wide)

    def product(pair, m, zz, first, width):
        at = pl.ds(2 * pair, 2)
        columns = span(zz * wide + first, width)
        out = jnp.dot(
            xbuf[at].reshape(-1, depth), wbuf[m, zz, :, span(first, width)],
            preferred_element_type=jnp.float32,
        ).astype(jnp.bfloat16)
        kvbuf[m, at, :, columns] = out.reshape(2, rows, width)
        return columns

    def keep(m, columns):
        for i, slot in ((2, s), (3, diag)):
            kv[m, span(slot * rows, rows), columns] = kvbuf[m, i, :, columns]

    def multiply(m, zz):
        got(wbuf.at[m, zz, :, sib_lanes], sib_recv.at[m, zz])

        def some(pair, _):
            product(pair, m, zz, 0, wide)
            return 0

        lax.fori_loop(0, 2, some, 0)
        keep(m, columns_of(zz))

    def send_columns(m, columns):
        for i, p in enumerate((xs, ys)):
            remote(
                kvbuf.at[m, i, :, columns], kv.at[m, span(s * rows, rows), columns],
                out_send, out_recv, (p, t),
            ).start()

    scale = MAP_HEAD_SIZE ** (-0.5)
    row = lax.broadcasted_iota(jnp.int32, (state_rows, 1), 0)
    row_map = row // (CORES * seq_count)
    row_seq = (row // CORES) % seq_count
    row_head = row % CORES

    def by_seq(new, first):
        values = jnp.zeros((state_rows, new.shape[1]), jnp.float32)
        for b in range(seq_count):
            values = jnp.where(row_seq == b, new[first + b : first + b + 1], values)
        return values

    def by_head(values):
        return functools.reduce(
            jnp.add,
            [jnp.where(row_head == i, values[:, i * VD : (i + 1) * VD], 0.0) for i in range(CORES)],
        )

    def new_rows(zz):
        return jnp.concatenate([qbuf[zz * CORES + i] for i in range(CORES)], axis=1)

    def query_of(new):
        lane = lax.broadcasted_iota(jnp.int32, (state_rows, wide), 1)
        mine = lane // MAP_HEAD_SIZE == row_head * 2 + row_map
        return jnp.where(mine, by_seq(new, 0), 0.0)

    def score(j, zz):
        query = query_of(new_rows(zz)).astype(jnp.bfloat16)
        keys = kvbuf[0, :, :, columns_of(zz)].reshape(-1, wide)
        scores = lax.dot_general(
            query, keys, (((1,), (1,)), ((), ())), preferred_element_type=jnp.float32
        ) * scale
        at = lax.broadcasted_iota(jnp.int32, scores.shape, 1) // rows
        spans = sp_count // seq_count
        owner = jnp.where(at == 0, xs, jnp.where(at == 1, ys, s)) // spans
        mine = owner == row_seq
        peak = jnp.max(jnp.where(mine, scores, far_below), axis=1, keepdims=True)
        raised = jnp.where(mine, jnp.exp(scores - peak), 0.0)
        total = jnp.sum(raised, axis=1, keepdims=True)
        high = raised.astype(jnp.bfloat16)
        low = (raised - high.astype(jnp.float32)).astype(jnp.bfloat16)
        pbuf[j, :state_rows] = high
        pbuf[j, state_rows:] = low
        pstat[j, 0] = jnp.broadcast_to(peak, (state_rows, VD))
        pstat[j, 1] = jnp.broadcast_to(total, (state_rows, VD))

    def weigh(j, zz):
        values = kvbuf[1, :, :, columns_of(zz)].reshape(-1, wide)
        both = jnp.dot(pbuf[j], values, preferred_element_type=jnp.float32)
        return by_head(both[:state_rows] + both[state_rows:]), pstat[j, 0][:, :1], pstat[j, 1][:, :1]

    def send_state(zz):
        view = stbuf.at[z, zz, pl.ds(0, state_rows + 1)]
        for p in z_peers:
            push(view, st_send, st_recv.at[zz], p)

    mine_at = chips - 1
    loads[2].wait()
    loads[3].wait()
    before = None
    for core in (c, 1 - c):
        for m in range(2):
            if core is not c:
                got(wbuf.at[m, z, :, sib_lanes], sib_recv.at[m, z])
            columns = product(0, m, z, core * cols, cols)
            if before is not None:
                send_columns(*before)
            before = (m, columns)

    def vectors():
        loads[4].wait()
        loads[5].wait()
        vector = token[...]
        me_q = jnp.dot(vector, wq[...], preferred_element_type=jnp.float32)
        me_k = jnp.dot(vector, wbuf[0, z, :, lanes], preferred_element_type=jnp.float32)
        me_v = jnp.dot(vector, wbuf[1, z, :, lanes], preferred_element_type=jnp.float32)
        for i, value in enumerate((me_q, me_k, me_v)):
            value = value.astype(jnp.bfloat16).astype(jnp.float32)
            qbuf[t, i * seq_count : (i + 1) * seq_count, :] = value[:seq_count]
    def own_block():
        loads[6].wait()
        far_prompt.wait_recv()

        def some(m, _):
            product(1, m, z, 0, wide)
            keep(m, columns_of(z))
            return 0

        lax.fori_loop(0, 2, some, 0)
        got(qbuf.at[sib], pk_recv.at[sib])
        score(mine_at, z)
        new = new_rows(z)
        own_score = jnp.sum(query_of(new) * by_seq(new, seq_count), axis=1, keepdims=True) * scale
        holder = jnp.logical_and(s == 0, c == 0)
        own = (
            jnp.where(holder, by_head(by_seq(new, 2 * seq_count)), 0.0),
            jnp.where(holder, own_score, far_below),
            jnp.where(holder, jnp.ones_like(own_score), 0.0),
        )
        pack(stbuf.at[z, z], 0, state_rows, merged([weigh(mine_at, z), own]))

    def compute(g):
        j, m = group(g)
        zz, _ = source(j)
        multiply(m, zz)

        @pl.when(m == 0)
        def _():
            for i in range(CORES):
                got(qbuf.at[zz * CORES + i], pk_recv.at[zz * CORES + i])
            score(j, zz)

        @pl.when(m == 1)
        def _():
            pack(stbuf.at[z, zz], 0, state_rows, weigh(j, zz))

    def results(g):
        j, m = group(g)
        zz, _ = source(j)
        send_columns(m, columns_of(zz))

    def state(g):
        j, m = group(g)
        zz, _ = source(j)
        pl.when(m == 1)(lambda: send_state(zz))

    groups = 2 * (chips - 1)
    def finish(g):
        compute(g)
        results(g)
        state(g)

    own_at = jnp.where(inside, 7, 4)

    def work(e, _):
        arrive(e)

        @pl.when(e == 0)
        def _():
            send_columns(*before)
            vectors()

        @pl.when(e == 1)
        def _():
            for p in peers:
                push(qbuf.at[t], pk_send, pk_recv.at[t], p)

        pl.when(e == own_at)(own_block)
        pl.when(e == own_at + 1)(lambda: send_state(z))
        outside = jnp.logical_not(inside)
        done = jnp.where(e < 9, e - 6, e - 7)
        pl.when(outside & (e >= 6) & (e != 9))(lambda: finish(done))
        ready = jnp.where(inside, e - 10, jnp.where(e < 8, e - 5, e - 6))
        pl.when((ready >= 0) & (inside | ((e != 8) & (e < 11))))(lambda: arrive_secondary(ready))
        return 0

    events = 2 * groups
    lax.fori_loop(0, events, work, 0)

    def rest(g, _):
        finish(g)
        pl.when(g + 2 < groups)(lambda: arrive_secondary(g + 2))
        return 0

    lax.fori_loop(0, jnp.where(inside, groups - 1, 0), rest, 0)
    pl.when(jnp.logical_not(inside))(lambda: arrive_secondary(groups - 1))

    me = s * CORES + c
    ends = (0, chips - 1)
    middle = tuple(range(1, chips - 1))

    def join_z(k, blocks):
        for i, zz in enumerate(blocks):
            got(stbuf.at[pl.ds(0, chips - 1), zz, pl.ds(0, state_rows + 1)], st_recv.at[zz])
            whole = merged([unpack(stbuf.at[a, zz], 0, state_rows, state_rows) for a in range(chips)])
            pack(finbuf.at[k, me], i * state_rows, len(blocks) * state_rows + i, whole)

    def send_joined(k, blocks):
        view = finbuf.at[k, me, pl.ds(0, len(blocks) * (state_rows + 1))]
        for p in plane_peers + cross_peers + [(s, sib)]:
            push(view, fin_send, fin_recv.at[k], p)

    join_z(0, middle)
    compute(groups - 1)
    send_joined(0, middle)
    state(groups - 1)
    results(groups - 1)
    join_z(1, ends)
    send_joined(1, ends)
    others = sp_count * CORES - 1
    fin_rows = pl.ds(0, 2 * (state_rows + 1))
    for k in range(2):
        got(finbuf.at[k, pl.ds(0, others), fin_rows], fin_recv.at[k])

    others_rows = pl.ds(0, 2)
    far_prompt.wait_send()
    got(kvbuf.at[:, others_rows], out_recv)
    gone(kvbuf.at[:, others_rows], out_send)
    gone(wbuf.at[0, pl.ds(0, chips - 1), :, lanes], xy_send)
    gone(wbuf.at[:, :, :, lanes], sib_send)
    gone(qbuf.at[pl.ds(0, tp_count - 1)], pk_send)
    gone(stbuf.at[pl.ds(0, chips - 1), :, pl.ds(0, state_rows + 1)], st_send)
    gone(finbuf.at[:, pl.ds(0, others), fin_rows], fin_send)
    for direction, count in ((-1, chips - z), (1, z + 1)):
        for n in range(1, chips):
            @pl.when(jnp.logical_and(has_next(direction), count == n))
            def _(direction=direction, n=n):
                gone(
                    wbuf.at[:, pl.ds(0, n), pl.ds(0, half), lanes],
                    line_send.at[(direction + 1) // 2],
                )


def store_kernel(
    blocks, kv, finbuf, balance_hbm, gain_hbm, keys_out, values_out, read_out, read, balance, gain, sem
):
    copies = [
        pltpu.make_async_copy(balance_hbm, balance, sem.at[0]),
        pltpu.make_async_copy(gain_hbm, gain, sem.at[1]),
        pltpu.make_async_copy(kv.at[0], keys_out, sem.at[2]),
        pltpu.make_async_copy(kv.at[1], values_out, sem.at[3]),
        pltpu.make_async_copy(read, read_out, sem.at[4]),
    ]
    for a in copies[:4]:
        a.start()
    devices, state_rows = finbuf.shape[1], CORES * 2 * read.shape[0]
    fold = state_rows // 2
    seq_count = read.shape[0]
    heads = {}
    for k, zz_list in enumerate(blocks):
        for i, zz in enumerate(zz_list):
            at, stat_at = i * state_rows, len(zz_list) * state_rows + i
            weighted, _, total = merged(
                [unpack(finbuf.at[k, a], at, stat_at, state_rows) for a in range(devices)]
            )
            heads[zz] = weighted / total
    copies[0].wait()
    copies[1].wait()
    for zz, heads_out in heads.items():
        lane = lax.broadcasted_iota(jnp.int32, (fold, HEADS), 1)
        chosen = lane == zz * CORES + lax.broadcasted_iota(jnp.int32, (fold, HEADS), 0) % CORES
        second = jnp.sum(jnp.where(chosen, balance[...], 0.0), axis=1, keepdims=True)
        blended = heads_out[:fold] - second * heads_out[fold:]
        normed = (
            blended
            * lax.rsqrt(jnp.mean(blended * blended, axis=1, keepdims=True) + norm_eps)
            * gain[...]
        )
        for b in range(seq_count):
            for h in range(CORES):
                r = b * CORES + h
                read[b : b + 1, (zz * CORES + h) * VD : (zz * CORES + h + 1) * VD] = normed[r : r + 1]
    copies[4].start()
    for a in copies[2:]:
        a.wait()


def fused(prompt, new_token, query_proj_matrix, key_weight, value_weight, map_balance, head_gain):
    seq_count, _, span_count, _, piece_rows, width = prompt.shape
    sp_count, tp_count = lax.axis_size("sp"), lax.axis_size("tp")
    cols = key_weight.shape[1]
    slots = seq_count * span_count
    chips = tp_count // CORES
    key_width = cols * tp_count
    block_rows = sp_count * piece_rows
    state_rows = CORES * 2 * seq_count
    any_space = pl.BlockSpec(memory_space=pltpu.HBM)
    vmem = pl.BlockSpec(memory_space=pltpu.VMEM)
    dma = pltpu.SemaphoreType.DMA
    kv, states = pl.pallas_call(
        functools.partial(step_kernel, (sp_count, tp_count, seq_count)),
        out_shape=[
            pltpu.VMEM((2, block_rows, key_width), jnp.bfloat16),
            pltpu.VMEM((2, sp_count * CORES, 2 * state_rows + 8, VD), jnp.float32),
        ],
        in_specs=[any_space] * 5,
        out_specs=[vmem, vmem],
        scratch_shapes=[
            pltpu.VMEM((slots, piece_rows, width), jnp.bfloat16),
            pltpu.VMEM((2, chips, width, CORES * cols), jnp.bfloat16),
            pltpu.VMEM((2, slots, piece_rows, key_width), jnp.bfloat16),
            pltpu.VMEM((width, cols), jnp.bfloat16),
            pltpu.VMEM((seq_count, width), jnp.bfloat16),
            pltpu.VMEM((tp_count, 8, cols), jnp.float32),
            pltpu.VMEM((chips, 2 * state_rows, slots * piece_rows), jnp.bfloat16),
            pltpu.VMEM((chips, 2, state_rows, VD), jnp.float32),
            pltpu.VMEM((chips, chips, 2 * state_rows, VD), jnp.float32),
            dma((7,)), dma(()), dma(()), dma((2,)), dma((2, chips, PIECES)), dma(()), dma((2, chips)),
            dma(()), dma((2, chips)),
            dma(()), dma(()), dma(()), dma((tp_count,)), dma(()), dma((chips,)), dma(()), dma((2,)),
        ],
        compiler_params=pltpu.CompilerParams(
            collective_id=0, has_side_effects=True, vmem_limit_bytes=61 * 1024 * 1024 + 512 * 1024
        ),
    )(
        prompt.reshape(slots, piece_rows, width),
        new_token, query_proj_matrix, key_weight, value_weight,
    )
    blocks = (tuple(range(1, chips - 1)), (0, chips - 1))
    keys, values, read = pl.pallas_call(
        functools.partial(store_kernel, blocks),
        out_shape=[
            jax.ShapeDtypeStruct((block_rows, key_width), jnp.bfloat16),
            jax.ShapeDtypeStruct((block_rows, key_width), jnp.bfloat16),
            jax.ShapeDtypeStruct((seq_count, HEADS * VD), jnp.float32),
        ],
        in_specs=[vmem, vmem, any_space, any_space],
        out_specs=[any_space] * 3,
        scratch_shapes=[
            pltpu.VMEM((seq_count, HEADS * VD), jnp.float32),
            pltpu.VMEM((1, HEADS), jnp.float32),
            pltpu.VMEM((1, VD), jnp.float32),
            dma((5,)),
        ],
        compiler_params=pltpu.CompilerParams(vmem_limit_bytes=1024 * 1024),
    )(kv, states, map_balance[None, :], head_gain[None, :])
    shape = (1, 1, block_rows, key_width)
    return keys.reshape(shape), values.reshape(shape), read


def fits(mesh, key_weight, value_weight, prompt):
    tp_count, sp_count = mesh.shape["tp"], mesh.shape["sp"]
    seq_count, _, span_count = prompt.shape[:3]
    cols = key_weight.shape[1] // tp_count
    return (
        sp_count == 4
        and seq_count * span_count == sp_count
        and tp_count % CORES == 0
        and tp_count == 4 * CORES
        and cols == VD
        and 3 * seq_count <= 8
        and key_weight.shape == value_weight.shape
    )


def solution(mesh):
    in_specs = (
        P(None, "tp", None, "sp", None, None),
        P(),
        P(None, "tp"),
        P(None, "tp"),
        P(None, "tp"),
        P(),
        P(),
    )
    out_specs = (P("sp", "tp", None, None), P("sp", "tp", None, None), P())

    def step(prompt, new_token, query_proj_matrix, key_weight, value_weight, map_balance, head_gain):
        body = fused if fits(mesh, key_weight, value_weight, prompt) else shards
        mapped = jax.shard_map(
            body, mesh=mesh, in_specs=in_specs, out_specs=out_specs, check_vma=False
        )
        return mapped(
            prompt, new_token, query_proj_matrix, key_weight, value_weight, map_balance, head_gain
        )

    return step
```

```python
import functools

import jax
import jax.numpy as jnp
from jax import lax
from jax.experimental import pallas as pl
from jax.experimental.pallas import tpu as pltpu
from jax.sharding import PartitionSpec as P

HEADS = 8
MAP_HEAD_SIZE = 64
VD = 128


norm_eps = 1e-06
far_below = -1e30


def joined(part, axis, combine):
    gathered = jax.tree.map(lambda a: lax.all_gather(a, axis), part)

    def take(source):
        return jax.tree.map(lambda a: lax.dynamic_index_in_dim(a, source, 0, False), gathered)

    return lax.fori_loop(
        1, lax.axis_size(axis), lambda source, state: combine(state, take(source)), take(0)
    )


def fill_cols(source, w_piece):
    product = jnp.dot(source, w_piece, preferred_element_type=jnp.float32).astype(jnp.bfloat16)
    return product


def local_new(new_token, query_proj_matrix, key_weight, value_weight):
    return (
        jnp.dot(new_token, query_proj_matrix, preferred_element_type=jnp.float32).astype(
            jnp.bfloat16
        ),
        jnp.dot(new_token, key_weight, preferred_element_type=jnp.float32).astype(jnp.bfloat16),
        jnp.dot(new_token, value_weight, preferred_element_type=jnp.float32).astype(jnp.bfloat16),
    )


def partial_read(query_matrix_rows, key_rows, value_rows):
    logit_scores = jnp.einsum(
        "bhmd,bjhmd->bhmj", query_matrix_rows, key_rows, preferred_element_type=jnp.float32
    ) * MAP_HEAD_SIZE ** (-0.5)
    peak = jnp.max(logit_scores, axis=-1)
    weights_exp = jnp.exp(logit_scores - peak[..., None])
    totals = jnp.sum(weights_exp, axis=-1)
    weighted = jnp.einsum("bhmj,bjhe->bhme", weights_exp, value_rows.astype(jnp.float32))
    return (peak, totals, weighted)


def combine(first, second):
    peak_a, totals_a, weighted_a = first
    peak_b, totals_b, weighted_b = second
    peak = jnp.maximum(peak_a, peak_b)
    factor_a = jnp.exp(peak_a - peak)
    factor_b = jnp.exp(peak_b - peak)
    return (
        peak,
        totals_a * factor_a + totals_b * factor_b,
        weighted_a * factor_a[..., None] + weighted_b * factor_b[..., None],
    )


def shards(prompt, new_token, query_proj_matrix, key_weight, value_weight, map_balance, head_gain):
    seq_count, _, span_count, _, piece_rows, model_width = prompt.shape
    token_rows = prompt.reshape(seq_count * span_count * piece_rows, model_width)
    tp_count = lax.axis_size("tp")
    key_width = key_weight.shape[1] * tp_count
    value_width = value_weight.shape[1] * tp_count
    key_piece = lax.all_gather(key_weight, "tp", axis=1, tiled=True)
    value_piece = lax.all_gather(value_weight, "tp", axis=1, tiled=True)
    key_rows = fill_cols(token_rows, key_piece)
    value_rows = fill_cols(token_rows, value_piece)
    own_columns = local_new(new_token, query_proj_matrix, key_weight, value_weight)
    queries, new_keys, new_values = (
        lax.all_gather(own_columns[0], "tp", axis=1, tiled=True),
        lax.all_gather(own_columns[1], "tp", axis=1, tiled=True),
        lax.all_gather(own_columns[2], "tp", axis=1, tiled=True),
    )
    slot_count = seq_count * span_count
    cached_keys, cached_values = (
        lax.all_to_all(
            key_rows.reshape(slot_count, piece_rows, key_width),
            "sp",
            split_axis=0,
            concat_axis=1,
            tiled=True,
        ),
        lax.all_to_all(
            value_rows.reshape(slot_count, piece_rows, value_width),
            "sp",
            split_axis=0,
            concat_axis=1,
            tiled=True,
        ),
    )
    block_rows = cached_keys.shape[1]
    key_cache = cached_keys.reshape(1, 1, block_rows, key_width)
    value_cache = cached_values.reshape(1, 1, block_rows, value_width)
    all_queries = queries.reshape(seq_count, HEADS, 2, MAP_HEAD_SIZE)
    own_seq = lax.axis_index("sp") // span_count
    own_query = lax.dynamic_slice_in_dim(all_queries, own_seq, 1, 0)
    peak, totals, weighted = partial_read(
        own_query,
        cached_keys.reshape(1, block_rows, HEADS, 2, MAP_HEAD_SIZE),
        cached_values.reshape(1, block_rows, HEADS, VD),
    )
    chosen = jnp.arange(seq_count) == own_seq
    chosen_rows = chosen[:, None, None]
    spread = (
        jnp.where(chosen_rows, peak, far_below),
        jnp.where(chosen_rows, totals, 0.0),
        jnp.where(chosen_rows[..., None], weighted, 0.0),
    )
    merged = joined(spread, ("sp", "tp"), combine)
    own_keys = new_keys.reshape(seq_count, HEADS, 2, MAP_HEAD_SIZE)
    own_score = jnp.einsum(
        "bhmd,bhmd->bhm", all_queries, own_keys, preferred_element_type=jnp.float32
    ) * MAP_HEAD_SIZE ** (-0.5)
    own_values = new_values.astype(jnp.float32).reshape(seq_count, HEADS, VD)
    own_weighted = jnp.broadcast_to(own_values[:, :, None, :], (seq_count, HEADS, 2, VD))
    own_state = (own_score, jnp.ones_like(own_score), own_weighted)
    _, totals, weighted = combine(merged, own_state)
    heads_out = weighted / totals[..., None]
    blended = heads_out[:, :, 0] - map_balance[None, :, None] * heads_out[:, :, 1]
    normed = (
        blended
        * lax.rsqrt(jnp.mean(blended * blended, axis=-1, keepdims=True) + norm_eps)
        * head_gain
    )
    return (key_cache, value_cache, normed.reshape(seq_count, HEADS * VD))


MESH = pl.DeviceIdType.MESH
CORES = 2
PIECES = 2


def merged(states):
    peak = functools.reduce(jnp.maximum, [a[1] for a in states])
    factors = [jnp.exp(a[1] - peak) for a in states]
    weighted = functools.reduce(jnp.add, [a[0] * f for a, f in zip(states, factors)])
    total = functools.reduce(jnp.add, [a[2] * f for a, f in zip(states, factors)])
    return weighted, peak, total


def pack(ref, at, stat_at, state):
    weighted, peak, total = state
    rows = weighted.shape[0]
    lane = lax.broadcasted_iota(jnp.int32, weighted.shape, 1)
    row = lax.broadcasted_iota(jnp.int32, weighted.shape, 0)
    stats = jnp.where(lane == row, peak, jnp.where(lane == row + rows, total, 0.0))
    ref[at : at + rows] = weighted
    ref[stat_at : stat_at + 1] = jnp.sum(stats, axis=0, keepdims=True)


def unpack(ref, at, stat_at, rows):
    weighted = ref[at : at + rows]
    lane = lax.broadcasted_iota(jnp.int32, weighted.shape, 1)
    row = lax.broadcasted_iota(jnp.int32, weighted.shape, 0)
    stats = ref[stat_at : stat_at + 1]
    peak = jnp.sum(jnp.where(lane == row, stats, 0.0), axis=1, keepdims=True)
    total = jnp.sum(jnp.where(lane == row + rows, stats, 0.0), axis=1, keepdims=True)
    return weighted, peak, total


def step_kernel(
    dims,
    prompt, token_hbm, wq_hbm, wk_hbm, wv_hbm,
    kv, finbuf,
    xbuf, wbuf, kvbuf, upbuf, wq, token, qbuf, pbuf, pstat, stbuf,
    loc, far_send, far_recv, line_send, prim_recv, xy_send, sec_recv, relay_recv, sib_send, sib_recv,
    out_send, out_recv, up_recv, pk_send, pk_recv, st_send, st_recv, fin_send, fin_recv,
):
    sp_count, tp_count, seq_count = dims
    _, _, depth, wide = wbuf.shape
    cols = wide // CORES
    chips = tp_count // CORES
    rows = xbuf.shape[1]
    state_rows = CORES * 2 * seq_count
    s = lax.axis_index("sp")
    t = lax.axis_index("tp")
    z = t // CORES
    c = t % CORES
    sib = z * CORES + (1 - c)
    xs = s + 1 - 2 * (s % 2)
    ys = (s + 2) % 4
    diag = 3 - s
    prim = (s + s // 2) % 2
    sec = 1 - prim
    turn = s // 2
    near = jnp.minimum(z, chips - 1 - z)
    inside = near > 0
    outside = jnp.logical_not(inside)
    half = depth // 2
    step = half // PIECES
    part_rows = step // 2

    def lanes_of(core):
        return pl.ds(pl.multiple_of(core * cols, cols), cols)

    lanes, sib_lanes = lanes_of(c), lanes_of(1 - c)

    loads = [
        pltpu.make_async_copy(wk_hbm, wbuf.at[0, z, :, lanes], loc.at[0]),
        pltpu.make_async_copy(wv_hbm, wbuf.at[1, z, :, lanes], loc.at[1]),
        pltpu.make_async_copy(prompt.at[xs], xbuf.at[0], loc.at[2]),
        pltpu.make_async_copy(prompt.at[ys], xbuf.at[1], loc.at[3]),
        pltpu.make_async_copy(token_hbm, token, loc.at[4]),
        pltpu.make_async_copy(wq_hbm, wq, loc.at[5]),
        pltpu.make_async_copy(prompt.at[s], xbuf.at[2], loc.at[6]),
    ]
    for a in loads:
        a.start()

    peers = [(s, (t + d) % tp_count) for d in range(1, tp_count)]
    z_peers = [(s, (t + d * CORES) % tp_count) for d in range(1, chips)]
    plane_peers = [((s + d) % sp_count, t) for d in range(1, sp_count)]
    cross_peers = [((s + d) % sp_count, sib) for d in range(1, sp_count)]
    barrier = pltpu.get_barrier_semaphore()
    greeted = peers + plane_peers + cross_peers
    for p in greeted:
        pl.semaphore_signal(barrier, inc=1, device_id=p, device_id_type=MESH)
    pl.semaphore_wait(barrier, len(greeted))

    def remote(src, dst, send, recv, dev):
        return pltpu.make_async_remote_copy(
            src_ref=src, dst_ref=dst, send_sem=send, recv_sem=recv, device_id=dev, device_id_type=MESH
        )

    def push(view, send, recv, dev):
        remote(view, view, send, recv, dev).start()

    def got(view, recv):
        remote(view, view, xy_send, recv, (s, sib)).wait_recv()

    def gone(view, send):
        remote(view, view, send, loc.at[0], (s, sib)).wait_send()

    def span(start, size):
        return pl.ds(pl.multiple_of(start, size), size)

    def piece_of(m, zz, p):
        return wbuf.at[m, zz, span(prim * half + p * step, step), lanes]

    def line(direction, m, zz, p):
        view = piece_of(m, zz, p)
        push(view, line_send.at[(direction + 1) // 2], prim_recv.at[m, zz, p], (s, t + direction * CORES))

    def has_next(direction):
        return (z > 0) if direction < 0 else (z < chips - 1)

    def to_end(direction):
        return (z == 1) if direction < 0 else (z == chips - 2)

    far_prompt = remote(prompt.at[diag], xbuf.at[3], far_send, far_recv, (diag, t))
    far_prompt.start()
    for m in range(2):
        loads[m].wait()
        for direction in (-1, 1):
            @pl.when(jnp.logical_and(has_next(direction), to_end(direction)))
            def _(direction=direction, m=m):
                line(direction, m, z, turn)

            @pl.when(jnp.logical_and(has_next(direction), jnp.logical_not(to_end(direction))))
            def _(direction=direction, m=m):
                for p in range(PIECES):
                    line(direction, m, z, p)
        push(wbuf.at[m, z, :, lanes], sib_send, sib_recv.at[m, z], (s, sib))

    def source(j):
        j = j + 1
        paired = j <= 2 * near
        dist = jnp.where(paired, (j + 1) // 2, j - near)
        from_left = jnp.where(paired, j % 2 == 1, z > near)
        return jnp.where(from_left, z - dist, z + dist), from_left

    def event(e):
        both = jnp.logical_and(inside, e < 8)
        j = jnp.where(both, e % 2, e // 4)
        m = jnp.where(both, e // 4, (e // 2) % 2)
        p = jnp.where(both, (e // 2) % 2, e % 2)
        single = jnp.logical_and(outside, e < 4)
        return j, jnp.where(single, e % 2, m), jnp.where(single, turn, p)

    def group(g):
        both = jnp.logical_and(inside, g < 4)
        return jnp.where(both, g % 2, g // 2), jnp.where(both, g // 2, g % 2)

    def arrive(e):
        j, m, p = event(e)
        zz, from_left = source(j)
        view = piece_of(m, zz, p)
        got(view, prim_recv.at[m, zz, p])
        on_right = jnp.logical_and(from_left, z < chips - 1)
        on_left = jnp.logical_and(jnp.logical_not(from_left), z > 0)
        pl.when(on_right)(lambda: line(1, m, zz, p))
        pl.when(on_left)(lambda: line(-1, m, zz, p))
        single = jnp.logical_and(outside, e < 4)

        @pl.when(single)
        def _():
            for to in (xs, ys):
                push(view, xy_send, sec_recv.at[m, zz], (to, t))

        @pl.when(jnp.logical_not(single))
        def _():
            for h, to in enumerate((xs, ys)):
                part = part_of(prim, m, zz, p, h)
                push(part, xy_send, sec_recv.at[m, zz], (to, t))

        push(view, sib_send, sib_recv.at[m, zz], (s, sib))

    def part_of(which, m, zz, p, h):
        return wbuf.at[m, zz, span(which * half + p * step + h * part_rows, part_rows), lanes]

    def arrive_secondary(g):
        j, m = group(g)
        zz, _ = source(j)
        view = wbuf.at[m, zz, span(sec * half, half), lanes]
        got(view, sec_recv.at[m, zz])

        @pl.when(jnp.logical_and(outside, g < 2))
        def _():
            push(part_of(sec, m, zz, 1 - turn, 0), xy_send, relay_recv.at[m], (xs, t))
            push(part_of(sec, m, zz, turn, 1), xy_send, relay_recv.at[m], (ys, t))

        push(view, sib_send, sib_recv.at[m, zz], (s, sib))

    def arrive_relayed(m):
        zz, _ = source(0)
        view = piece_of(m, zz, 1 - turn)
        got(view, relay_recv.at[m])
        push(view, sib_send, sib_recv.at[m, zz], (s, sib))

    def columns_of(zz):
        return pl.ds(pl.multiple_of(zz * wide, wide), wide)

    def product(pair, m, zz, first, width):
        at = pl.ds(2 * pair, 2)
        columns = span(zz * wide + first, width)
        out = jnp.dot(
            xbuf[at].reshape(-1, depth), wbuf[m, zz, :, span(first, width)],
            preferred_element_type=jnp.float32,
        ).astype(jnp.bfloat16)
        kvbuf[m, at, :, columns] = out.reshape(2, rows, width)
        return columns

    def keep(m, columns):
        for i, slot in ((2, s), (3, diag)):
            kv[m, span(slot * rows, rows), columns] = kvbuf[m, i, :, columns]

    def multiply(m, zz):
        got(wbuf.at[m, zz, :, sib_lanes], sib_recv.at[m, zz])

        def some(pair, _):
            product(pair, m, zz, 0, wide)
            return 0

        lax.fori_loop(0, 2, some, 0)
        keep(m, columns_of(zz))

    def send_columns(m, columns):
        for i, p in enumerate((xs, ys)):
            remote(
                kvbuf.at[m, i, :, columns], kv.at[m, span(s * rows, rows), columns],
                out_send, out_recv, (p, t),
            ).start()

    scale = MAP_HEAD_SIZE ** (-0.5)
    row = lax.broadcasted_iota(jnp.int32, (state_rows, 1), 0)
    row_map = row // (CORES * seq_count)
    row_seq = (row // CORES) % seq_count
    row_head = row % CORES

    def by_seq(new, first):
        values = jnp.zeros((state_rows, new.shape[1]), jnp.float32)
        for b in range(seq_count):
            values = jnp.where(row_seq == b, new[first + b : first + b + 1], values)
        return values

    def by_head(values):
        return functools.reduce(
            jnp.add,
            [jnp.where(row_head == i, values[:, i * VD : (i + 1) * VD], 0.0) for i in range(CORES)],
        )

    def new_rows(zz):
        return jnp.concatenate([qbuf[zz * CORES + i] for i in range(CORES)], axis=1)

    def query_of(new):
        lane = lax.broadcasted_iota(jnp.int32, (state_rows, wide), 1)
        mine = lane // MAP_HEAD_SIZE == row_head * 2 + row_map
        return jnp.where(mine, by_seq(new, 0), 0.0)

    def score(j, zz):
        query = query_of(new_rows(zz)).astype(jnp.bfloat16)
        keys = kvbuf[0, :, :, columns_of(zz)].reshape(-1, wide)
        scores = lax.dot_general(
            query, keys, (((1,), (1,)), ((), ())), preferred_element_type=jnp.float32
        ) * scale
        at = lax.broadcasted_iota(jnp.int32, scores.shape, 1) // rows
        spans = sp_count // seq_count
        owner = jnp.where(at == 0, xs, jnp.where(at == 1, ys, s)) // spans
        mine = owner == row_seq
        peak = jnp.max(jnp.where(mine, scores, far_below), axis=1, keepdims=True)
        raised = jnp.where(mine, jnp.exp(scores - peak), 0.0)
        total = jnp.sum(raised, axis=1, keepdims=True)
        high = raised.astype(jnp.bfloat16)
        low = (raised - high.astype(jnp.float32)).astype(jnp.bfloat16)
        pbuf[j, :state_rows] = high
        pbuf[j, state_rows:] = low
        pstat[j, 0] = jnp.broadcast_to(peak, (state_rows, VD))
        pstat[j, 1] = jnp.broadcast_to(total, (state_rows, VD))

    def weigh(j, zz):
        values = kvbuf[1, :, :, columns_of(zz)].reshape(-1, wide)
        both = jnp.dot(pbuf[j], values, preferred_element_type=jnp.float32)
        return by_head(both[:state_rows] + both[state_rows:]), pstat[j, 0][:, :1], pstat[j, 1][:, :1]

    def send_state(zz):
        view = stbuf.at[z, zz, pl.ds(0, state_rows + 1)]
        for p in z_peers:
            push(view, st_send, st_recv.at[zz], p)

    mine_at = chips - 1
    loads[2].wait()
    loads[3].wait()
    before = None
    for core in (c, 1 - c):
        for m in range(2):
            if core is not c:
                got(wbuf.at[m, z, :, sib_lanes], sib_recv.at[m, z])
            columns = product(0, m, z, core * cols, cols)
            if before is not None:
                pl.when(inside)(lambda before=before: send_columns(*before))
            before = (m, columns)

    def vectors():
        loads[4].wait()
        loads[5].wait()
        vector = token[...]
        me_q = jnp.dot(vector, wq[...], preferred_element_type=jnp.float32)
        me_k = jnp.dot(vector, wbuf[0, z, :, lanes], preferred_element_type=jnp.float32)
        me_v = jnp.dot(vector, wbuf[1, z, :, lanes], preferred_element_type=jnp.float32)
        for i, value in enumerate((me_q, me_k, me_v)):
            value = value.astype(jnp.bfloat16).astype(jnp.float32)
            qbuf[t, i * seq_count : (i + 1) * seq_count, :] = value[:seq_count]
    def own_block():
        loads[6].wait()
        far_prompt.wait_recv()

        def some(m, _):
            product(1, m, z, 0, wide)
            keep(m, columns_of(z))
            return 0

        lax.fori_loop(0, 2, some, 0)
        got(qbuf.at[sib], pk_recv.at[sib])
        score(mine_at, z)
        new = new_rows(z)
        own_score = jnp.sum(query_of(new) * by_seq(new, seq_count), axis=1, keepdims=True) * scale
        holder = jnp.logical_and(s == 0, c == 0)
        own = (
            jnp.where(holder, by_head(by_seq(new, 2 * seq_count)), 0.0),
            jnp.where(holder, own_score, far_below),
            jnp.where(holder, jnp.ones_like(own_score), 0.0),
        )
        pack(stbuf.at[z, z], 0, state_rows, merged([weigh(mine_at, z), own]))

    def compute(g):
        j, m = group(g)
        zz, _ = source(j)
        multiply(m, zz)

        @pl.when(m == 0)
        def _():
            for i in range(CORES):
                got(qbuf.at[zz * CORES + i], pk_recv.at[zz * CORES + i])
            score(j, zz)

        @pl.when(m == 1)
        def _():
            pack(stbuf.at[z, zz], 0, state_rows, weigh(j, zz))

    def results(g):
        j, m = group(g)
        zz, _ = source(j)
        send_columns(m, columns_of(zz))

    def state(g):
        j, m = group(g)
        zz, _ = source(j)
        pl.when(m == 1)(lambda: send_state(zz))

    groups = 2 * (chips - 1)
    def finish(g):
        compute(g)
        results(g)
        state(g)

    own_at = jnp.where(inside, 7, 5)

    def work(e, _):
        arrive(e)

        @pl.when(e == 2)
        def _():
            pl.when(inside)(lambda: send_columns(*before))

            @pl.when(outside)
            def _():
                inner = jnp.where(z == 0, t + CORES, t - CORES)
                for m in range(2):
                    for i, p in enumerate((xs, ys)):
                        remote(
                            kvbuf.at[m, i, :, columns_of(z)], upbuf.at[m, i],
                            out_send, up_recv, (p, inner),
                        ).start()

            vectors()

        @pl.when(e == 3)
        def _():
            for p in peers:
                push(qbuf.at[t], pk_send, pk_recv.at[t], p)

        pl.when(e == own_at)(own_block)
        pl.when(e == own_at + 1)(lambda: send_state(z))
        pl.when(outside & (e == 9))(lambda: compute(2))
        ready = jnp.where(inside, e - 10, jnp.where(e < 9, e - 6, e - 7))
        pl.when((ready >= 0) & (inside | ((e != 9) & (e < 11))))(lambda: arrive_secondary(ready))
        pl.when(outside & (e == 10))(lambda: arrive_relayed(0))
        return 0

    events = 2 * groups
    lax.fori_loop(jnp.where(inside, 0, 2), events, work, 0)

    @pl.when(inside)
    def _():
        got(upbuf, up_recv)
        outer = jnp.where(z == 1, z - 1, z + 1)
        for m in range(2):
            for i, p in enumerate((xs, ys)):
                remote(
                    upbuf.at[m, i], kv.at[m, span(p * rows, rows), columns_of(outer)],
                    out_send, out_recv, (s, outer * CORES + c),
                ).start()

    def rest(i, _):
        g = jnp.where(inside, i, jnp.where(i < 2, 3 * i, jnp.where(i == 2, 1, 4)))
        finish(g)

        @pl.when(inside & (i + 2 < groups))
        def _():
            arrive_secondary(i + 2)

        @pl.when(outside & (i == 0))
        def _():
            arrive_secondary(4)
            results(2)
            arrive_relayed(1)

        return 0

    lax.fori_loop(0, jnp.where(inside, groups - 1, groups - 2), rest, 0)
    pl.when(outside)(lambda: arrive_secondary(groups - 1))

    me = s * CORES + c
    ends = (0, chips - 1)
    middle = tuple(range(1, chips - 1))

    def join_z(k, blocks):
        for i, zz in enumerate(blocks):
            got(stbuf.at[pl.ds(0, chips - 1), zz, pl.ds(0, state_rows + 1)], st_recv.at[zz])
            whole = merged([unpack(stbuf.at[a, zz], 0, state_rows, state_rows) for a in range(chips)])
            pack(finbuf.at[k, me], i * state_rows, len(blocks) * state_rows + i, whole)

    def send_joined(k, blocks):
        view = finbuf.at[k, me, pl.ds(0, len(blocks) * (state_rows + 1))]
        for p in plane_peers + cross_peers + [(s, sib)]:
            push(view, fin_send, fin_recv.at[k], p)

    compute(groups - 1)
    results(groups - 1)
    state(groups - 1)
    join_z(0, middle)
    send_joined(0, middle)
    join_z(1, ends)
    send_joined(1, ends)
    others = sp_count * CORES - 1
    fin_rows = pl.ds(0, 2 * (state_rows + 1))
    for k in range(2):
        got(finbuf.at[k, pl.ds(0, others), fin_rows], fin_recv.at[k])

    def pieces_view(count):
        return wbuf.at[:, 0, pl.ds(0, count * step * cols // (2 * wide)), :]

    others_rows = pl.ds(0, 2)
    far_prompt.wait_send()
    got(kvbuf.at[:, others_rows], out_recv)
    for pieces, on in ((10, inside), (8, outside)):
        pl.when(on)(lambda pieces=pieces: gone(pieces_view(pieces), out_send))
    for pieces, on in ((12, inside), (14, outside)):
        pl.when(on)(lambda pieces=pieces: gone(pieces_view(pieces), xy_send))
    gone(wbuf.at[:, :, :, lanes], sib_send)
    gone(qbuf.at[pl.ds(0, tp_count - 1)], pk_send)
    gone(stbuf.at[pl.ds(0, chips - 1), :, pl.ds(0, state_rows + 1)], st_send)
    gone(finbuf.at[:, pl.ds(0, others), fin_rows], fin_send)
    for direction, count in ((-1, chips - z), (1, z + 1)):
        for n in range(1, chips):
            for fewer in (0, 2):
                @pl.when(has_next(direction) & (count == n) & (to_end(direction) == (fewer > 0)))
                def _(direction=direction, pieces=4 * n - fewer):
                    gone(pieces_view(pieces), line_send.at[(direction + 1) // 2])


def store_kernel(
    blocks, kv, finbuf, balance_hbm, gain_hbm, keys_out, values_out, read_out, read, balance, gain, sem
):
    copies = [
        pltpu.make_async_copy(balance_hbm, balance, sem.at[0]),
        pltpu.make_async_copy(gain_hbm, gain, sem.at[1]),
        pltpu.make_async_copy(kv.at[0], keys_out, sem.at[2]),
        pltpu.make_async_copy(kv.at[1], values_out, sem.at[3]),
        pltpu.make_async_copy(read, read_out, sem.at[4]),
    ]
    for a in copies[:4]:
        a.start()
    devices, state_rows = finbuf.shape[1], CORES * 2 * read.shape[0]
    fold = state_rows // 2
    seq_count = read.shape[0]
    heads = {}
    for k, zz_list in enumerate(blocks):
        for i, zz in enumerate(zz_list):
            at, stat_at = i * state_rows, len(zz_list) * state_rows + i
            weighted, _, total = merged(
                [unpack(finbuf.at[k, a], at, stat_at, state_rows) for a in range(devices)]
            )
            heads[zz] = weighted / total
    copies[0].wait()
    copies[1].wait()
    for zz, heads_out in heads.items():
        lane = lax.broadcasted_iota(jnp.int32, (fold, HEADS), 1)
        chosen = lane == zz * CORES + lax.broadcasted_iota(jnp.int32, (fold, HEADS), 0) % CORES
        second = jnp.sum(jnp.where(chosen, balance[...], 0.0), axis=1, keepdims=True)
        blended = heads_out[:fold] - second * heads_out[fold:]
        normed = (
            blended
            * lax.rsqrt(jnp.mean(blended * blended, axis=1, keepdims=True) + norm_eps)
            * gain[...]
        )
        for b in range(seq_count):
            for h in range(CORES):
                r = b * CORES + h
                read[b : b + 1, (zz * CORES + h) * VD : (zz * CORES + h + 1) * VD] = normed[r : r + 1]
    copies[4].start()
    for a in copies[2:]:
        a.wait()


def fused(prompt, new_token, query_proj_matrix, key_weight, value_weight, map_balance, head_gain):
    seq_count, _, span_count, _, piece_rows, width = prompt.shape
    sp_count, tp_count = lax.axis_size("sp"), lax.axis_size("tp")
    cols = key_weight.shape[1]
    slots = seq_count * span_count
    chips = tp_count // CORES
    key_width = cols * tp_count
    block_rows = sp_count * piece_rows
    state_rows = CORES * 2 * seq_count
    any_space = pl.BlockSpec(memory_space=pltpu.HBM)
    vmem = pl.BlockSpec(memory_space=pltpu.VMEM)
    dma = pltpu.SemaphoreType.DMA
    kv, states = pl.pallas_call(
        functools.partial(step_kernel, (sp_count, tp_count, seq_count)),
        out_shape=[
            pltpu.VMEM((2, block_rows, key_width), jnp.bfloat16),
            pltpu.VMEM((2, sp_count * CORES, 2 * state_rows + 8, VD), jnp.float32),
        ],
        in_specs=[any_space] * 5,
        out_specs=[vmem, vmem],
        scratch_shapes=[
            pltpu.VMEM((slots, piece_rows, width), jnp.bfloat16),
            pltpu.VMEM((2, chips, width, CORES * cols), jnp.bfloat16),
            pltpu.VMEM((2, slots, piece_rows, key_width), jnp.bfloat16),
            pltpu.VMEM((2, 2, piece_rows, CORES * cols), jnp.bfloat16),
            pltpu.VMEM((width, cols), jnp.bfloat16),
            pltpu.VMEM((seq_count, width), jnp.bfloat16),
            pltpu.VMEM((tp_count, 8, cols), jnp.float32),
            pltpu.VMEM((chips, 2 * state_rows, slots * piece_rows), jnp.bfloat16),
            pltpu.VMEM((chips, 2, state_rows, VD), jnp.float32),
            pltpu.VMEM((chips, chips, 2 * state_rows, VD), jnp.float32),
            dma((7,)), dma(()), dma(()), dma((2,)), dma((2, chips, PIECES)), dma(()), dma((2, chips)), dma((2,)),
            dma(()), dma((2, chips)),
            dma(()), dma(()), dma(()), dma(()), dma((tp_count,)), dma(()), dma((chips,)), dma(()), dma((2,)),
        ],
        compiler_params=pltpu.CompilerParams(
            collective_id=0, has_side_effects=True, vmem_limit_bytes=61 * 1024 * 1024 + 512 * 1024
        ),
    )(
        prompt.reshape(slots, piece_rows, width),
        new_token, query_proj_matrix, key_weight, value_weight,
    )
    blocks = (tuple(range(1, chips - 1)), (0, chips - 1))
    keys, values, read = pl.pallas_call(
        functools.partial(store_kernel, blocks),
        out_shape=[
            jax.ShapeDtypeStruct((block_rows, key_width), jnp.bfloat16),
            jax.ShapeDtypeStruct((block_rows, key_width), jnp.bfloat16),
            jax.ShapeDtypeStruct((seq_count, HEADS * VD), jnp.float32),
        ],
        in_specs=[vmem, vmem, any_space, any_space],
        out_specs=[any_space] * 3,
        scratch_shapes=[
            pltpu.VMEM((seq_count, HEADS * VD), jnp.float32),
            pltpu.VMEM((1, HEADS), jnp.float32),
            pltpu.VMEM((1, VD), jnp.float32),
            dma((5,)),
        ],
        compiler_params=pltpu.CompilerParams(vmem_limit_bytes=1024 * 1024),
    )(kv, states, map_balance[None, :], head_gain[None, :])
    shape = (1, 1, block_rows, key_width)
    return keys.reshape(shape), values.reshape(shape), read


def fits(mesh, key_weight, value_weight, prompt):
    tp_count, sp_count = mesh.shape["tp"], mesh.shape["sp"]
    seq_count, _, span_count = prompt.shape[:3]
    cols = key_weight.shape[1] // tp_count
    return (
        sp_count == 4
        and seq_count * span_count == sp_count
        and tp_count % CORES == 0
        and tp_count == 4 * CORES
        and cols == VD
        and 3 * seq_count <= 8
        and key_weight.shape == value_weight.shape
    )


def solution(mesh):
    in_specs = (
        P(None, "tp", None, "sp", None, None),
        P(),
        P(None, "tp"),
        P(None, "tp"),
        P(None, "tp"),
        P(),
        P(),
    )
    out_specs = (P("sp", "tp", None, None), P("sp", "tp", None, None), P())

    def step(prompt, new_token, query_proj_matrix, key_weight, value_weight, map_balance, head_gain):
        body = fused if fits(mesh, key_weight, value_weight, prompt) else shards
        mapped = jax.shard_map(
            body, mesh=mesh, in_specs=in_specs, out_specs=out_specs, check_vma=False
        )
        return mapped(
            prompt, new_token, query_proj_matrix, key_weight, value_weight, map_balance, head_gain
        )

    return step
```

```python
import functools

import jax
import jax.numpy as jnp
from jax import lax
from jax.experimental import pallas as pl
from jax.experimental.pallas import tpu as pltpu
from jax.sharding import PartitionSpec as P

HEADS = 8
MAP_HEAD_SIZE = 64
VD = 128


norm_eps = 1e-06
far_below = -1e30


def joined(part, axis, combine):
    gathered = jax.tree.map(lambda a: lax.all_gather(a, axis), part)

    def take(source):
        return jax.tree.map(lambda a: lax.dynamic_index_in_dim(a, source, 0, False), gathered)

    return lax.fori_loop(
        1, lax.axis_size(axis), lambda source, state: combine(state, take(source)), take(0)
    )


def fill_cols(source, w_piece):
    product = jnp.dot(source, w_piece, preferred_element_type=jnp.float32).astype(jnp.bfloat16)
    return product


def local_new(new_token, query_proj_matrix, key_weight, value_weight):
    return (
        jnp.dot(new_token, query_proj_matrix, preferred_element_type=jnp.float32).astype(
            jnp.bfloat16
        ),
        jnp.dot(new_token, key_weight, preferred_element_type=jnp.float32).astype(jnp.bfloat16),
        jnp.dot(new_token, value_weight, preferred_element_type=jnp.float32).astype(jnp.bfloat16),
    )


def partial_read(query_matrix_rows, key_rows, value_rows):
    logit_scores = jnp.einsum(
        "bhmd,bjhmd->bhmj", query_matrix_rows, key_rows, preferred_element_type=jnp.float32
    ) * MAP_HEAD_SIZE ** (-0.5)
    peak = jnp.max(logit_scores, axis=-1)
    weights_exp = jnp.exp(logit_scores - peak[..., None])
    totals = jnp.sum(weights_exp, axis=-1)
    weighted = jnp.einsum("bhmj,bjhe->bhme", weights_exp, value_rows.astype(jnp.float32))
    return (peak, totals, weighted)


def combine(first, second):
    peak_a, totals_a, weighted_a = first
    peak_b, totals_b, weighted_b = second
    peak = jnp.maximum(peak_a, peak_b)
    factor_a = jnp.exp(peak_a - peak)
    factor_b = jnp.exp(peak_b - peak)
    return (
        peak,
        totals_a * factor_a + totals_b * factor_b,
        weighted_a * factor_a[..., None] + weighted_b * factor_b[..., None],
    )


def shards(prompt, new_token, query_proj_matrix, key_weight, value_weight, map_balance, head_gain):
    seq_count, _, span_count, _, piece_rows, model_width = prompt.shape
    token_rows = prompt.reshape(seq_count * span_count * piece_rows, model_width)
    tp_count = lax.axis_size("tp")
    key_width = key_weight.shape[1] * tp_count
    value_width = value_weight.shape[1] * tp_count
    key_piece = lax.all_gather(key_weight, "tp", axis=1, tiled=True)
    value_piece = lax.all_gather(value_weight, "tp", axis=1, tiled=True)
    key_rows = fill_cols(token_rows, key_piece)
    value_rows = fill_cols(token_rows, value_piece)
    own_columns = local_new(new_token, query_proj_matrix, key_weight, value_weight)
    queries, new_keys, new_values = (
        lax.all_gather(own_columns[0], "tp", axis=1, tiled=True),
        lax.all_gather(own_columns[1], "tp", axis=1, tiled=True),
        lax.all_gather(own_columns[2], "tp", axis=1, tiled=True),
    )
    slot_count = seq_count * span_count
    cached_keys, cached_values = (
        lax.all_to_all(
            key_rows.reshape(slot_count, piece_rows, key_width),
            "sp",
            split_axis=0,
            concat_axis=1,
            tiled=True,
        ),
        lax.all_to_all(
            value_rows.reshape(slot_count, piece_rows, value_width),
            "sp",
            split_axis=0,
            concat_axis=1,
            tiled=True,
        ),
    )
    block_rows = cached_keys.shape[1]
    key_cache = cached_keys.reshape(1, 1, block_rows, key_width)
    value_cache = cached_values.reshape(1, 1, block_rows, value_width)
    all_queries = queries.reshape(seq_count, HEADS, 2, MAP_HEAD_SIZE)
    own_seq = lax.axis_index("sp") // span_count
    own_query = lax.dynamic_slice_in_dim(all_queries, own_seq, 1, 0)
    peak, totals, weighted = partial_read(
        own_query,
        cached_keys.reshape(1, block_rows, HEADS, 2, MAP_HEAD_SIZE),
        cached_values.reshape(1, block_rows, HEADS, VD),
    )
    chosen = jnp.arange(seq_count) == own_seq
    chosen_rows = chosen[:, None, None]
    spread = (
        jnp.where(chosen_rows, peak, far_below),
        jnp.where(chosen_rows, totals, 0.0),
        jnp.where(chosen_rows[..., None], weighted, 0.0),
    )
    merged = joined(spread, ("sp", "tp"), combine)
    own_keys = new_keys.reshape(seq_count, HEADS, 2, MAP_HEAD_SIZE)
    own_score = jnp.einsum(
        "bhmd,bhmd->bhm", all_queries, own_keys, preferred_element_type=jnp.float32
    ) * MAP_HEAD_SIZE ** (-0.5)
    own_values = new_values.astype(jnp.float32).reshape(seq_count, HEADS, VD)
    own_weighted = jnp.broadcast_to(own_values[:, :, None, :], (seq_count, HEADS, 2, VD))
    own_state = (own_score, jnp.ones_like(own_score), own_weighted)
    _, totals, weighted = combine(merged, own_state)
    heads_out = weighted / totals[..., None]
    blended = heads_out[:, :, 0] - map_balance[None, :, None] * heads_out[:, :, 1]
    normed = (
        blended
        * lax.rsqrt(jnp.mean(blended * blended, axis=-1, keepdims=True) + norm_eps)
        * head_gain
    )
    return (key_cache, value_cache, normed.reshape(seq_count, HEADS * VD))


MESH = pl.DeviceIdType.MESH
CORES = 2
PIECES = 2


def merged(states):
    peak = functools.reduce(jnp.maximum, [a[1] for a in states])
    factors = [jnp.exp(a[1] - peak) for a in states]
    weighted = functools.reduce(jnp.add, [a[0] * f for a, f in zip(states, factors)])
    total = functools.reduce(jnp.add, [a[2] * f for a, f in zip(states, factors)])
    return weighted, peak, total


def pack(ref, at, stat_at, state):
    weighted, peak, total = state
    rows = weighted.shape[0]
    lane = lax.broadcasted_iota(jnp.int32, weighted.shape, 1)
    row = lax.broadcasted_iota(jnp.int32, weighted.shape, 0)
    stats = jnp.where(lane == row, peak, jnp.where(lane == row + rows, total, 0.0))
    ref[at : at + rows] = weighted
    ref[stat_at : stat_at + 1] = jnp.sum(stats, axis=0, keepdims=True)


def unpack(ref, at, stat_at, rows):
    weighted = ref[at : at + rows]
    lane = lax.broadcasted_iota(jnp.int32, weighted.shape, 1)
    row = lax.broadcasted_iota(jnp.int32, weighted.shape, 0)
    stats = ref[stat_at : stat_at + 1]
    peak = jnp.sum(jnp.where(lane == row, stats, 0.0), axis=1, keepdims=True)
    total = jnp.sum(jnp.where(lane == row + rows, stats, 0.0), axis=1, keepdims=True)
    return weighted, peak, total


def step_kernel(
    dims,
    prompt, token_hbm, wq_hbm, wk_hbm, wv_hbm,
    kv, finbuf,
    xbuf, wbuf, kvbuf, upbuf, partial, wq, token, qbuf, pbuf, pstat, stbuf,
    loc, far_send, far_recv, line_send, prim_recv, xy_send, sec_recv, relay_recv, sib_send, sib_recv,
    out_send, out_recv, up_recv, pk_send, pk_recv, st_send, st_recv, fin_send, fin_recv,
):
    sp_count, tp_count, seq_count = dims
    _, _, depth, wide = wbuf.shape
    cols = wide // CORES
    chips = tp_count // CORES
    rows = xbuf.shape[1]
    state_rows = CORES * 2 * seq_count
    s = lax.axis_index("sp")
    t = lax.axis_index("tp")
    z = t // CORES
    c = t % CORES
    sib = z * CORES + (1 - c)
    xs = s + 1 - 2 * (s % 2)
    ys = (s + 2) % 4
    diag = 3 - s
    prim = (s + s // 2) % 2
    sec = 1 - prim
    turn = s // 2
    near = jnp.minimum(z, chips - 1 - z)
    inside = near > 0
    outside = jnp.logical_not(inside)
    half = depth // 2
    step = half // PIECES
    part_rows = step // 2

    def lanes_of(core):
        return pl.ds(pl.multiple_of(core * cols, cols), cols)

    lanes, sib_lanes = lanes_of(c), lanes_of(1 - c)

    loads = [
        pltpu.make_async_copy(wk_hbm, wbuf.at[0, z, :, lanes], loc.at[0]),
        pltpu.make_async_copy(wv_hbm, wbuf.at[1, z, :, lanes], loc.at[1]),
        pltpu.make_async_copy(prompt.at[xs], xbuf.at[0], loc.at[2]),
        pltpu.make_async_copy(prompt.at[ys], xbuf.at[1], loc.at[3]),
        pltpu.make_async_copy(token_hbm, token, loc.at[4]),
        pltpu.make_async_copy(wq_hbm, wq, loc.at[5]),
        pltpu.make_async_copy(prompt.at[s], xbuf.at[2], loc.at[6]),
    ]
    for a in loads:
        a.start()

    z_peers = [(s, (t + d * CORES) % tp_count) for d in range(1, chips)]
    plane_peers = [((s + d) % sp_count, t) for d in range(1, sp_count)]
    cross_peers = [((s + d) % sp_count, sib) for d in range(1, sp_count)]
    barrier = pltpu.get_barrier_semaphore()
    greeted = plane_peers + [(s, sib)]

    def greet(p):
        pl.semaphore_signal(barrier, inc=1, device_id=p, device_id_type=MESH)

    pl.when(z > 0)(lambda: greet((s, t - CORES)))
    pl.when(z < chips - 1)(lambda: greet((s, t + CORES)))
    for p in greeted:
        greet(p)
    pl.semaphore_wait(barrier, len(greeted) + jnp.where(inside, 2, 1))

    def remote(src, dst, send, recv, dev):
        return pltpu.make_async_remote_copy(
            src_ref=src, dst_ref=dst, send_sem=send, recv_sem=recv, device_id=dev, device_id_type=MESH
        )

    def push(view, send, recv, dev):
        remote(view, view, send, recv, dev).start()

    def got(view, recv):
        remote(view, view, xy_send, recv, (s, sib)).wait_recv()

    def gone(view, send):
        remote(view, view, send, loc.at[0], (s, sib)).wait_send()

    def span(start, size):
        return pl.ds(pl.multiple_of(start, size), size)

    def piece_of(m, zz, p):
        return wbuf.at[m, zz, span(prim * half + p * step, step), lanes]

    def line(direction, m, zz, p):
        view = piece_of(m, zz, p)
        push(view, line_send.at[(direction + 1) // 2], prim_recv.at[m, zz, p], (s, t + direction * CORES))

    def has_next(direction):
        return (z > 0) if direction < 0 else (z < chips - 1)

    def to_end(direction):
        return (z == 1) if direction < 0 else (z == chips - 2)

    far_prompt = remote(prompt.at[diag], xbuf.at[3], far_send, far_recv, (diag, t))
    far_prompt.start()
    for m in range(2):
        loads[m].wait()
        for direction in (-1, 1):
            @pl.when(jnp.logical_and(has_next(direction), to_end(direction)))
            def _(direction=direction, m=m):
                line(direction, m, z, turn)

            @pl.when(jnp.logical_and(has_next(direction), jnp.logical_not(to_end(direction))))
            def _(direction=direction, m=m):
                for p in range(PIECES):
                    line(direction, m, z, p)
        push(wbuf.at[m, z, :, lanes], sib_send, sib_recv.at[m, z], (s, sib))
    inner = jnp.where(z == 0, t + CORES, t - CORES)
    outer = jnp.where(z == 1, z - 1, z + 1)

    def source(j):
        j = j + 1
        paired = j <= 2 * near
        dist = jnp.where(paired, (j + 1) // 2, j - near)
        from_left = jnp.where(paired, j % 2 == 1, z > near)
        return jnp.where(from_left, z - dist, z + dist), from_left

    def event(e):
        both = jnp.logical_and(inside, e < 8)
        j = jnp.where(both, e % 2, e // 4)
        m = jnp.where(both, e // 4, (e // 2) % 2)
        p = jnp.where(both, (e // 2) % 2, e % 2)
        single = jnp.logical_and(outside, e < 4)
        return j, jnp.where(single, e % 2, m), jnp.where(single, turn, p)

    def group(g):
        both = jnp.logical_and(inside, g < 4)
        return jnp.where(both, g % 2, g // 2), jnp.where(both, g // 2, g % 2)

    def arrive(e):
        j, m, p = event(e)
        zz, from_left = source(j)
        view = piece_of(m, zz, p)
        got(view, prim_recv.at[m, zz, p])
        on_right = jnp.logical_and(from_left, z < chips - 1)
        on_left = jnp.logical_and(jnp.logical_not(from_left), z > 0)
        pl.when(on_right)(lambda: line(1, m, zz, p))
        pl.when(on_left)(lambda: line(-1, m, zz, p))
        single = jnp.logical_and(outside, e < 4)

        @pl.when(single)
        def _():
            for to in (xs, ys):
                push(view, xy_send, sec_recv.at[m, zz], (to, t))

        whole = jnp.logical_and(inside, zz == outer)

        @pl.when(jnp.logical_not(jnp.logical_or(single, whole)))
        def _():
            for h, to in enumerate((xs, ys)):
                part = part_of(prim, m, zz, p, h)
                push(part, xy_send, sec_recv.at[m, zz], (to, t))

        last = jnp.logical_and(j == chips - 2, m == 1)
        push(view, sib_send, sib_recv.at[jnp.where(last, 2, m), zz], (s, sib))

    def part_of(which, m, zz, p, h):
        return wbuf.at[m, zz, span(which * half + p * step + h * part_rows, part_rows), lanes]

    def arrive_secondary(g):
        j, m = group(g)
        zz, _ = source(j)
        view = wbuf.at[m, zz, span(sec * half, half), lanes]
        got(view, sec_recv.at[m, zz])

        @pl.when(jnp.logical_and(outside, g < 2))
        def _():
            push(part_of(sec, m, zz, 1 - turn, 0), xy_send, relay_recv.at[m], (xs, t))
            push(part_of(sec, m, zz, turn, 1), xy_send, relay_recv.at[m], (ys, t))

        push(view, sib_send, sib_recv.at[m, zz], (s, sib))

    def arrive_relayed(m):
        zz, _ = source(0)
        view = piece_of(m, zz, 1 - turn)
        got(view, relay_recv.at[m])
        push(view, sib_send, sib_recv.at[m, zz], (s, sib))

    def columns_of(zz):
        return pl.ds(pl.multiple_of(zz * wide, wide), wide)

    def product(pair, m, zz, first, width):
        at = pl.ds(2 * pair, 2)
        columns = span(zz * wide + first, width)
        out = jnp.dot(
            xbuf[at].reshape(-1, depth), wbuf[m, zz, :, span(first, width)],
            preferred_element_type=jnp.float32,
        ).astype(jnp.bfloat16)
        kvbuf[m, at, :, columns] = out.reshape(2, rows, width)
        return columns

    def keep(m, columns):
        for i, slot in ((2, s), (3, diag)):
            kv[m, span(slot * rows, rows), columns] = kvbuf[m, i, :, columns]

    def multiply(m, zz):
        got(wbuf.at[m, zz, :, sib_lanes], sib_recv.at[m, zz])

        def body(pair, _):
            product(pair, m, zz, 0, wide)
            return 0

        lax.fori_loop(0, 2, body, 0)
        keep(m, columns_of(zz))

    last_zz = source(chips - 2)[0]

    def halves(pair, which):
        at = span(which * half, half)
        return jnp.dot(
            xbuf[pl.ds(2 * pair, 2), :, at].reshape(-1, half), wbuf[1, last_zz, at, :],
            preferred_element_type=jnp.float32,
        )

    def last_begin():
        got(wbuf.at[1, last_zz, span(prim * half, half), sib_lanes], sib_recv.at[2, last_zz])

        def body(pair, _):
            partial[pair] = halves(pair, prim)
            return 0

        lax.fori_loop(0, 2, body, 0)

    def last_end():
        got(wbuf.at[1, last_zz, span(sec * half, half), sib_lanes], sib_recv.at[1, last_zz])

        def body(pair, _):
            out = (partial[pair] + halves(pair, sec)).astype(jnp.bfloat16)
            kvbuf[1, pl.ds(2 * pair, 2), :, columns_of(last_zz)] = out.reshape(2, rows, wide)
            return 0

        lax.fori_loop(0, 2, body, 0)
        keep(1, columns_of(last_zz))

    def send_columns(m, columns):
        for i, p in enumerate((xs, ys)):
            remote(
                kvbuf.at[m, i, :, columns], kv.at[m, span(s * rows, rows), columns],
                out_send, out_recv, (p, t),
            ).start()

    scale = MAP_HEAD_SIZE ** (-0.5)
    row = lax.broadcasted_iota(jnp.int32, (state_rows, 1), 0)
    row_map = row // (CORES * seq_count)
    row_seq = (row // CORES) % seq_count
    row_head = row % CORES

    def by_seq(new, first):
        values = jnp.zeros((state_rows, new.shape[1]), jnp.float32)
        for b in range(seq_count):
            values = jnp.where(row_seq == b, new[first + b : first + b + 1], values)
        return values

    def by_head(values):
        return functools.reduce(
            jnp.add,
            [jnp.where(row_head == i, values[:, i * VD : (i + 1) * VD], 0.0) for i in range(CORES)],
        )

    def new_rows(zz):
        return jnp.concatenate([qbuf[zz * CORES + i] for i in range(CORES)], axis=1)

    def query_of(new):
        lane = lax.broadcasted_iota(jnp.int32, (state_rows, wide), 1)
        mine = lane // MAP_HEAD_SIZE == row_head * 2 + row_map
        return jnp.where(mine, by_seq(new, 0), 0.0)

    def score(j, zz):
        query = query_of(new_rows(zz)).astype(jnp.bfloat16)
        keys = kvbuf[0, :, :, columns_of(zz)].reshape(-1, wide)
        scores = lax.dot_general(
            query, keys, (((1,), (1,)), ((), ())), preferred_element_type=jnp.float32
        ) * scale
        at = lax.broadcasted_iota(jnp.int32, scores.shape, 1) // rows
        spans = sp_count // seq_count
        owner = jnp.where(at == 0, xs, jnp.where(at == 1, ys, s)) // spans
        mine = owner == row_seq
        peak = jnp.max(jnp.where(mine, scores, far_below), axis=1, keepdims=True)
        raised = jnp.where(mine, jnp.exp(scores - peak), 0.0)
        total = jnp.sum(raised, axis=1, keepdims=True)
        high = raised.astype(jnp.bfloat16)
        low = (raised - high.astype(jnp.float32)).astype(jnp.bfloat16)
        pbuf[j, :state_rows] = high
        pbuf[j, state_rows:] = low
        pstat[j, 0] = jnp.broadcast_to(peak, (state_rows, VD))
        pstat[j, 1] = jnp.broadcast_to(total, (state_rows, VD))

    def weigh(j, zz):
        values = kvbuf[1, :, :, columns_of(zz)].reshape(-1, wide)
        both = jnp.dot(pbuf[j], values, preferred_element_type=jnp.float32)
        return by_head(both[:state_rows] + both[state_rows:]), pstat[j, 0][:, :1], pstat[j, 1][:, :1]

    def send_state(zz):
        view = stbuf.at[z, zz, pl.ds(0, state_rows + 1)]
        for p in z_peers:
            push(view, st_send, st_recv.at[zz], p)

    def send_up(slot, m, zz, recv):
        for i, p in enumerate((xs, ys)):
            remote(kvbuf.at[m, i, :, columns_of(zz)], upbuf.at[slot, i], out_send, recv, (p, inner)).start()

    def pass_down(slot, m, zz):
        for i, p in enumerate((xs, ys)):
            remote(
                upbuf.at[slot, i], kv.at[m, span(p * rows, rows), columns_of(zz)],
                out_send, out_recv, (s, outer * CORES + c),
            ).start()

    mine_at = chips - 1
    loads[2].wait()
    loads[3].wait()
    before = None
    for core in (c, 1 - c):
        for m in range(2):
            if core is not c:
                got(wbuf.at[m, z, :, sib_lanes], sib_recv.at[m, z])
            columns = product(0, m, z, core * cols, cols)
            if before is not None:
                pl.when(inside)(lambda before=before: send_columns(*before))
            before = (m, columns)

    def vectors():
        loads[4].wait()
        loads[5].wait()
        vector = token[...]
        me_q = jnp.dot(vector, wq[...], preferred_element_type=jnp.float32)
        me_k = jnp.dot(vector, wbuf[0, z, :, lanes], preferred_element_type=jnp.float32)
        me_v = jnp.dot(vector, wbuf[1, z, :, lanes], preferred_element_type=jnp.float32)
        for i, value in enumerate((me_q, me_k, me_v)):
            value = value.astype(jnp.bfloat16).astype(jnp.float32)
            qbuf[t, i * seq_count : (i + 1) * seq_count, :] = value[:seq_count]
    def own_block():
        loads[6].wait()
        far_prompt.wait_recv()

        def some(m, _):
            product(1, m, z, 0, wide)
            keep(m, columns_of(z))
            return 0

        lax.fori_loop(0, 2, some, 0)
        score(mine_at, z)
        new = new_rows(z)
        own_score = jnp.sum(query_of(new) * by_seq(new, seq_count), axis=1, keepdims=True) * scale
        holder = jnp.logical_and(s == 0, c == 0)
        own = (
            jnp.where(holder, by_head(by_seq(new, 2 * seq_count)), 0.0),
            jnp.where(holder, own_score, far_below),
            jnp.where(holder, jnp.ones_like(own_score), 0.0),
        )
        pack(stbuf.at[z, z], 0, state_rows, merged([weigh(mine_at, z), own]))

    def compute(g):
        j, m = group(g)
        zz, _ = source(j)
        multiply(m, zz)

        @pl.when(m == 0)
        def _():
            got(qbuf.at[span(zz * CORES, CORES)], pk_recv.at[zz])
            score(j, zz)

        @pl.when(m == 1)
        def _():
            pack(stbuf.at[z, zz], 0, state_rows, weigh(j, zz))

    def results(g):
        j, m = group(g)
        zz, _ = source(j)
        send_columns(m, columns_of(zz))

    def state(g):
        j, m = group(g)
        zz, _ = source(j)
        pl.when(m == 1)(lambda: send_state(zz))

    groups = 2 * (chips - 1)
    def finish(g):
        compute(g)
        results(g)
        state(g)

    own_at = jnp.where(inside, 7, 5)

    def work(e, _):
        arrive(e)

        @pl.when(e == 2)
        def _():
            pl.when(inside)(lambda: send_columns(*before))
            vectors()

        @pl.when(e == 3)
        def _():
            push(qbuf.at[t], pk_send, pk_recv.at[z], (s, sib))

        @pl.when(e == 4)
        def _():
            got(qbuf.at[sib], pk_recv.at[z])
            for p in z_peers:
                push(qbuf.at[span(z * CORES, CORES)], pk_send, pk_recv.at[z], p)

            @pl.when(outside)
            def _():
                for m in range(2):
                    view = wbuf.at[m, z, span(sec * half, half), lanes]
                    push(view, line_send.at[jnp.where(z == 0, 1, 0)], sec_recv.at[m, z], (s, inner))
                for m in range(2):
                    send_up(m, m, z, up_recv.at[0])

        pl.when(e == own_at)(own_block)
        pl.when(e == own_at + 1)(lambda: send_state(z))
        pl.when(outside & (e >= 9) & (e < 11))(lambda: arrive_relayed(e - 9))
        pl.when(outside & (e == 9))(lambda: send_up(2, 0, source(1)[0], up_recv.at[1]))
        ready = jnp.where(inside, e - 9, jnp.where(e < 9, e - 6, e - 7))
        pl.when((ready >= 0) & (inside | (e != 9)))(lambda: arrive_secondary(ready))
        now = jnp.where(inside, e - 10, jnp.where(e == 8, 2, e - 9))
        pl.when(jnp.where(inside, e >= 10, (e >= 8) & (e < 11)))(lambda: compute(now))
        return 0

    events = 2 * groups
    lax.fori_loop(jnp.where(inside, 0, 2), events, work, 0)
    results(0)
    results(1)
    state(1)

    def rest(i, _):
        @pl.when(inside & (i == 2))
        def _():
            got(upbuf.at[pl.ds(0, 2)], up_recv.at[0])
            for m in range(2):
                pass_down(m, m, outer)

        pl.when(inside & (i < 2))(lambda: arrive_secondary(i + 3))
        finish(jnp.where(inside, i + 2, i + 3))
        return 0

    lax.fori_loop(0, jnp.where(inside, 3, 2), rest, 0)

    me = s * CORES + c
    ends = (0, chips - 1)
    middle = tuple(range(1, chips - 1))

    def join_z(k, blocks):
        for i, zz in enumerate(blocks):
            got(stbuf.at[pl.ds(0, chips - 1), zz, pl.ds(0, state_rows + 1)], st_recv.at[zz])
            whole = merged([unpack(stbuf.at[a, zz], 0, state_rows, state_rows) for a in range(chips)])
            pack(finbuf.at[k, me], i * state_rows, len(blocks) * state_rows + i, whole)

    def send_joined(k, blocks):
        view = finbuf.at[k, me, pl.ds(0, len(blocks) * (state_rows + 1))]
        for p in plane_peers + cross_peers + [(s, sib)]:
            push(view, fin_send, fin_recv.at[k], p)

    last_begin()
    arrive_secondary(groups - 1)
    last_end()
    pack(stbuf.at[z, last_zz], 0, state_rows, weigh(chips - 2, last_zz))
    results(groups - 1)
    state(groups - 1)

    @pl.when(inside)
    def _():
        got(upbuf.at[2], up_recv.at[1])
        pass_down(2, 0, 2 * z - outer)

    join_z(0, middle)
    send_joined(0, middle)
    join_z(1, ends)
    send_joined(1, ends)
    others = sp_count * CORES - 1
    fin_rows = pl.ds(0, 2 * (state_rows + 1))
    for k in range(2):
        got(finbuf.at[k, pl.ds(0, others), fin_rows], fin_recv.at[k])

    def pieces_view(count):
        return wbuf.at[:, 0, pl.ds(0, count * step * cols // (2 * wide)), :]

    others_rows = pl.ds(0, 2)
    far_prompt.wait_send()
    got(kvbuf.at[:, others_rows], out_recv)
    for pieces, on in ((11, inside), (8, outside)):
        pl.when(on)(lambda pieces=pieces: gone(pieces_view(pieces), out_send))
    for pieces, on in ((8, inside), (14, outside)):
        pl.when(on)(lambda pieces=pieces: gone(pieces_view(pieces), xy_send))
    gone(wbuf.at[:, :, :, lanes], sib_send)
    gone(qbuf.at[pl.ds(0, tp_count - 1)], pk_send)
    gone(stbuf.at[pl.ds(0, chips - 1), :, pl.ds(0, state_rows + 1)], st_send)
    gone(finbuf.at[:, pl.ds(0, others), fin_rows], fin_send)
    for direction in (-1, 1):
        for pieces, last in ((10, True), (8, False)):
            @pl.when(jnp.logical_and(has_next(direction), to_end(direction) == last))
            def _(direction=direction, pieces=pieces):
                gone(pieces_view(pieces), line_send.at[(direction + 1) // 2])


def store_kernel(
    blocks, kv, finbuf, balance_hbm, gain_hbm, keys_out, values_out, read_out, read, balance, gain, sem
):
    copies = [
        pltpu.make_async_copy(balance_hbm, balance, sem.at[0]),
        pltpu.make_async_copy(gain_hbm, gain, sem.at[1]),
        pltpu.make_async_copy(kv.at[0], keys_out, sem.at[2]),
        pltpu.make_async_copy(kv.at[1], values_out, sem.at[3]),
        pltpu.make_async_copy(read, read_out, sem.at[4]),
    ]
    for a in copies[:4]:
        a.start()
    devices, state_rows = finbuf.shape[1], CORES * 2 * read.shape[0]
    fold = state_rows // 2
    seq_count = read.shape[0]
    heads = {}
    for k, zz_list in enumerate(blocks):
        for i, zz in enumerate(zz_list):
            at, stat_at = i * state_rows, len(zz_list) * state_rows + i
            weighted, _, total = merged(
                [unpack(finbuf.at[k, a], at, stat_at, state_rows) for a in range(devices)]
            )
            heads[zz] = weighted / total
    copies[0].wait()
    copies[1].wait()
    for zz, heads_out in heads.items():
        lane = lax.broadcasted_iota(jnp.int32, (fold, HEADS), 1)
        chosen = lane == zz * CORES + lax.broadcasted_iota(jnp.int32, (fold, HEADS), 0) % CORES
        second = jnp.sum(jnp.where(chosen, balance[...], 0.0), axis=1, keepdims=True)
        blended = heads_out[:fold] - second * heads_out[fold:]
        normed = (
            blended
            * lax.rsqrt(jnp.mean(blended * blended, axis=1, keepdims=True) + norm_eps)
            * gain[...]
        )
        for b in range(seq_count):
            for h in range(CORES):
                r = b * CORES + h
                read[b : b + 1, (zz * CORES + h) * VD : (zz * CORES + h + 1) * VD] = normed[r : r + 1]
    copies[4].start()
    for a in copies[2:]:
        a.wait()


def fused(prompt, new_token, query_proj_matrix, key_weight, value_weight, map_balance, head_gain):
    seq_count, _, span_count, _, piece_rows, width = prompt.shape
    sp_count, tp_count = lax.axis_size("sp"), lax.axis_size("tp")
    cols = key_weight.shape[1]
    slots = seq_count * span_count
    chips = tp_count // CORES
    key_width = cols * tp_count
    block_rows = sp_count * piece_rows
    state_rows = CORES * 2 * seq_count
    any_space = pl.BlockSpec(memory_space=pltpu.HBM)
    vmem = pl.BlockSpec(memory_space=pltpu.VMEM)
    dma = pltpu.SemaphoreType.DMA
    kv, states = pl.pallas_call(
        functools.partial(step_kernel, (sp_count, tp_count, seq_count)),
        out_shape=[
            pltpu.VMEM((2, block_rows, key_width), jnp.bfloat16),
            pltpu.VMEM((2, sp_count * CORES, 2 * state_rows + 8, VD), jnp.float32),
        ],
        in_specs=[any_space] * 5,
        out_specs=[vmem, vmem],
        scratch_shapes=[
            pltpu.VMEM((slots, piece_rows, width), jnp.bfloat16),
            pltpu.VMEM((2, chips, width, CORES * cols), jnp.bfloat16),
            pltpu.VMEM((2, slots, piece_rows, key_width), jnp.bfloat16),
            pltpu.VMEM((3, 2, piece_rows, CORES * cols), jnp.bfloat16),
            pltpu.VMEM((2, 2 * piece_rows, CORES * cols), jnp.float32),
            pltpu.VMEM((width, cols), jnp.bfloat16),
            pltpu.VMEM((seq_count, width), jnp.bfloat16),
            pltpu.VMEM((tp_count, 8, cols), jnp.float32),
            pltpu.VMEM((chips, 2 * state_rows, slots * piece_rows), jnp.bfloat16),
            pltpu.VMEM((chips, 2, state_rows, VD), jnp.float32),
            pltpu.VMEM((chips, chips, 2 * state_rows, VD), jnp.float32),
            dma((7,)), dma(()), dma(()), dma((2,)), dma((2, chips, PIECES)), dma(()), dma((2, chips)), dma((2,)),
            dma(()), dma((3, chips)),
            dma(()), dma(()), dma((2,)), dma(()), dma((chips,)), dma(()), dma((chips,)), dma(()), dma((2,)),
        ],
        compiler_params=pltpu.CompilerParams(
            collective_id=0, has_side_effects=True, vmem_limit_bytes=61 * 1024 * 1024 + 512 * 1024
        ),
    )(
        prompt.reshape(slots, piece_rows, width),
        new_token, query_proj_matrix, key_weight, value_weight,
    )
    blocks = (tuple(range(1, chips - 1)), (0, chips - 1))
    keys, values, read = pl.pallas_call(
        functools.partial(store_kernel, blocks),
        out_shape=[
            jax.ShapeDtypeStruct((block_rows, key_width), jnp.bfloat16),
            jax.ShapeDtypeStruct((block_rows, key_width), jnp.bfloat16),
            jax.ShapeDtypeStruct((seq_count, HEADS * VD), jnp.float32),
        ],
        in_specs=[vmem, vmem, any_space, any_space],
        out_specs=[any_space] * 3,
        scratch_shapes=[
            pltpu.VMEM((seq_count, HEADS * VD), jnp.float32),
            pltpu.VMEM((1, HEADS), jnp.float32),
            pltpu.VMEM((1, VD), jnp.float32),
            dma((5,)),
        ],
        compiler_params=pltpu.CompilerParams(vmem_limit_bytes=1024 * 1024),
    )(kv, states, map_balance[None, :], head_gain[None, :])
    shape = (1, 1, block_rows, key_width)
    return keys.reshape(shape), values.reshape(shape), read


def fits(mesh, key_weight, value_weight, prompt):
    tp_count, sp_count = mesh.shape["tp"], mesh.shape["sp"]
    seq_count, _, span_count = prompt.shape[:3]
    cols = key_weight.shape[1] // tp_count
    return (
        sp_count == 4
        and seq_count * span_count == sp_count
        and tp_count % CORES == 0
        and tp_count == 4 * CORES
        and cols == VD
        and 3 * seq_count <= 8
        and key_weight.shape == value_weight.shape
    )


def solution(mesh):
    in_specs = (
        P(None, "tp", None, "sp", None, None),
        P(),
        P(None, "tp"),
        P(None, "tp"),
        P(None, "tp"),
        P(),
        P(),
    )
    out_specs = (P("sp", "tp", None, None), P("sp", "tp", None, None), P())

    def step(prompt, new_token, query_proj_matrix, key_weight, value_weight, map_balance, head_gain):
        body = fused if fits(mesh, key_weight, value_weight, prompt) else shards
        mapped = jax.shard_map(
            body, mesh=mesh, in_specs=in_specs, out_specs=out_specs, check_vma=False
        )
        return mapped(
            prompt, new_token, query_proj_matrix, key_weight, value_weight, map_balance, head_gain
        )

    return step
```

```python
import functools

import jax
import jax.numpy as jnp
from jax import lax
from jax.experimental import pallas as pl
from jax.experimental.pallas import tpu as pltpu
from jax.sharding import PartitionSpec as P

HEADS = 8
MAP_HEAD_SIZE = 64
VD = 128


norm_eps = 1e-06
far_below = -1e30


def joined(part, axis, combine):
    gathered = jax.tree.map(lambda a: lax.all_gather(a, axis), part)

    def take(source):
        return jax.tree.map(lambda a: lax.dynamic_index_in_dim(a, source, 0, False), gathered)

    return lax.fori_loop(
        1, lax.axis_size(axis), lambda source, state: combine(state, take(source)), take(0)
    )


def fill_cols(source, w_piece):
    product = jnp.dot(source, w_piece, preferred_element_type=jnp.float32).astype(jnp.bfloat16)
    return product


def local_new(new_token, query_proj_matrix, key_weight, value_weight):
    return (
        jnp.dot(new_token, query_proj_matrix, preferred_element_type=jnp.float32).astype(
            jnp.bfloat16
        ),
        jnp.dot(new_token, key_weight, preferred_element_type=jnp.float32).astype(jnp.bfloat16),
        jnp.dot(new_token, value_weight, preferred_element_type=jnp.float32).astype(jnp.bfloat16),
    )


def partial_read(query_matrix_rows, key_rows, value_rows):
    logit_scores = jnp.einsum(
        "bhmd,bjhmd->bhmj", query_matrix_rows, key_rows, preferred_element_type=jnp.float32
    ) * MAP_HEAD_SIZE ** (-0.5)
    peak = jnp.max(logit_scores, axis=-1)
    weights_exp = jnp.exp(logit_scores - peak[..., None])
    totals = jnp.sum(weights_exp, axis=-1)
    weighted = jnp.einsum("bhmj,bjhe->bhme", weights_exp, value_rows.astype(jnp.float32))
    return (peak, totals, weighted)


def combine(first, second):
    peak_a, totals_a, weighted_a = first
    peak_b, totals_b, weighted_b = second
    peak = jnp.maximum(peak_a, peak_b)
    factor_a = jnp.exp(peak_a - peak)
    factor_b = jnp.exp(peak_b - peak)
    return (
        peak,
        totals_a * factor_a + totals_b * factor_b,
        weighted_a * factor_a[..., None] + weighted_b * factor_b[..., None],
    )


def shards(prompt, new_token, query_proj_matrix, key_weight, value_weight, map_balance, head_gain):
    seq_count, _, span_count, _, piece_rows, model_width = prompt.shape
    token_rows = prompt.reshape(seq_count * span_count * piece_rows, model_width)
    tp_count = lax.axis_size("tp")
    key_width = key_weight.shape[1] * tp_count
    value_width = value_weight.shape[1] * tp_count
    key_piece = lax.all_gather(key_weight, "tp", axis=1, tiled=True)
    value_piece = lax.all_gather(value_weight, "tp", axis=1, tiled=True)
    key_rows = fill_cols(token_rows, key_piece)
    value_rows = fill_cols(token_rows, value_piece)
    own_columns = local_new(new_token, query_proj_matrix, key_weight, value_weight)
    queries, new_keys, new_values = (
        lax.all_gather(own_columns[0], "tp", axis=1, tiled=True),
        lax.all_gather(own_columns[1], "tp", axis=1, tiled=True),
        lax.all_gather(own_columns[2], "tp", axis=1, tiled=True),
    )
    slot_count = seq_count * span_count
    cached_keys, cached_values = (
        lax.all_to_all(
            key_rows.reshape(slot_count, piece_rows, key_width),
            "sp",
            split_axis=0,
            concat_axis=1,
            tiled=True,
        ),
        lax.all_to_all(
            value_rows.reshape(slot_count, piece_rows, value_width),
            "sp",
            split_axis=0,
            concat_axis=1,
            tiled=True,
        ),
    )
    block_rows = cached_keys.shape[1]
    key_cache = cached_keys.reshape(1, 1, block_rows, key_width)
    value_cache = cached_values.reshape(1, 1, block_rows, value_width)
    all_queries = queries.reshape(seq_count, HEADS, 2, MAP_HEAD_SIZE)
    own_seq = lax.axis_index("sp") // span_count
    own_query = lax.dynamic_slice_in_dim(all_queries, own_seq, 1, 0)
    peak, totals, weighted = partial_read(
        own_query,
        cached_keys.reshape(1, block_rows, HEADS, 2, MAP_HEAD_SIZE),
        cached_values.reshape(1, block_rows, HEADS, VD),
    )
    chosen = jnp.arange(seq_count) == own_seq
    chosen_rows = chosen[:, None, None]
    spread = (
        jnp.where(chosen_rows, peak, far_below),
        jnp.where(chosen_rows, totals, 0.0),
        jnp.where(chosen_rows[..., None], weighted, 0.0),
    )
    merged = joined(spread, ("sp", "tp"), combine)
    own_keys = new_keys.reshape(seq_count, HEADS, 2, MAP_HEAD_SIZE)
    own_score = jnp.einsum(
        "bhmd,bhmd->bhm", all_queries, own_keys, preferred_element_type=jnp.float32
    ) * MAP_HEAD_SIZE ** (-0.5)
    own_values = new_values.astype(jnp.float32).reshape(seq_count, HEADS, VD)
    own_weighted = jnp.broadcast_to(own_values[:, :, None, :], (seq_count, HEADS, 2, VD))
    own_state = (own_score, jnp.ones_like(own_score), own_weighted)
    _, totals, weighted = combine(merged, own_state)
    heads_out = weighted / totals[..., None]
    blended = heads_out[:, :, 0] - map_balance[None, :, None] * heads_out[:, :, 1]
    normed = (
        blended
        * lax.rsqrt(jnp.mean(blended * blended, axis=-1, keepdims=True) + norm_eps)
        * head_gain
    )
    return (key_cache, value_cache, normed.reshape(seq_count, HEADS * VD))


MESH = pl.DeviceIdType.MESH
CORES = 2
PIECES = 2


def merged(states):
    peak = functools.reduce(jnp.maximum, [a[1] for a in states])
    factors = [jnp.exp(a[1] - peak) for a in states]
    weighted = functools.reduce(jnp.add, [a[0] * f for a, f in zip(states, factors)])
    total = functools.reduce(jnp.add, [a[2] * f for a, f in zip(states, factors)])
    return weighted, peak, total


def pack(ref, at, stat_at, state):
    weighted, peak, total = state
    rows = weighted.shape[0]
    lane = lax.broadcasted_iota(jnp.int32, weighted.shape, 1)
    row = lax.broadcasted_iota(jnp.int32, weighted.shape, 0)
    stats = jnp.where(lane == row, peak, jnp.where(lane == row + rows, total, 0.0))
    ref[at : at + rows] = weighted
    ref[stat_at : stat_at + 1] = jnp.sum(stats, axis=0, keepdims=True)


def unpack(ref, at, stat_at, rows):
    weighted = ref[at : at + rows]
    lane = lax.broadcasted_iota(jnp.int32, weighted.shape, 1)
    row = lax.broadcasted_iota(jnp.int32, weighted.shape, 0)
    stats = ref[stat_at : stat_at + 1]
    peak = jnp.sum(jnp.where(lane == row, stats, 0.0), axis=1, keepdims=True)
    total = jnp.sum(jnp.where(lane == row + rows, stats, 0.0), axis=1, keepdims=True)
    return weighted, peak, total


def step_kernel(
    dims,
    prompt, token_hbm, wq_hbm, wk_hbm, wv_hbm,
    kv, finbuf,
    xbuf, wbuf, kvbuf, upbuf, partial, wq, token, qbuf, pbuf, pstat, stbuf,
    loc, far_send, far_recv, line_send, prim_recv, xy_send, sec_recv, relay_recv, sib_send, sib_recv,
    out_send, out_recv, up_recv, pk_send, pk_recv, st_send, st_recv, fin_send, fin_recv,
):
    sp_count, tp_count, seq_count = dims
    _, _, depth, wide = wbuf.shape
    cols = wide // CORES
    chips = tp_count // CORES
    rows = xbuf.shape[1]
    state_rows = CORES * 2 * seq_count
    s = lax.axis_index("sp")
    t = lax.axis_index("tp")
    z = t // CORES
    c = t % CORES
    sib = z * CORES + (1 - c)
    xs = s + 1 - 2 * (s % 2)
    ys = (s + 2) % 4
    diag = 3 - s
    prim = (s + s // 2) % 2
    sec = 1 - prim
    turn = s // 2
    near = jnp.minimum(z, chips - 1 - z)
    inside = near > 0
    outside = jnp.logical_not(inside)
    half = depth // 2
    step = half // PIECES
    part_rows = step // 2

    def lanes_of(core):
        return pl.ds(pl.multiple_of(core * cols, cols), cols)

    lanes, sib_lanes = lanes_of(c), lanes_of(1 - c)

    loads = [
        pltpu.make_async_copy(wk_hbm, wbuf.at[0, z, :, lanes], loc.at[0]),
        pltpu.make_async_copy(wv_hbm, wbuf.at[1, z, :, lanes], loc.at[1]),
        pltpu.make_async_copy(prompt.at[xs], xbuf.at[0], loc.at[2]),
        pltpu.make_async_copy(prompt.at[ys], xbuf.at[1], loc.at[3]),
        pltpu.make_async_copy(token_hbm, token, loc.at[4]),
        pltpu.make_async_copy(wq_hbm, wq, loc.at[5]),
        pltpu.make_async_copy(prompt.at[s], xbuf.at[2], loc.at[6]),
    ]
    for a in loads:
        a.start()

    z_peers = [(s, (t + d * CORES) % tp_count) for d in range(1, chips)]
    plane_peers = [((s + d) % sp_count, t) for d in range(1, sp_count)]
    cross_peers = [((s + d) % sp_count, sib) for d in range(1, sp_count)]
    barrier = pltpu.get_barrier_semaphore()
    greeted = plane_peers + [(s, sib)]

    def greet(p):
        pl.semaphore_signal(barrier, inc=1, device_id=p, device_id_type=MESH)

    pl.when(z > 0)(lambda: greet((s, t - CORES)))
    pl.when(z < chips - 1)(lambda: greet((s, t + CORES)))
    for p in greeted:
        greet(p)
    pl.semaphore_wait(barrier, len(greeted) + jnp.where(inside, 2, 1))

    def remote(src, dst, send, recv, dev):
        return pltpu.make_async_remote_copy(
            src_ref=src, dst_ref=dst, send_sem=send, recv_sem=recv, device_id=dev, device_id_type=MESH
        )

    def push(view, send, recv, dev):
        remote(view, view, send, recv, dev).start()

    def got(view, recv):
        remote(view, view, xy_send, recv, (s, sib)).wait_recv()

    def gone(view, send):
        remote(view, view, send, loc.at[0], (s, sib)).wait_send()

    def span(start, size):
        return pl.ds(pl.multiple_of(start, size), size)

    def piece_of(m, zz, p):
        return wbuf.at[m, zz, span(prim * half + p * step, step), lanes]

    def line(direction, m, zz, p):
        view = piece_of(m, zz, p)
        push(view, line_send.at[(direction + 1) // 2], prim_recv.at[m, zz, p], (s, t + direction * CORES))

    def has_next(direction):
        return (z > 0) if direction < 0 else (z < chips - 1)

    def to_end(direction):
        return (z == 1) if direction < 0 else (z == chips - 2)

    far_prompt = remote(prompt.at[diag], xbuf.at[3], far_send, far_recv, (diag, t))
    far_prompt.start()
    for m in range(2):
        loads[m].wait()
        for direction in (-1, 1):
            @pl.when(jnp.logical_and(has_next(direction), to_end(direction)))
            def _(direction=direction, m=m):
                line(direction, m, z, turn)

            @pl.when(jnp.logical_and(has_next(direction), jnp.logical_not(to_end(direction))))
            def _(direction=direction, m=m):
                for p in range(PIECES):
                    line(direction, m, z, p)
        push(wbuf.at[m, z, :, lanes], sib_send, sib_recv.at[m, z], (s, sib))
    inner = jnp.where(z == 0, t + CORES, t - CORES)
    outer = jnp.where(z == 1, z - 1, z + 1)

    def source(j):
        j = j + 1
        paired = j <= 2 * near
        dist = jnp.where(paired, (j + 1) // 2, j - near)
        from_left = jnp.where(paired, j % 2 == 1, z > near)
        return jnp.where(from_left, z - dist, z + dist), from_left

    def event(e):
        both = jnp.logical_and(inside, e < 8)
        j = jnp.where(both, e % 2, e // 4)
        m = jnp.where(both, e // 4, (e // 2) % 2)
        p = jnp.where(both, (e // 2) % 2, e % 2)
        single = jnp.logical_and(outside, e < 4)
        return j, jnp.where(single, e % 2, m), jnp.where(single, turn, p)

    def group(g):
        both = jnp.logical_and(inside, g < 4)
        return jnp.where(both, g % 2, g // 2), jnp.where(both, g // 2, g % 2)

    def arrive(e):
        j, m, p = event(e)
        zz, from_left = source(j)
        view = piece_of(m, zz, p)
        got(view, prim_recv.at[m, zz, p])
        on_right = jnp.logical_and(from_left, z < chips - 1)
        on_left = jnp.logical_and(jnp.logical_not(from_left), z > 0)
        pl.when(on_right)(lambda: line(1, m, zz, p))
        pl.when(on_left)(lambda: line(-1, m, zz, p))
        single = jnp.logical_and(outside, e < 4)

        @pl.when(single)
        def _():
            for to in (xs, ys):
                push(view, xy_send, sec_recv.at[m, zz], (to, t))

        whole = jnp.logical_and(inside, zz == outer)

        @pl.when(jnp.logical_not(jnp.logical_or(single, whole)))
        def _():
            for h, to in enumerate((xs, ys)):
                part = part_of(prim, m, zz, p, h)
                push(part, xy_send, sec_recv.at[m, zz], (to, t))

        last = jnp.logical_and(j == chips - 2, m == 1)
        push(view, sib_send, sib_recv.at[jnp.where(last, 2, m), zz], (s, sib))

    def part_of(which, m, zz, p, h):
        return wbuf.at[m, zz, span(which * half + p * step + h * part_rows, part_rows), lanes]

    def arrive_secondary(g):
        j, m = group(g)
        zz, _ = source(j)
        view = wbuf.at[m, zz, span(sec * half, half), lanes]
        got(view, sec_recv.at[m, zz])

        @pl.when(jnp.logical_and(outside, g < 2))
        def _():
            push(part_of(sec, m, zz, 1 - turn, 0), xy_send, relay_recv.at[m], (xs, t))
            push(part_of(sec, m, zz, turn, 1), xy_send, relay_recv.at[m], (ys, t))

        push(view, sib_send, sib_recv.at[m, zz], (s, sib))

    def arrive_relayed(m):
        zz, _ = source(0)
        view = piece_of(m, zz, 1 - turn)
        got(view, relay_recv.at[m])
        push(view, sib_send, sib_recv.at[m, zz], (s, sib))

    def columns_of(zz):
        return pl.ds(pl.multiple_of(zz * wide, wide), wide)

    def product(pair, m, zz, first, width):
        at = pl.ds(2 * pair, 2)
        columns = span(zz * wide + first, width)
        out = jnp.dot(
            xbuf[at].reshape(-1, depth), wbuf[m, zz, :, span(first, width)],
            preferred_element_type=jnp.float32,
        ).astype(jnp.bfloat16)
        kvbuf[m, at, :, columns] = out.reshape(2, rows, width)
        return columns

    def whole_product(m, zz):
        out = jnp.dot(
            xbuf[...].reshape(-1, depth), wbuf[m, zz], preferred_element_type=jnp.float32
        ).astype(jnp.bfloat16)
        kvbuf[m, :, :, columns_of(zz)] = out.reshape(sp_count, rows, wide)

    def keep(m, columns):
        for i, slot in ((2, s), (3, diag)):
            kv[m, span(slot * rows, rows), columns] = kvbuf[m, i, :, columns]

    def multiply(m, zz):
        got(wbuf.at[m, zz, :, sib_lanes], sib_recv.at[m, zz])

        whole_product(m, zz)
        keep(m, columns_of(zz))

    last_zz = source(chips - 2)[0]

    def halves(which):
        at = span(which * half, half)
        return jnp.dot(
            xbuf[:, :, at].reshape(-1, half), wbuf[1, last_zz, at, :], preferred_element_type=jnp.float32
        )

    def last_begin():
        got(wbuf.at[1, last_zz, span(prim * half, half), sib_lanes], sib_recv.at[2, last_zz])
        partial[...] = halves(prim)

    def last_end():
        got(wbuf.at[1, last_zz, span(sec * half, half), sib_lanes], sib_recv.at[1, last_zz])
        out = (partial[...] + halves(sec)).astype(jnp.bfloat16)
        kvbuf[1, :, :, columns_of(last_zz)] = out.reshape(sp_count, rows, wide)
        keep(1, columns_of(last_zz))

    def send_columns(m, columns):
        for i, p in enumerate((xs, ys)):
            remote(
                kvbuf.at[m, i, :, columns], kv.at[m, span(s * rows, rows), columns],
                out_send, out_recv, (p, t),
            ).start()

    scale = MAP_HEAD_SIZE ** (-0.5)
    row = lax.broadcasted_iota(jnp.int32, (state_rows, 1), 0)
    row_map = row // (CORES * seq_count)
    row_seq = (row // CORES) % seq_count
    row_head = row % CORES

    def by_seq(new, first):
        values = jnp.zeros((state_rows, new.shape[1]), jnp.float32)
        for b in range(seq_count):
            values = jnp.where(row_seq == b, new[first + b : first + b + 1], values)
        return values

    def by_head(values):
        return functools.reduce(
            jnp.add,
            [jnp.where(row_head == i, values[:, i * VD : (i + 1) * VD], 0.0) for i in range(CORES)],
        )

    def new_rows(zz):
        return jnp.concatenate([qbuf[zz * CORES + i] for i in range(CORES)], axis=1)

    def query_of(new):
        lane = lax.broadcasted_iota(jnp.int32, (state_rows, wide), 1)
        mine = lane // MAP_HEAD_SIZE == row_head * 2 + row_map
        return jnp.where(mine, by_seq(new, 0), 0.0)

    def score(j, zz):
        query = query_of(new_rows(zz)).astype(jnp.bfloat16)
        keys = kvbuf[0, :, :, columns_of(zz)].reshape(-1, wide)
        scores = lax.dot_general(
            query, keys, (((1,), (1,)), ((), ())), preferred_element_type=jnp.float32
        ) * scale
        at = lax.broadcasted_iota(jnp.int32, scores.shape, 1) // rows
        spans = sp_count // seq_count
        owner = jnp.where(at == 0, xs, jnp.where(at == 1, ys, s)) // spans
        mine = owner == row_seq
        peak = jnp.max(jnp.where(mine, scores, far_below), axis=1, keepdims=True)
        raised = jnp.where(mine, jnp.exp(scores - peak), 0.0)
        total = jnp.sum(raised, axis=1, keepdims=True)
        high = raised.astype(jnp.bfloat16)
        low = (raised - high.astype(jnp.float32)).astype(jnp.bfloat16)
        pbuf[j, :state_rows] = high
        pbuf[j, state_rows:] = low
        pstat[j, 0] = jnp.broadcast_to(peak, (state_rows, VD))
        pstat[j, 1] = jnp.broadcast_to(total, (state_rows, VD))

    def weigh(j, zz):
        values = kvbuf[1, :, :, columns_of(zz)].reshape(-1, wide)
        both = jnp.dot(pbuf[j], values, preferred_element_type=jnp.float32)
        return by_head(both[:state_rows] + both[state_rows:]), pstat[j, 0][:, :1], pstat[j, 1][:, :1]

    def send_state(zz):
        view = stbuf.at[z, zz, pl.ds(0, state_rows + 1)]
        for p in z_peers:
            push(view, st_send, st_recv.at[zz], p)

    def send_up(slot, m, zz, recv):
        for i, p in enumerate((xs, ys)):
            remote(kvbuf.at[m, i, :, columns_of(zz)], upbuf.at[slot, i], out_send, recv, (p, inner)).start()

    def pass_down(slot, m, zz):
        for i, p in enumerate((xs, ys)):
            remote(
                upbuf.at[slot, i], kv.at[m, span(p * rows, rows), columns_of(zz)],
                out_send, out_recv, (s, outer * CORES + c),
            ).start()

    mine_at = chips - 1
    loads[2].wait()
    loads[3].wait()
    before = None
    for core in (c, 1 - c):
        for m in range(2):
            if core is not c:
                got(wbuf.at[m, z, :, sib_lanes], sib_recv.at[m, z])
            columns = product(0, m, z, core * cols, cols)
            if before is not None:
                pl.when(inside)(lambda before=before: send_columns(*before))
            before = (m, columns)

    def vectors():
        loads[4].wait()
        loads[5].wait()
        vector = token[...]
        me_q = jnp.dot(vector, wq[...], preferred_element_type=jnp.float32)
        me_k = jnp.dot(vector, wbuf[0, z, :, lanes], preferred_element_type=jnp.float32)
        me_v = jnp.dot(vector, wbuf[1, z, :, lanes], preferred_element_type=jnp.float32)
        for i, value in enumerate((me_q, me_k, me_v)):
            value = value.astype(jnp.bfloat16).astype(jnp.float32)
            qbuf[t, i * seq_count : (i + 1) * seq_count, :] = value[:seq_count]
    def own_block():
        loads[6].wait()
        far_prompt.wait_recv()

        def some(m, _):
            product(1, m, z, 0, wide)
            keep(m, columns_of(z))
            return 0

        lax.fori_loop(0, 2, some, 0)
        score(mine_at, z)
        new = new_rows(z)
        own_score = jnp.sum(query_of(new) * by_seq(new, seq_count), axis=1, keepdims=True) * scale
        holder = jnp.logical_and(s == 0, c == 0)
        own = (
            jnp.where(holder, by_head(by_seq(new, 2 * seq_count)), 0.0),
            jnp.where(holder, own_score, far_below),
            jnp.where(holder, jnp.ones_like(own_score), 0.0),
        )
        pack(stbuf.at[z, z], 0, state_rows, merged([weigh(mine_at, z), own]))

    def compute(g):
        j, m = group(g)
        zz, _ = source(j)
        multiply(m, zz)

        @pl.when(m == 0)
        def _():
            got(qbuf.at[span(zz * CORES, CORES)], pk_recv.at[zz])
            score(j, zz)

        @pl.when(m == 1)
        def _():
            pack(stbuf.at[z, zz], 0, state_rows, weigh(j, zz))

    def results(g):
        j, m = group(g)
        zz, _ = source(j)
        send_columns(m, columns_of(zz))

    def state(g):
        j, m = group(g)
        zz, _ = source(j)
        pl.when(m == 1)(lambda: send_state(zz))

    groups = 2 * (chips - 1)
    def finish(g):
        compute(g)
        results(g)
        state(g)

    own_at = jnp.where(inside, 7, 5)

    def work(e, _):
        arrive(e)

        @pl.when(e == 2)
        def _():
            pl.when(inside)(lambda: send_columns(*before))
            vectors()

        @pl.when(e == 3)
        def _():
            push(qbuf.at[t], pk_send, pk_recv.at[z], (s, sib))

        @pl.when(e == 4)
        def _():
            got(qbuf.at[sib], pk_recv.at[z])
            for p in z_peers:
                push(qbuf.at[span(z * CORES, CORES)], pk_send, pk_recv.at[z], p)

            @pl.when(outside)
            def _():
                for m in range(2):
                    view = wbuf.at[m, z, span(sec * half, half), lanes]
                    push(view, line_send.at[jnp.where(z == 0, 1, 0)], sec_recv.at[m, z], (s, inner))
                for m in range(2):
                    send_up(m, m, z, up_recv.at[0])

        pl.when(e == own_at)(own_block)
        pl.when(e == own_at + 1)(lambda: send_state(z))
        pl.when(outside & (e >= 9) & (e < 11))(lambda: arrive_relayed(e - 9))
        pl.when(outside & (e == 9))(lambda: send_up(2, 0, source(1)[0], up_recv.at[1]))
        ready = jnp.where(inside, e - 9, jnp.where(e < 9, e - 6, e - 7))
        pl.when((ready >= 0) & (inside | (e != 9)))(lambda: arrive_secondary(ready))
        now = jnp.where(inside, e - 10, jnp.where(e == 8, 2, e - 9))
        pl.when(jnp.where(inside, e >= 10, (e == 8) | (e == 9)))(lambda: compute(now))
        return 0

    events = 2 * groups
    lax.fori_loop(jnp.where(inside, 0, 2), events, work, 0)
    results(0)
    pl.when(inside)(lambda: results(1))

    def rest(i, _):
        @pl.when(inside & (i == 2))
        def _():
            got(upbuf.at[pl.ds(0, 2)], up_recv.at[0])
            for m in range(2):
                pass_down(m, m, outer)

        pl.when(inside & (i < 2))(lambda: arrive_secondary(i + 3))

        @pl.when(i == 2)
        def _():
            last_begin()
            arrive_secondary(groups - 1)

        finish(jnp.where(outside & (i == 0), 1, i + 2))
        return 0

    lax.fori_loop(0, 3, rest, 0)

    me = s * CORES + c
    ends = (0, chips - 1)
    middle = tuple(range(1, chips - 1))

    def join_z(k, blocks):
        for i, zz in enumerate(blocks):
            got(stbuf.at[pl.ds(0, chips - 1), zz, pl.ds(0, state_rows + 1)], st_recv.at[zz])
            whole = merged([unpack(stbuf.at[a, zz], 0, state_rows, state_rows) for a in range(chips)])
            pack(finbuf.at[k, me], i * state_rows, len(blocks) * state_rows + i, whole)

    def send_joined(k, blocks):
        view = finbuf.at[k, me, pl.ds(0, len(blocks) * (state_rows + 1))]
        for p in plane_peers + cross_peers + [(s, sib)]:
            push(view, fin_send, fin_recv.at[k], p)

    last_end()
    pack(stbuf.at[z, last_zz], 0, state_rows, weigh(chips - 2, last_zz))
    results(groups - 1)
    state(groups - 1)

    @pl.when(inside)
    def _():
        got(upbuf.at[2], up_recv.at[1])
        pass_down(2, 0, 2 * z - outer)

    join_z(0, middle)
    send_joined(0, middle)
    join_z(1, ends)
    send_joined(1, ends)
    others = sp_count * CORES - 1
    fin_rows = pl.ds(0, 2 * (state_rows + 1))
    for k in range(2):
        got(finbuf.at[k, pl.ds(0, others), fin_rows], fin_recv.at[k])

    def pieces_view(count):
        return wbuf.at[:, 0, pl.ds(0, count * step * cols // (2 * wide)), :]

    others_rows = pl.ds(0, 2)
    far_prompt.wait_send()
    got(kvbuf.at[:, others_rows], out_recv)
    for pieces, on in ((11, inside), (8, outside)):
        pl.when(on)(lambda pieces=pieces: gone(pieces_view(pieces), out_send))
    for pieces, on in ((8, inside), (14, outside)):
        pl.when(on)(lambda pieces=pieces: gone(pieces_view(pieces), xy_send))
    gone(wbuf.at[:, :, :, lanes], sib_send)
    gone(qbuf.at[pl.ds(0, tp_count - 1)], pk_send)
    gone(stbuf.at[pl.ds(0, chips - 1), :, pl.ds(0, state_rows + 1)], st_send)
    gone(finbuf.at[:, pl.ds(0, others), fin_rows], fin_send)
    for direction in (-1, 1):
        for pieces, last in ((10, True), (8, False)):
            @pl.when(jnp.logical_and(has_next(direction), to_end(direction) == last))
            def _(direction=direction, pieces=pieces):
                gone(pieces_view(pieces), line_send.at[(direction + 1) // 2])


def store_kernel(
    blocks, kv, finbuf, balance_hbm, gain_hbm, keys_out, values_out, read_out, read, balance, gain, sem
):
    copies = [
        pltpu.make_async_copy(balance_hbm, balance, sem.at[0]),
        pltpu.make_async_copy(gain_hbm, gain, sem.at[1]),
        pltpu.make_async_copy(kv.at[0], keys_out, sem.at[2]),
        pltpu.make_async_copy(kv.at[1], values_out, sem.at[3]),
        pltpu.make_async_copy(read, read_out, sem.at[4]),
    ]
    for a in copies[:4]:
        a.start()
    devices, state_rows = finbuf.shape[1], CORES * 2 * read.shape[0]
    fold = state_rows // 2
    seq_count = read.shape[0]
    heads = {}
    for k, zz_list in enumerate(blocks):
        for i, zz in enumerate(zz_list):
            at, stat_at = i * state_rows, len(zz_list) * state_rows + i
            weighted, _, total = merged(
                [unpack(finbuf.at[k, a], at, stat_at, state_rows) for a in range(devices)]
            )
            heads[zz] = weighted / total
    copies[0].wait()
    copies[1].wait()
    for zz, heads_out in heads.items():
        lane = lax.broadcasted_iota(jnp.int32, (fold, HEADS), 1)
        chosen = lane == zz * CORES + lax.broadcasted_iota(jnp.int32, (fold, HEADS), 0) % CORES
        second = jnp.sum(jnp.where(chosen, balance[...], 0.0), axis=1, keepdims=True)
        blended = heads_out[:fold] - second * heads_out[fold:]
        normed = (
            blended
            * lax.rsqrt(jnp.mean(blended * blended, axis=1, keepdims=True) + norm_eps)
            * gain[...]
        )
        for b in range(seq_count):
            for h in range(CORES):
                r = b * CORES + h
                read[b : b + 1, (zz * CORES + h) * VD : (zz * CORES + h + 1) * VD] = normed[r : r + 1]
    copies[4].start()
    for a in copies[2:]:
        a.wait()


def fused(prompt, new_token, query_proj_matrix, key_weight, value_weight, map_balance, head_gain):
    seq_count, _, span_count, _, piece_rows, width = prompt.shape
    sp_count, tp_count = lax.axis_size("sp"), lax.axis_size("tp")
    cols = key_weight.shape[1]
    slots = seq_count * span_count
    chips = tp_count // CORES
    key_width = cols * tp_count
    block_rows = sp_count * piece_rows
    state_rows = CORES * 2 * seq_count
    any_space = pl.BlockSpec(memory_space=pltpu.HBM)
    vmem = pl.BlockSpec(memory_space=pltpu.VMEM)
    dma = pltpu.SemaphoreType.DMA
    kv, states = pl.pallas_call(
        functools.partial(step_kernel, (sp_count, tp_count, seq_count)),
        out_shape=[
            pltpu.VMEM((2, block_rows, key_width), jnp.bfloat16),
            pltpu.VMEM((2, sp_count * CORES, 2 * state_rows + 8, VD), jnp.float32),
        ],
        in_specs=[any_space] * 5,
        out_specs=[vmem, vmem],
        scratch_shapes=[
            pltpu.VMEM((slots, piece_rows, width), jnp.bfloat16),
            pltpu.VMEM((2, chips, width, CORES * cols), jnp.bfloat16),
            pltpu.VMEM((2, slots, piece_rows, key_width), jnp.bfloat16),
            pltpu.VMEM((3, 2, piece_rows, CORES * cols), jnp.bfloat16),
            pltpu.VMEM((slots * piece_rows, CORES * cols), jnp.float32),
            pltpu.VMEM((width, cols), jnp.bfloat16),
            pltpu.VMEM((seq_count, width), jnp.bfloat16),
            pltpu.VMEM((tp_count, 8, cols), jnp.float32),
            pltpu.VMEM((chips, 2 * state_rows, slots * piece_rows), jnp.bfloat16),
            pltpu.VMEM((chips, 2, state_rows, VD), jnp.float32),
            pltpu.VMEM((chips, chips, 2 * state_rows, VD), jnp.float32),
            dma((7,)), dma(()), dma(()), dma((2,)), dma((2, chips, PIECES)), dma(()), dma((2, chips)), dma((2,)),
            dma(()), dma((3, chips)),
            dma(()), dma(()), dma((2,)), dma(()), dma((chips,)), dma(()), dma((chips,)), dma(()), dma((2,)),
        ],
        compiler_params=pltpu.CompilerParams(
            collective_id=0, has_side_effects=True, vmem_limit_bytes=61 * 1024 * 1024 + 512 * 1024
        ),
    )(
        prompt.reshape(slots, piece_rows, width),
        new_token, query_proj_matrix, key_weight, value_weight,
    )
    blocks = (tuple(range(1, chips - 1)), (0, chips - 1))
    keys, values, read = pl.pallas_call(
        functools.partial(store_kernel, blocks),
        out_shape=[
            jax.ShapeDtypeStruct((block_rows, key_width), jnp.bfloat16),
            jax.ShapeDtypeStruct((block_rows, key_width), jnp.bfloat16),
            jax.ShapeDtypeStruct((seq_count, HEADS * VD), jnp.float32),
        ],
        in_specs=[vmem, vmem, any_space, any_space],
        out_specs=[any_space] * 3,
        scratch_shapes=[
            pltpu.VMEM((seq_count, HEADS * VD), jnp.float32),
            pltpu.VMEM((1, HEADS), jnp.float32),
            pltpu.VMEM((1, VD), jnp.float32),
            dma((5,)),
        ],
        compiler_params=pltpu.CompilerParams(vmem_limit_bytes=1024 * 1024),
    )(kv, states, map_balance[None, :], head_gain[None, :])
    shape = (1, 1, block_rows, key_width)
    return keys.reshape(shape), values.reshape(shape), read


def fits(mesh, key_weight, value_weight, prompt):
    tp_count, sp_count = mesh.shape["tp"], mesh.shape["sp"]
    seq_count, _, span_count = prompt.shape[:3]
    cols = key_weight.shape[1] // tp_count
    return (
        sp_count == 4
        and seq_count * span_count == sp_count
        and tp_count % CORES == 0
        and tp_count == 4 * CORES
        and cols == VD
        and 3 * seq_count <= 8
        and key_weight.shape == value_weight.shape
    )


def solution(mesh):
    in_specs = (
        P(None, "tp", None, "sp", None, None),
        P(),
        P(None, "tp"),
        P(None, "tp"),
        P(None, "tp"),
        P(),
        P(),
    )
    out_specs = (P("sp", "tp", None, None), P("sp", "tp", None, None), P())

    def step(prompt, new_token, query_proj_matrix, key_weight, value_weight, map_balance, head_gain):
        body = fused if fits(mesh, key_weight, value_weight, prompt) else shards
        mapped = jax.shard_map(
            body, mesh=mesh, in_specs=in_specs, out_specs=out_specs, check_vma=False
        )
        return mapped(
            prompt, new_token, query_proj_matrix, key_weight, value_weight, map_balance, head_gain
        )

    return step
```

```python
import functools

import jax
import jax.numpy as jnp
from jax import lax
from jax.experimental import pallas as pl
from jax.experimental.pallas import tpu as pltpu
from jax.sharding import PartitionSpec as P

HEADS = 8
MAP_HEAD_SIZE = 64
VD = 128


norm_eps = 1e-06
far_below = -1e30


def joined(part, axis, combine):
    gathered = jax.tree.map(lambda a: lax.all_gather(a, axis), part)

    def take(source):
        return jax.tree.map(lambda a: lax.dynamic_index_in_dim(a, source, 0, False), gathered)

    return lax.fori_loop(
        1, lax.axis_size(axis), lambda source, state: combine(state, take(source)), take(0)
    )


def fill_cols(source, w_piece):
    product = jnp.dot(source, w_piece, preferred_element_type=jnp.float32).astype(jnp.bfloat16)
    return product


def local_new(new_token, query_proj_matrix, key_weight, value_weight):
    return (
        jnp.dot(new_token, query_proj_matrix, preferred_element_type=jnp.float32).astype(
            jnp.bfloat16
        ),
        jnp.dot(new_token, key_weight, preferred_element_type=jnp.float32).astype(jnp.bfloat16),
        jnp.dot(new_token, value_weight, preferred_element_type=jnp.float32).astype(jnp.bfloat16),
    )


def partial_read(query_matrix_rows, key_rows, value_rows):
    logit_scores = jnp.einsum(
        "bhmd,bjhmd->bhmj", query_matrix_rows, key_rows, preferred_element_type=jnp.float32
    ) * MAP_HEAD_SIZE ** (-0.5)
    peak = jnp.max(logit_scores, axis=-1)
    weights_exp = jnp.exp(logit_scores - peak[..., None])
    totals = jnp.sum(weights_exp, axis=-1)
    weighted = jnp.einsum("bhmj,bjhe->bhme", weights_exp, value_rows.astype(jnp.float32))
    return (peak, totals, weighted)


def combine(first, second):
    peak_a, totals_a, weighted_a = first
    peak_b, totals_b, weighted_b = second
    peak = jnp.maximum(peak_a, peak_b)
    factor_a = jnp.exp(peak_a - peak)
    factor_b = jnp.exp(peak_b - peak)
    return (
        peak,
        totals_a * factor_a + totals_b * factor_b,
        weighted_a * factor_a[..., None] + weighted_b * factor_b[..., None],
    )


def shards(prompt, new_token, query_proj_matrix, key_weight, value_weight, map_balance, head_gain):
    seq_count, _, span_count, _, piece_rows, model_width = prompt.shape
    token_rows = prompt.reshape(seq_count * span_count * piece_rows, model_width)
    tp_count = lax.axis_size("tp")
    key_width = key_weight.shape[1] * tp_count
    value_width = value_weight.shape[1] * tp_count
    key_piece = lax.all_gather(key_weight, "tp", axis=1, tiled=True)
    value_piece = lax.all_gather(value_weight, "tp", axis=1, tiled=True)
    key_rows = fill_cols(token_rows, key_piece)
    value_rows = fill_cols(token_rows, value_piece)
    own_columns = local_new(new_token, query_proj_matrix, key_weight, value_weight)
    queries, new_keys, new_values = (
        lax.all_gather(own_columns[0], "tp", axis=1, tiled=True),
        lax.all_gather(own_columns[1], "tp", axis=1, tiled=True),
        lax.all_gather(own_columns[2], "tp", axis=1, tiled=True),
    )
    slot_count = seq_count * span_count
    cached_keys, cached_values = (
        lax.all_to_all(
            key_rows.reshape(slot_count, piece_rows, key_width),
            "sp",
            split_axis=0,
            concat_axis=1,
            tiled=True,
        ),
        lax.all_to_all(
            value_rows.reshape(slot_count, piece_rows, value_width),
            "sp",
            split_axis=0,
            concat_axis=1,
            tiled=True,
        ),
    )
    block_rows = cached_keys.shape[1]
    key_cache = cached_keys.reshape(1, 1, block_rows, key_width)
    value_cache = cached_values.reshape(1, 1, block_rows, value_width)
    all_queries = queries.reshape(seq_count, HEADS, 2, MAP_HEAD_SIZE)
    own_seq = lax.axis_index("sp") // span_count
    own_query = lax.dynamic_slice_in_dim(all_queries, own_seq, 1, 0)
    peak, totals, weighted = partial_read(
        own_query,
        cached_keys.reshape(1, block_rows, HEADS, 2, MAP_HEAD_SIZE),
        cached_values.reshape(1, block_rows, HEADS, VD),
    )
    chosen = jnp.arange(seq_count) == own_seq
    chosen_rows = chosen[:, None, None]
    spread = (
        jnp.where(chosen_rows, peak, far_below),
        jnp.where(chosen_rows, totals, 0.0),
        jnp.where(chosen_rows[..., None], weighted, 0.0),
    )
    merged = joined(spread, ("sp", "tp"), combine)
    own_keys = new_keys.reshape(seq_count, HEADS, 2, MAP_HEAD_SIZE)
    own_score = jnp.einsum(
        "bhmd,bhmd->bhm", all_queries, own_keys, preferred_element_type=jnp.float32
    ) * MAP_HEAD_SIZE ** (-0.5)
    own_values = new_values.astype(jnp.float32).reshape(seq_count, HEADS, VD)
    own_weighted = jnp.broadcast_to(own_values[:, :, None, :], (seq_count, HEADS, 2, VD))
    own_state = (own_score, jnp.ones_like(own_score), own_weighted)
    _, totals, weighted = combine(merged, own_state)
    heads_out = weighted / totals[..., None]
    blended = heads_out[:, :, 0] - map_balance[None, :, None] * heads_out[:, :, 1]
    normed = (
        blended
        * lax.rsqrt(jnp.mean(blended * blended, axis=-1, keepdims=True) + norm_eps)
        * head_gain
    )
    return (key_cache, value_cache, normed.reshape(seq_count, HEADS * VD))


MESH = pl.DeviceIdType.MESH
CORES = 2
PIECES = 2


def merged(states):
    peak = functools.reduce(jnp.maximum, [a[1] for a in states])
    factors = [jnp.exp(a[1] - peak) for a in states]
    weighted = functools.reduce(jnp.add, [a[0] * f for a, f in zip(states, factors)])
    total = functools.reduce(jnp.add, [a[2] * f for a, f in zip(states, factors)])
    return weighted, peak, total


def pack(ref, at, stat_at, state):
    weighted, peak, total = state
    rows = weighted.shape[0]
    lane = lax.broadcasted_iota(jnp.int32, weighted.shape, 1)
    row = lax.broadcasted_iota(jnp.int32, weighted.shape, 0)
    stats = jnp.where(lane == row, peak, jnp.where(lane == row + rows, total, 0.0))
    ref[at : at + rows] = weighted
    ref[stat_at : stat_at + 1] = jnp.sum(stats, axis=0, keepdims=True)


def unpack(ref, at, stat_at, rows):
    weighted = ref[at : at + rows]
    lane = lax.broadcasted_iota(jnp.int32, weighted.shape, 1)
    row = lax.broadcasted_iota(jnp.int32, weighted.shape, 0)
    stats = ref[stat_at : stat_at + 1]
    peak = jnp.sum(jnp.where(lane == row, stats, 0.0), axis=1, keepdims=True)
    total = jnp.sum(jnp.where(lane == row + rows, stats, 0.0), axis=1, keepdims=True)
    return weighted, peak, total


def step_kernel(
    dims,
    prompt, token_hbm, wq_hbm, wk_hbm, wv_hbm,
    kv, finbuf,
    xbuf, wbuf, kvbuf, upbuf, partial, wq, token, qbuf, pbuf, pstat, stbuf,
    loc, far_send, far_recv, line_send, prim_recv, xy_send, sec_recv, relay_recv, sib_send, sib_recv,
    out_send, out_recv, up_recv, pk_send, pk_recv, st_send, st_recv, fin_send, fin_recv,
):
    sp_count, tp_count, seq_count = dims
    _, _, depth, wide = wbuf.shape
    cols = wide // CORES
    chips = tp_count // CORES
    rows = xbuf.shape[1]
    state_rows = CORES * 2 * seq_count
    s = lax.axis_index("sp")
    t = lax.axis_index("tp")
    z = t // CORES
    c = t % CORES
    sib = z * CORES + (1 - c)
    xs = s + 1 - 2 * (s % 2)
    ys = (s + 2) % 4
    diag = 3 - s
    prim = (s + s // 2) % 2
    sec = 1 - prim
    turn = s // 2
    near = jnp.minimum(z, chips - 1 - z)
    inside = near > 0
    outside = jnp.logical_not(inside)
    half = depth // 2
    step = half // PIECES
    part_rows = step // 2

    def lanes_of(core):
        return pl.ds(pl.multiple_of(core * cols, cols), cols)

    lanes, sib_lanes = lanes_of(c), lanes_of(1 - c)

    loads = [
        pltpu.make_async_copy(wk_hbm, wbuf.at[0, z, :, lanes], loc.at[0]),
        pltpu.make_async_copy(wv_hbm, wbuf.at[1, z, :, lanes], loc.at[1]),
        pltpu.make_async_copy(prompt.at[xs], xbuf.at[0], loc.at[2]),
        pltpu.make_async_copy(prompt.at[ys], xbuf.at[1], loc.at[3]),
        pltpu.make_async_copy(token_hbm, token, loc.at[4]),
        pltpu.make_async_copy(wq_hbm, wq, loc.at[5]),
        pltpu.make_async_copy(prompt.at[s], xbuf.at[2], loc.at[6]),
    ]
    for a in loads:
        a.start()

    z_peers = [(s, (t + d * CORES) % tp_count) for d in range(1, chips)]
    plane_peers = [((s + d) % sp_count, t) for d in range(1, sp_count)]
    cross_peers = [((s + d) % sp_count, sib) for d in range(1, sp_count)]
    barrier = pltpu.get_barrier_semaphore()
    greeted = plane_peers + [(s, sib)]

    def greet(p):
        pl.semaphore_signal(barrier, inc=1, device_id=p, device_id_type=MESH)

    pl.when(z > 0)(lambda: greet((s, t - CORES)))
    pl.when(z < chips - 1)(lambda: greet((s, t + CORES)))
    for p in greeted:
        greet(p)
    pl.semaphore_wait(barrier, len(greeted) + jnp.where(inside, 2, 1))

    def remote(src, dst, send, recv, dev):
        return pltpu.make_async_remote_copy(
            src_ref=src, dst_ref=dst, send_sem=send, recv_sem=recv, device_id=dev, device_id_type=MESH
        )

    def push(view, send, recv, dev):
        remote(view, view, send, recv, dev).start()

    def got(view, recv):
        remote(view, view, xy_send, recv, (s, sib)).wait_recv()

    def gone(view, send):
        remote(view, view, send, loc.at[0], (s, sib)).wait_send()

    def span(start, size):
        return pl.ds(pl.multiple_of(start, size), size)

    def piece_of(m, zz, p):
        return wbuf.at[m, zz, span(prim * half + p * step, step), lanes]

    def line(direction, m, zz, p):
        view = piece_of(m, zz, p)
        push(view, line_send.at[(direction + 1) // 2], prim_recv.at[m, zz, p], (s, t + direction * CORES))

    def has_next(direction):
        return (z > 0) if direction < 0 else (z < chips - 1)

    def to_end(direction):
        return (z == 1) if direction < 0 else (z == chips - 2)

    far_prompt = remote(prompt.at[diag], xbuf.at[3], far_send, far_recv, (diag, t))
    far_prompt.start()
    for m in range(2):
        loads[m].wait()
        for direction in (-1, 1):
            @pl.when(jnp.logical_and(has_next(direction), to_end(direction)))
            def _(direction=direction, m=m):
                line(direction, m, z, turn)

            @pl.when(jnp.logical_and(has_next(direction), jnp.logical_not(to_end(direction))))
            def _(direction=direction, m=m):
                for p in range(PIECES):
                    line(direction, m, z, p)
        push(wbuf.at[m, z, :, lanes], sib_send, sib_recv.at[m, z], (s, sib))
    inner = jnp.where(z == 0, t + CORES, t - CORES)
    outer = jnp.where(z == 1, z - 1, z + 1)

    def source(j):
        j = j + 1
        paired = j <= 2 * near
        dist = jnp.where(paired, (j + 1) // 2, j - near)
        from_left = jnp.where(paired, j % 2 == 1, z > near)
        return jnp.where(from_left, z - dist, z + dist), from_left

    def event(e):
        both = jnp.logical_and(inside, e < 8)
        j = jnp.where(both, e % 2, e // 4)
        m = jnp.where(both, e // 4, (e // 2) % 2)
        p = jnp.where(both, (e // 2) % 2, e % 2)
        single = jnp.logical_and(outside, e < 4)
        return j, jnp.where(single, e % 2, m), jnp.where(single, turn, p)

    def group(g):
        both = jnp.logical_and(inside, g < 4)
        return jnp.where(both, g % 2, g // 2), jnp.where(both, g // 2, g % 2)

    def arrive(e):
        j, m, p = event(e)
        zz, from_left = source(j)
        view = piece_of(m, zz, p)
        got(view, prim_recv.at[m, zz, p])
        on_right = jnp.logical_and(from_left, z < chips - 1)
        on_left = jnp.logical_and(jnp.logical_not(from_left), z > 0)
        pl.when(on_right)(lambda: line(1, m, zz, p))
        pl.when(on_left)(lambda: line(-1, m, zz, p))
        single = jnp.logical_and(outside, e < 4)

        @pl.when(single)
        def _():
            for to in (xs, ys):
                push(view, xy_send, sec_recv.at[m, zz], (to, t))

        whole = jnp.logical_and(inside, zz == outer)

        @pl.when(jnp.logical_not(jnp.logical_or(single, whole)))
        def _():
            for h, to in enumerate((xs, ys)):
                part = part_of(prim, m, zz, p, h)
                push(part, xy_send, sec_recv.at[m, zz], (to, t))

        last = jnp.logical_and(j == chips - 2, m == 1)
        push(view, sib_send, sib_recv.at[jnp.where(last, 2, m), zz], (s, sib))

    def part_of(which, m, zz, p, h):
        return wbuf.at[m, zz, span(which * half + p * step + h * part_rows, part_rows), lanes]

    def arrive_secondary(g):
        j, m = group(g)
        zz, _ = source(j)
        view = wbuf.at[m, zz, span(sec * half, half), lanes]
        got(view, sec_recv.at[m, zz])

        @pl.when(jnp.logical_and(outside, g < 2))
        def _():
            push(part_of(sec, m, zz, 1 - turn, 0), xy_send, relay_recv.at[m], (xs, t))
            push(part_of(sec, m, zz, turn, 1), xy_send, relay_recv.at[m], (ys, t))

        push(view, sib_send, sib_recv.at[m, zz], (s, sib))

    def arrive_relayed(m):
        zz, _ = source(0)
        view = piece_of(m, zz, 1 - turn)
        got(view, relay_recv.at[m])
        push(view, sib_send, sib_recv.at[m, zz], (s, sib))

    def columns_of(zz):
        return pl.ds(pl.multiple_of(zz * wide, wide), wide)

    def product(pair, m, zz, first, width):
        at = pl.ds(2 * pair, 2)
        columns = span(zz * wide + first, width)
        out = jnp.dot(
            xbuf[at].reshape(-1, depth), wbuf[m, zz, :, span(first, width)],
            preferred_element_type=jnp.float32,
        ).astype(jnp.bfloat16)
        kvbuf[m, at, :, columns] = out.reshape(2, rows, width)
        return columns

    def whole_product(m, zz):
        out = jnp.dot(
            xbuf[...].reshape(-1, depth), wbuf[m, zz], preferred_element_type=jnp.float32
        ).astype(jnp.bfloat16)
        kvbuf[m, :, :, columns_of(zz)] = out.reshape(sp_count, rows, wide)

    def keep(m, columns):
        for i, slot in ((2, s), (3, diag)):
            kv[m, span(slot * rows, rows), columns] = kvbuf[m, i, :, columns]

    def multiply(m, zz):
        got(wbuf.at[m, zz, :, sib_lanes], sib_recv.at[m, zz])

        whole_product(m, zz)
        keep(m, columns_of(zz))

    last_zz = source(chips - 2)[0]

    def halves(which):
        at = span(which * half, half)
        return jnp.dot(
            xbuf[:, :, at].reshape(-1, half), wbuf[1, last_zz, at, :], preferred_element_type=jnp.float32
        )

    def last_begin():
        got(wbuf.at[1, last_zz, span(prim * half, half), sib_lanes], sib_recv.at[2, last_zz])
        partial[...] = halves(prim)

    def last_end():
        got(wbuf.at[1, last_zz, span(sec * half, half), sib_lanes], sib_recv.at[1, last_zz])
        out = (partial[...] + halves(sec)).astype(jnp.bfloat16)
        kvbuf[1, :, :, columns_of(last_zz)] = out.reshape(sp_count, rows, wide)
        keep(1, columns_of(last_zz))

    def send_columns(m, columns):
        for i, p in enumerate((xs, ys)):
            remote(
                kvbuf.at[m, i, :, columns], kv.at[m, span(s * rows, rows), columns],
                out_send, out_recv, (p, t),
            ).start()

    scale = MAP_HEAD_SIZE ** (-0.5)
    row = lax.broadcasted_iota(jnp.int32, (state_rows, 1), 0)
    row_map = row // (CORES * seq_count)
    row_seq = (row // CORES) % seq_count
    row_head = row % CORES

    def by_seq(new, first):
        values = jnp.zeros((state_rows, new.shape[1]), jnp.float32)
        for b in range(seq_count):
            values = jnp.where(row_seq == b, new[first + b : first + b + 1], values)
        return values

    def by_head(values):
        return functools.reduce(
            jnp.add,
            [jnp.where(row_head == i, values[:, i * VD : (i + 1) * VD], 0.0) for i in range(CORES)],
        )

    def queries_of(zz):
        return qbuf.at[span(zz * CORES, CORES), pl.ds(0, seq_count)]

    def new_rows(zz):
        return jnp.concatenate([qbuf[zz * CORES + i] for i in range(CORES)], axis=1)

    def query_of(new):
        lane = lax.broadcasted_iota(jnp.int32, (state_rows, wide), 1)
        mine = lane // MAP_HEAD_SIZE == row_head * 2 + row_map
        return jnp.where(mine, by_seq(new, 0), 0.0)

    def score(j, zz):
        query = query_of(new_rows(zz)).astype(jnp.bfloat16)
        keys = kvbuf[0, :, :, columns_of(zz)].reshape(-1, wide)
        scores = lax.dot_general(
            query, keys, (((1,), (1,)), ((), ())), preferred_element_type=jnp.float32
        ) * scale
        at = lax.broadcasted_iota(jnp.int32, scores.shape, 1) // rows
        spans = sp_count // seq_count
        owner = jnp.where(at == 0, xs, jnp.where(at == 1, ys, s)) // spans
        mine = owner == row_seq
        peak = jnp.max(jnp.where(mine, scores, far_below), axis=1, keepdims=True)
        raised = jnp.where(mine, jnp.exp(scores - peak), 0.0)
        total = jnp.sum(raised, axis=1, keepdims=True)
        high = raised.astype(jnp.bfloat16)
        low = (raised - high.astype(jnp.float32)).astype(jnp.bfloat16)
        pbuf[j, :state_rows] = high
        pbuf[j, state_rows:] = low
        pstat[j, 0] = jnp.broadcast_to(peak, (state_rows, VD))
        pstat[j, 1] = jnp.broadcast_to(total, (state_rows, VD))

    def weigh(j, zz):
        values = kvbuf[1, :, :, columns_of(zz)].reshape(-1, wide)
        both = jnp.dot(pbuf[j], values, preferred_element_type=jnp.float32)
        return by_head(both[:state_rows] + both[state_rows:]), pstat[j, 0][:, :1], pstat[j, 1][:, :1]

    def send_state(zz):
        view = stbuf.at[z, zz, pl.ds(0, state_rows + 1)]
        for p in z_peers:
            push(view, st_send, st_recv.at[zz], p)

    def send_up(slot, m, zz, recv):
        for i, p in enumerate((xs, ys)):
            remote(kvbuf.at[m, i, :, columns_of(zz)], upbuf.at[slot, i], out_send, recv, (p, inner)).start()

    def pass_down(slot, m, zz):
        for i, p in enumerate((xs, ys)):
            remote(
                upbuf.at[slot, i], kv.at[m, span(p * rows, rows), columns_of(zz)],
                out_send, out_recv, (s, outer * CORES + c),
            ).start()

    mine_at = chips - 1
    loads[2].wait()
    loads[3].wait()
    before = None
    for core in (c, 1 - c):
        for m in range(2):
            if core is not c:
                got(wbuf.at[m, z, :, sib_lanes], sib_recv.at[m, z])
            columns = product(0, m, z, core * cols, cols)
            if before is not None:
                pl.when(inside)(lambda before=before: send_columns(*before))
            before = (m, columns)

    def vectors():
        loads[4].wait()
        loads[5].wait()
        vector = token[...]
        me_q = jnp.dot(vector, wq[...], preferred_element_type=jnp.float32)
        me_k = jnp.dot(vector, wbuf[0, z, :, lanes], preferred_element_type=jnp.float32)
        me_v = jnp.dot(vector, wbuf[1, z, :, lanes], preferred_element_type=jnp.float32)
        for i, value in enumerate((me_q, me_k, me_v)):
            value = value.astype(jnp.bfloat16).astype(jnp.float32)
            qbuf[t, i * seq_count : (i + 1) * seq_count, :] = value[:seq_count]
    def own_block():
        loads[6].wait()
        far_prompt.wait_recv()

        def some(m, _):
            product(1, m, z, 0, wide)
            keep(m, columns_of(z))
            return 0

        lax.fori_loop(0, 2, some, 0)
        score(mine_at, z)
        new = new_rows(z)
        own_score = jnp.sum(query_of(new) * by_seq(new, seq_count), axis=1, keepdims=True) * scale
        holder = jnp.logical_and(s == 0, c == 0)
        own = (
            jnp.where(holder, by_head(by_seq(new, 2 * seq_count)), 0.0),
            jnp.where(holder, own_score, far_below),
            jnp.where(holder, jnp.ones_like(own_score), 0.0),
        )
        pack(stbuf.at[z, z], 0, state_rows, merged([weigh(mine_at, z), own]))

    def compute(g):
        j, m = group(g)
        zz, _ = source(j)
        multiply(m, zz)

        @pl.when(m == 0)
        def _():
            got(queries_of(zz), pk_recv.at[zz])
            score(j, zz)

        @pl.when(m == 1)
        def _():
            pack(stbuf.at[z, zz], 0, state_rows, weigh(j, zz))

    def results(g):
        j, m = group(g)
        zz, _ = source(j)
        send_columns(m, columns_of(zz))

    def state(g):
        j, m = group(g)
        zz, _ = source(j)
        pl.when(m == 1)(lambda: send_state(zz))

    groups = 2 * (chips - 1)
    own_at = jnp.where(inside, 7, 5)

    def work(e, _):
        arrive(e)

        @pl.when(e == 2)
        def _():
            pl.when(inside)(lambda: send_columns(*before))
            vectors()

        @pl.when(e == 3)
        def _():
            push(qbuf.at[t], pk_send, pk_recv.at[z], (s, sib))

        @pl.when(e == 4)
        def _():
            got(qbuf.at[sib], pk_recv.at[z])
            for p in z_peers:
                push(queries_of(z), pk_send, pk_recv.at[z], p)

            @pl.when(outside)
            def _():
                for m in range(2):
                    view = wbuf.at[m, z, span(sec * half, half), lanes]
                    push(view, line_send.at[jnp.where(z == 0, 1, 0)], sec_recv.at[m, z], (s, inner))
                for m in range(2):
                    send_up(m, m, z, up_recv.at[0])

        pl.when(e == own_at)(own_block)
        pl.when(outside & (e >= 9) & (e < 11))(lambda: arrive_relayed(e - 9))
        pl.when(outside & (e == 9))(lambda: send_up(2, 0, source(1)[0], up_recv.at[1]))
        ready = jnp.where(inside, e - 9, jnp.where(e < 9, e - 6, e - 7))
        pl.when((ready >= 0) & (inside | ((e != 9) & (e < 11))))(lambda: arrive_secondary(ready))
        now = jnp.where(inside, e - 10, jnp.where(e == 8, 2, e - 9))
        pl.when(jnp.where(inside, e >= 10, (e == 8) | (e == 9)))(lambda: compute(now))
        return 0

    events = 2 * groups
    lax.fori_loop(jnp.where(inside, 0, 2), events, work, 0)

    @pl.when(inside)
    def _():
        results(0)
        results(1)

    pl.when(outside)(lambda: send_state(z))

    def rest(i, _):
        @pl.when(inside & (i == 2))
        def _():
            send_state(z)
            state(2)
            state(3)
            got(upbuf.at[pl.ds(0, 2)], up_recv.at[0])
            for m in range(2):
                pass_down(m, m, outer)

        behind = jnp.where(inside, i + 3, groups - 2)
        pl.when(jnp.where(inside, i < 2, i == 1))(lambda: arrive_secondary(behind))

        @pl.when(i == 2)
        def _():
            last_begin()
            arrive_secondary(groups - 1)

        g = jnp.where(outside & (i == 0), 1, i + 2)
        compute(g)
        pl.when(outside & (i == 0))(lambda: results(0))
        results(g)
        pl.when(outside)(lambda: state(g))
        return 0

    lax.fori_loop(0, 3, rest, 0)

    me = s * CORES + c
    ends = (0, chips - 1)
    middle = tuple(range(1, chips - 1))

    def join_z(k, blocks):
        for i, zz in enumerate(blocks):
            got(stbuf.at[pl.ds(0, chips - 1), zz, pl.ds(0, state_rows + 1)], st_recv.at[zz])
            whole = merged([unpack(stbuf.at[a, zz], 0, state_rows, state_rows) for a in range(chips)])
            pack(finbuf.at[k, me], i * state_rows, len(blocks) * state_rows + i, whole)

    def send_joined(k, blocks):
        view = finbuf.at[k, me, pl.ds(0, len(blocks) * (state_rows + 1))]
        for p in plane_peers + cross_peers + [(s, sib)]:
            push(view, fin_send, fin_recv.at[k], p)

    last_end()
    pack(stbuf.at[z, last_zz], 0, state_rows, weigh(chips - 2, last_zz))
    results(groups - 1)
    state(groups - 1)

    @pl.when(inside)
    def _():
        got(upbuf.at[2], up_recv.at[1])
        pass_down(2, 0, 2 * z - outer)

    join_z(0, middle)
    send_joined(0, middle)
    join_z(1, ends)
    send_joined(1, ends)
    others = sp_count * CORES - 1
    fin_rows = pl.ds(0, 2 * (state_rows + 1))
    for k in range(2):
        got(finbuf.at[k, pl.ds(0, others), fin_rows], fin_recv.at[k])

    def pieces_view(count):
        return wbuf.at[:, 0, pl.ds(0, count * step * cols // (2 * wide)), :]

    others_rows = pl.ds(0, 2)
    far_prompt.wait_send()
    got(kvbuf.at[:, others_rows], out_recv)
    for pieces, on in ((11, inside), (8, outside)):
        pl.when(on)(lambda pieces=pieces: gone(pieces_view(pieces), out_send))
    for pieces, on in ((8, inside), (14, outside)):
        pl.when(on)(lambda pieces=pieces: gone(pieces_view(pieces), xy_send))
    gone(wbuf.at[:, :, :, lanes], sib_send)
    query_rows = qbuf.shape[1] + len(z_peers) * CORES * seq_count
    gone(qbuf.at[pl.ds(0, query_rows // 4), pl.ds(0, 4)], pk_send)
    gone(stbuf.at[pl.ds(0, chips - 1), :, pl.ds(0, state_rows + 1)], st_send)
    gone(finbuf.at[:, pl.ds(0, others), fin_rows], fin_send)
    for direction in (-1, 1):
        for pieces, last in ((10, True), (8, False)):
            @pl.when(jnp.logical_and(has_next(direction), to_end(direction) == last))
            def _(direction=direction, pieces=pieces):
                gone(pieces_view(pieces), line_send.at[(direction + 1) // 2])


def store_kernel(
    blocks, kv, finbuf, balance_hbm, gain_hbm, keys_out, values_out, read_out, read, balance, gain, sem
):
    copies = [
        pltpu.make_async_copy(balance_hbm, balance, sem.at[0]),
        pltpu.make_async_copy(gain_hbm, gain, sem.at[1]),
        pltpu.make_async_copy(kv.at[0], keys_out, sem.at[2]),
        pltpu.make_async_copy(kv.at[1], values_out, sem.at[3]),
        pltpu.make_async_copy(read, read_out, sem.at[4]),
    ]
    for a in copies[:4]:
        a.start()
    devices, state_rows = finbuf.shape[1], CORES * 2 * read.shape[0]
    fold = state_rows // 2
    seq_count = read.shape[0]
    heads = {}
    for k, zz_list in enumerate(blocks):
        for i, zz in enumerate(zz_list):
            at, stat_at = i * state_rows, len(zz_list) * state_rows + i
            weighted, _, total = merged(
                [unpack(finbuf.at[k, a], at, stat_at, state_rows) for a in range(devices)]
            )
            heads[zz] = weighted / total
    copies[0].wait()
    copies[1].wait()
    for zz, heads_out in heads.items():
        lane = lax.broadcasted_iota(jnp.int32, (fold, HEADS), 1)
        chosen = lane == zz * CORES + lax.broadcasted_iota(jnp.int32, (fold, HEADS), 0) % CORES
        second = jnp.sum(jnp.where(chosen, balance[...], 0.0), axis=1, keepdims=True)
        blended = heads_out[:fold] - second * heads_out[fold:]
        normed = (
            blended
            * lax.rsqrt(jnp.mean(blended * blended, axis=1, keepdims=True) + norm_eps)
            * gain[...]
        )
        for b in range(seq_count):
            for h in range(CORES):
                r = b * CORES + h
                read[b : b + 1, (zz * CORES + h) * VD : (zz * CORES + h + 1) * VD] = normed[r : r + 1]
    copies[4].start()
    for a in copies[2:]:
        a.wait()


def fused(prompt, new_token, query_proj_matrix, key_weight, value_weight, map_balance, head_gain):
    seq_count, _, span_count, _, piece_rows, width = prompt.shape
    sp_count, tp_count = lax.axis_size("sp"), lax.axis_size("tp")
    cols = key_weight.shape[1]
    slots = seq_count * span_count
    chips = tp_count // CORES
    key_width = cols * tp_count
    block_rows = sp_count * piece_rows
    state_rows = CORES * 2 * seq_count
    any_space = pl.BlockSpec(memory_space=pltpu.HBM)
    vmem = pl.BlockSpec(memory_space=pltpu.VMEM)
    dma = pltpu.SemaphoreType.DMA
    kv, states = pl.pallas_call(
        functools.partial(step_kernel, (sp_count, tp_count, seq_count)),
        out_shape=[
            pltpu.VMEM((2, block_rows, key_width), jnp.bfloat16),
            pltpu.VMEM((2, sp_count * CORES, 2 * state_rows + 8, VD), jnp.float32),
        ],
        in_specs=[any_space] * 5,
        out_specs=[vmem, vmem],
        scratch_shapes=[
            pltpu.VMEM((slots, piece_rows, width), jnp.bfloat16),
            pltpu.VMEM((2, chips, width, CORES * cols), jnp.bfloat16),
            pltpu.VMEM((2, slots, piece_rows, key_width), jnp.bfloat16),
            pltpu.VMEM((3, 2, piece_rows, CORES * cols), jnp.bfloat16),
            pltpu.VMEM((slots * piece_rows, CORES * cols), jnp.float32),
            pltpu.VMEM((width, cols), jnp.bfloat16),
            pltpu.VMEM((seq_count, width), jnp.bfloat16),
            pltpu.VMEM((tp_count, 8, cols), jnp.float32),
            pltpu.VMEM((chips, 2 * state_rows, slots * piece_rows), jnp.bfloat16),
            pltpu.VMEM((chips, 2, state_rows, VD), jnp.float32),
            pltpu.VMEM((chips, chips, 2 * state_rows, VD), jnp.float32),
            dma((7,)), dma(()), dma(()), dma((2,)), dma((2, chips, PIECES)), dma(()), dma((2, chips)), dma((2,)),
            dma(()), dma((3, chips)),
            dma(()), dma(()), dma((2,)), dma(()), dma((chips,)), dma(()), dma((chips,)), dma(()), dma((2,)),
        ],
        compiler_params=pltpu.CompilerParams(
            collective_id=0, has_side_effects=True, vmem_limit_bytes=61 * 1024 * 1024 + 512 * 1024
        ),
    )(
        prompt.reshape(slots, piece_rows, width),
        new_token, query_proj_matrix, key_weight, value_weight,
    )
    blocks = (tuple(range(1, chips - 1)), (0, chips - 1))
    keys, values, read = pl.pallas_call(
        functools.partial(store_kernel, blocks),
        out_shape=[
            jax.ShapeDtypeStruct((block_rows, key_width), jnp.bfloat16),
            jax.ShapeDtypeStruct((block_rows, key_width), jnp.bfloat16),
            jax.ShapeDtypeStruct((seq_count, HEADS * VD), jnp.float32),
        ],
        in_specs=[vmem, vmem, any_space, any_space],
        out_specs=[any_space] * 3,
        scratch_shapes=[
            pltpu.VMEM((seq_count, HEADS * VD), jnp.float32),
            pltpu.VMEM((1, HEADS), jnp.float32),
            pltpu.VMEM((1, VD), jnp.float32),
            dma((5,)),
        ],
        compiler_params=pltpu.CompilerParams(vmem_limit_bytes=1024 * 1024),
    )(kv, states, map_balance[None, :], head_gain[None, :])
    shape = (1, 1, block_rows, key_width)
    return keys.reshape(shape), values.reshape(shape), read


def fits(mesh, key_weight, value_weight, prompt):
    tp_count, sp_count = mesh.shape["tp"], mesh.shape["sp"]
    seq_count, _, span_count = prompt.shape[:3]
    cols = key_weight.shape[1] // tp_count
    return (
        sp_count == 4
        and seq_count * span_count == sp_count
        and tp_count % CORES == 0
        and tp_count == 4 * CORES
        and cols == VD
        and 3 * seq_count <= 8
        and key_weight.shape == value_weight.shape
    )


def solution(mesh):
    in_specs = (
        P(None, "tp", None, "sp", None, None),
        P(),
        P(None, "tp"),
        P(None, "tp"),
        P(None, "tp"),
        P(),
        P(),
    )
    out_specs = (P("sp", "tp", None, None), P("sp", "tp", None, None), P())

    def step(prompt, new_token, query_proj_matrix, key_weight, value_weight, map_balance, head_gain):
        body = fused if fits(mesh, key_weight, value_weight, prompt) else shards
        mapped = jax.shard_map(
            body, mesh=mesh, in_specs=in_specs, out_specs=out_specs, check_vma=False
        )
        return mapped(
            prompt, new_token, query_proj_matrix, key_weight, value_weight, map_balance, head_gain
        )

    return step
```

```python
import functools

import jax
import jax.numpy as jnp
from jax import lax
from jax.experimental import pallas as pl
from jax.experimental.pallas import tpu as pltpu
from jax.sharding import PartitionSpec as P

HEADS = 8
MAP_HEAD_SIZE = 64
VD = 128


norm_eps = 1e-06
far_below = -1e30


def joined(part, axis, combine):
    gathered = jax.tree.map(lambda a: lax.all_gather(a, axis), part)

    def take(source):
        return jax.tree.map(lambda a: lax.dynamic_index_in_dim(a, source, 0, False), gathered)

    return lax.fori_loop(
        1, lax.axis_size(axis), lambda source, state: combine(state, take(source)), take(0)
    )


def fill_cols(source, w_piece):
    product = jnp.dot(source, w_piece, preferred_element_type=jnp.float32).astype(jnp.bfloat16)
    return product


def local_new(new_token, query_proj_matrix, key_weight, value_weight):
    return (
        jnp.dot(new_token, query_proj_matrix, preferred_element_type=jnp.float32).astype(
            jnp.bfloat16
        ),
        jnp.dot(new_token, key_weight, preferred_element_type=jnp.float32).astype(jnp.bfloat16),
        jnp.dot(new_token, value_weight, preferred_element_type=jnp.float32).astype(jnp.bfloat16),
    )


def partial_read(query_matrix_rows, key_rows, value_rows):
    logit_scores = jnp.einsum(
        "bhmd,bjhmd->bhmj", query_matrix_rows, key_rows, preferred_element_type=jnp.float32
    ) * MAP_HEAD_SIZE ** (-0.5)
    peak = jnp.max(logit_scores, axis=-1)
    weights_exp = jnp.exp(logit_scores - peak[..., None])
    totals = jnp.sum(weights_exp, axis=-1)
    weighted = jnp.einsum("bhmj,bjhe->bhme", weights_exp, value_rows.astype(jnp.float32))
    return (peak, totals, weighted)


def combine(first, second):
    peak_a, totals_a, weighted_a = first
    peak_b, totals_b, weighted_b = second
    peak = jnp.maximum(peak_a, peak_b)
    factor_a = jnp.exp(peak_a - peak)
    factor_b = jnp.exp(peak_b - peak)
    return (
        peak,
        totals_a * factor_a + totals_b * factor_b,
        weighted_a * factor_a[..., None] + weighted_b * factor_b[..., None],
    )


def shards(prompt, new_token, query_proj_matrix, key_weight, value_weight, map_balance, head_gain):
    seq_count, _, span_count, _, piece_rows, model_width = prompt.shape
    token_rows = prompt.reshape(seq_count * span_count * piece_rows, model_width)
    tp_count = lax.axis_size("tp")
    key_width = key_weight.shape[1] * tp_count
    value_width = value_weight.shape[1] * tp_count
    key_piece = lax.all_gather(key_weight, "tp", axis=1, tiled=True)
    value_piece = lax.all_gather(value_weight, "tp", axis=1, tiled=True)
    key_rows = fill_cols(token_rows, key_piece)
    value_rows = fill_cols(token_rows, value_piece)
    own_columns = local_new(new_token, query_proj_matrix, key_weight, value_weight)
    queries, new_keys, new_values = (
        lax.all_gather(own_columns[0], "tp", axis=1, tiled=True),
        lax.all_gather(own_columns[1], "tp", axis=1, tiled=True),
        lax.all_gather(own_columns[2], "tp", axis=1, tiled=True),
    )
    slot_count = seq_count * span_count
    cached_keys, cached_values = (
        lax.all_to_all(
            key_rows.reshape(slot_count, piece_rows, key_width),
            "sp",
            split_axis=0,
            concat_axis=1,
            tiled=True,
        ),
        lax.all_to_all(
            value_rows.reshape(slot_count, piece_rows, value_width),
            "sp",
            split_axis=0,
            concat_axis=1,
            tiled=True,
        ),
    )
    block_rows = cached_keys.shape[1]
    key_cache = cached_keys.reshape(1, 1, block_rows, key_width)
    value_cache = cached_values.reshape(1, 1, block_rows, value_width)
    all_queries = queries.reshape(seq_count, HEADS, 2, MAP_HEAD_SIZE)
    own_seq = lax.axis_index("sp") // span_count
    own_query = lax.dynamic_slice_in_dim(all_queries, own_seq, 1, 0)
    peak, totals, weighted = partial_read(
        own_query,
        cached_keys.reshape(1, block_rows, HEADS, 2, MAP_HEAD_SIZE),
        cached_values.reshape(1, block_rows, HEADS, VD),
    )
    chosen = jnp.arange(seq_count) == own_seq
    chosen_rows = chosen[:, None, None]
    spread = (
        jnp.where(chosen_rows, peak, far_below),
        jnp.where(chosen_rows, totals, 0.0),
        jnp.where(chosen_rows[..., None], weighted, 0.0),
    )
    merged = joined(spread, ("sp", "tp"), combine)
    own_keys = new_keys.reshape(seq_count, HEADS, 2, MAP_HEAD_SIZE)
    own_score = jnp.einsum(
        "bhmd,bhmd->bhm", all_queries, own_keys, preferred_element_type=jnp.float32
    ) * MAP_HEAD_SIZE ** (-0.5)
    own_values = new_values.astype(jnp.float32).reshape(seq_count, HEADS, VD)
    own_weighted = jnp.broadcast_to(own_values[:, :, None, :], (seq_count, HEADS, 2, VD))
    own_state = (own_score, jnp.ones_like(own_score), own_weighted)
    _, totals, weighted = combine(merged, own_state)
    heads_out = weighted / totals[..., None]
    blended = heads_out[:, :, 0] - map_balance[None, :, None] * heads_out[:, :, 1]
    normed = (
        blended
        * lax.rsqrt(jnp.mean(blended * blended, axis=-1, keepdims=True) + norm_eps)
        * head_gain
    )
    return (key_cache, value_cache, normed.reshape(seq_count, HEADS * VD))


MESH = pl.DeviceIdType.MESH
CORES = 2
PIECES = 2


def merged(states):
    peak = functools.reduce(jnp.maximum, [a[1] for a in states])
    factors = [jnp.exp(a[1] - peak) for a in states]
    weighted = functools.reduce(jnp.add, [a[0] * f for a, f in zip(states, factors)])
    total = functools.reduce(jnp.add, [a[2] * f for a, f in zip(states, factors)])
    return weighted, peak, total


def pack(ref, at, stat_at, state):
    weighted, peak, total = state
    rows = weighted.shape[0]
    lane = lax.broadcasted_iota(jnp.int32, weighted.shape, 1)
    row = lax.broadcasted_iota(jnp.int32, weighted.shape, 0)
    stats = jnp.where(lane == row, peak, jnp.where(lane == row + rows, total, 0.0))
    ref[at : at + rows] = weighted
    ref[stat_at : stat_at + 1] = jnp.sum(stats, axis=0, keepdims=True)


def unpack(ref, at, stat_at, rows):
    weighted = ref[at : at + rows]
    lane = lax.broadcasted_iota(jnp.int32, weighted.shape, 1)
    row = lax.broadcasted_iota(jnp.int32, weighted.shape, 0)
    stats = ref[stat_at : stat_at + 1]
    peak = jnp.sum(jnp.where(lane == row, stats, 0.0), axis=1, keepdims=True)
    total = jnp.sum(jnp.where(lane == row + rows, stats, 0.0), axis=1, keepdims=True)
    return weighted, peak, total


def step_kernel(
    dims,
    prompt, token_hbm, wq_hbm, wk_hbm, wv_hbm,
    kv, finbuf,
    xbuf, wbuf, kvbuf, upbuf, partial, wq, token, qbuf, pbuf, pstat, stbuf,
    loc, far_send, far_recv, line_send, prim_recv, xy_send, sec_recv, relay_recv, sib_send, sib_recv,
    out_send, out_recv, up_recv, pk_send, pk_recv, st_send, st_recv, fin_send, fin_recv,
):
    sp_count, tp_count, seq_count = dims
    _, _, depth, wide = wbuf.shape
    cols = wide // CORES
    chips = tp_count // CORES
    rows = xbuf.shape[1]
    state_rows = CORES * 2 * seq_count
    s = lax.axis_index("sp")
    t = lax.axis_index("tp")
    z = t // CORES
    c = t % CORES
    sib = z * CORES + (1 - c)
    xs = s + 1 - 2 * (s % 2)
    ys = (s + 2) % 4
    diag = 3 - s
    prim = (s + s // 2) % 2
    sec = 1 - prim
    turn = s // 2
    near = jnp.minimum(z, chips - 1 - z)
    inside = near > 0
    outside = jnp.logical_not(inside)
    half = depth // 2
    step = half // PIECES
    part_rows = step // 2

    def lanes_of(core):
        return pl.ds(pl.multiple_of(core * cols, cols), cols)

    lanes, sib_lanes = lanes_of(c), lanes_of(1 - c)

    loads = [
        pltpu.make_async_copy(wk_hbm, wbuf.at[0, z, :, lanes], loc.at[0]),
        pltpu.make_async_copy(wv_hbm, wbuf.at[1, z, :, lanes], loc.at[1]),
        pltpu.make_async_copy(prompt.at[xs], xbuf.at[0], loc.at[2]),
        pltpu.make_async_copy(prompt.at[ys], xbuf.at[1], loc.at[3]),
        pltpu.make_async_copy(token_hbm, token, loc.at[4]),
        pltpu.make_async_copy(wq_hbm, wq, loc.at[5]),
        pltpu.make_async_copy(prompt.at[s], xbuf.at[2], loc.at[6]),
    ]
    for a in loads:
        a.start()

    z_peers = [(s, (t + d * CORES) % tp_count) for d in range(1, chips)]
    plane_peers = [((s + d) % sp_count, t) for d in range(1, sp_count)]
    cross_peers = [((s + d) % sp_count, sib) for d in range(1, sp_count)]
    barrier = pltpu.get_barrier_semaphore()
    greeted = plane_peers + [(s, sib)]

    def greet(p):
        pl.semaphore_signal(barrier, inc=1, device_id=p, device_id_type=MESH)

    pl.when(z > 0)(lambda: greet((s, t - CORES)))
    pl.when(z < chips - 1)(lambda: greet((s, t + CORES)))
    for p in greeted:
        greet(p)
    pl.semaphore_wait(barrier, len(greeted) + jnp.where(inside, 2, 1))

    def remote(src, dst, send, recv, dev):
        return pltpu.make_async_remote_copy(
            src_ref=src, dst_ref=dst, send_sem=send, recv_sem=recv, device_id=dev, device_id_type=MESH
        )

    def push(view, send, recv, dev):
        remote(view, view, send, recv, dev).start()

    def got(view, recv):
        remote(view, view, xy_send, recv, (s, sib)).wait_recv()

    def gone(view, send):
        remote(view, view, send, loc.at[0], (s, sib)).wait_send()

    def span(start, size):
        return pl.ds(pl.multiple_of(start, size), size)

    def piece_of(m, zz, p):
        return wbuf.at[m, zz, span(prim * half + p * step, step), lanes]

    def line(direction, m, zz, p):
        view = piece_of(m, zz, p)
        push(view, line_send.at[(direction + 1) // 2], prim_recv.at[m, zz, p], (s, t + direction * CORES))

    def has_next(direction):
        return (z > 0) if direction < 0 else (z < chips - 1)

    def to_end(direction):
        return (z == 1) if direction < 0 else (z == chips - 2)

    far_prompt = remote(prompt.at[diag], xbuf.at[3], far_send, far_recv, (diag, t))
    far_prompt.start()
    for m in range(2):
        loads[m].wait()
        for direction in (-1, 1):
            @pl.when(jnp.logical_and(has_next(direction), to_end(direction)))
            def _(direction=direction, m=m):
                line(direction, m, z, turn)

            @pl.when(jnp.logical_and(has_next(direction), jnp.logical_not(to_end(direction))))
            def _(direction=direction, m=m):
                for p in range(PIECES):
                    line(direction, m, z, p)
        push(wbuf.at[m, z, :, lanes], sib_send, sib_recv.at[m, z], (s, sib))
    inner = jnp.where(z == 0, t + CORES, t - CORES)
    outer = jnp.where(z == 1, z - 1, z + 1)

    def source(j):
        j = j + 1
        paired = j <= 2 * near
        dist = jnp.where(paired, (j + 1) // 2, j - near)
        from_left = jnp.where(paired, j % 2 == 1, z > near)
        return jnp.where(from_left, z - dist, z + dist), from_left

    def event(e):
        both = jnp.logical_and(inside, e < 8)
        j = jnp.where(both, e % 2, e // 4)
        m = jnp.where(both, e // 4, (e // 2) % 2)
        p = jnp.where(both, (e // 2) % 2, e % 2)
        single = jnp.logical_and(outside, e < 4)
        return j, jnp.where(single, e % 2, m), jnp.where(single, turn, p)

    def group(g):
        both = jnp.logical_and(inside, g < 4)
        return jnp.where(both, g % 2, g // 2), jnp.where(both, g // 2, g % 2)

    def arrive(e):
        j, m, p = event(e)
        zz, from_left = source(j)
        view = piece_of(m, zz, p)
        got(view, prim_recv.at[m, zz, p])
        on_right = jnp.logical_and(from_left, z < chips - 1)
        on_left = jnp.logical_and(jnp.logical_not(from_left), z > 0)
        pl.when(on_right)(lambda: line(1, m, zz, p))
        pl.when(on_left)(lambda: line(-1, m, zz, p))
        single = jnp.logical_and(outside, e < 4)

        @pl.when(single)
        def _():
            for to in (xs, ys):
                push(view, xy_send, sec_recv.at[m, zz], (to, t))

        whole = jnp.logical_and(inside, zz == outer)

        @pl.when(jnp.logical_not(jnp.logical_or(single, whole)))
        def _():
            for h, to in enumerate((xs, ys)):
                part = part_of(prim, m, zz, p, h)
                push(part, xy_send, sec_recv.at[m, zz], (to, t))

        last = jnp.logical_and(j == chips - 2, m == 1)
        push(view, sib_send, sib_recv.at[jnp.where(last, 2, m), zz], (s, sib))

    def part_of(which, m, zz, p, h):
        return wbuf.at[m, zz, span(which * half + p * step + h * part_rows, part_rows), lanes]

    def arrive_secondary(g):
        j, m = group(g)
        zz, _ = source(j)
        view = wbuf.at[m, zz, span(sec * half, half), lanes]
        got(view, sec_recv.at[m, zz])

        @pl.when(jnp.logical_and(outside, g < 2))
        def _():
            push(part_of(sec, m, zz, 1 - turn, 0), xy_send, relay_recv.at[m], (xs, t))
            push(part_of(sec, m, zz, turn, 1), xy_send, relay_recv.at[m], (ys, t))

        push(view, sib_send, sib_recv.at[m, zz], (s, sib))

    def arrive_relayed(m):
        zz, _ = source(0)
        view = piece_of(m, zz, 1 - turn)
        got(view, relay_recv.at[m])
        push(view, sib_send, sib_recv.at[m, zz], (s, sib))

    def columns_of(zz):
        return pl.ds(pl.multiple_of(zz * wide, wide), wide)

    def product(pair, m, zz, first, width):
        at = pl.ds(2 * pair, 2)
        columns = span(zz * wide + first, width)
        out = jnp.dot(
            xbuf[at].reshape(-1, depth), wbuf[m, zz, :, span(first, width)],
            preferred_element_type=jnp.float32,
        ).astype(jnp.bfloat16)
        kvbuf[m, at, :, columns] = out.reshape(2, rows, width)
        return columns

    def whole_product(m, zz):
        out = jnp.dot(
            xbuf[...].reshape(-1, depth), wbuf[m, zz], preferred_element_type=jnp.float32
        ).astype(jnp.bfloat16)
        kvbuf[m, :, :, columns_of(zz)] = out.reshape(sp_count, rows, wide)

    def keep(m, columns):
        for i, slot in ((2, s), (3, diag)):
            kv[m, span(slot * rows, rows), columns] = kvbuf[m, i, :, columns]

    def multiply(m, zz):
        got(wbuf.at[m, zz, :, sib_lanes], sib_recv.at[m, zz])

        whole_product(m, zz)
        keep(m, columns_of(zz))

    last_zz = source(chips - 2)[0]

    def halves(which):
        at = span(which * half, half)
        return jnp.dot(
            xbuf[:, :, at].reshape(-1, half), wbuf[1, last_zz, at, :], preferred_element_type=jnp.float32
        )

    def last_begin():
        got(wbuf.at[1, last_zz, span(prim * half, half), sib_lanes], sib_recv.at[2, last_zz])
        partial[...] = halves(prim)

    def last_end():
        got(wbuf.at[1, last_zz, span(sec * half, half), sib_lanes], sib_recv.at[1, last_zz])
        out = (partial[...] + halves(sec)).astype(jnp.bfloat16)
        kvbuf[1, :, :, columns_of(last_zz)] = out.reshape(sp_count, rows, wide)
        keep(1, columns_of(last_zz))

    def send_columns(m, columns):
        for i, p in enumerate((xs, ys)):
            remote(
                kvbuf.at[m, i, :, columns], kv.at[m, span(s * rows, rows), columns],
                out_send, out_recv, (p, t),
            ).start()

    scale = MAP_HEAD_SIZE ** (-0.5)
    row = lax.broadcasted_iota(jnp.int32, (state_rows, 1), 0)
    row_map = row // (CORES * seq_count)
    row_seq = (row // CORES) % seq_count
    row_head = row % CORES

    def by_seq(new, first):
        values = jnp.zeros((state_rows, new.shape[1]), jnp.float32)
        for b in range(seq_count):
            values = jnp.where(row_seq == b, new[first + b : first + b + 1], values)
        return values

    def by_head(values):
        return functools.reduce(
            jnp.add,
            [jnp.where(row_head == i, values[:, i * VD : (i + 1) * VD], 0.0) for i in range(CORES)],
        )

    def queries_of(zz):
        return qbuf.at[span(zz * CORES, CORES), pl.ds(0, seq_count)]

    def new_rows(zz):
        return jnp.concatenate([qbuf[zz * CORES + i] for i in range(CORES)], axis=1)

    def query_of(new):
        lane = lax.broadcasted_iota(jnp.int32, (state_rows, wide), 1)
        mine = lane // MAP_HEAD_SIZE == row_head * 2 + row_map
        return jnp.where(mine, by_seq(new, 0), 0.0)

    def score(j, zz):
        query = query_of(new_rows(zz)).astype(jnp.bfloat16)
        keys = kvbuf[0, :, :, columns_of(zz)].reshape(-1, wide)
        scores = lax.dot_general(
            query, keys, (((1,), (1,)), ((), ())), preferred_element_type=jnp.float32
        ) * scale
        at = lax.broadcasted_iota(jnp.int32, scores.shape, 1) // rows
        spans = sp_count // seq_count
        owner = jnp.where(at == 0, xs, jnp.where(at == 1, ys, s)) // spans
        mine = owner == row_seq
        peak = jnp.max(jnp.where(mine, scores, far_below), axis=1, keepdims=True)
        raised = jnp.where(mine, jnp.exp(scores - peak), 0.0)
        total = jnp.sum(raised, axis=1, keepdims=True)
        high = raised.astype(jnp.bfloat16)
        low = (raised - high.astype(jnp.float32)).astype(jnp.bfloat16)
        pbuf[j, :state_rows] = high
        pbuf[j, state_rows:] = low
        pstat[j, 0] = jnp.broadcast_to(peak, (state_rows, VD))
        pstat[j, 1] = jnp.broadcast_to(total, (state_rows, VD))

    def weigh(j, zz):
        values = kvbuf[1, :, :, columns_of(zz)].reshape(-1, wide)
        both = jnp.dot(pbuf[j], values, preferred_element_type=jnp.float32)
        return by_head(both[:state_rows] + both[state_rows:]), pstat[j, 0][:, :1], pstat[j, 1][:, :1]

    def send_state(zz):
        view = stbuf.at[z, zz, pl.ds(0, state_rows + 1)]
        for p in z_peers:
            push(view, st_send, st_recv.at[zz], p)

    def send_up(slot, m, zz, recv):
        for i, p in enumerate((xs, ys)):
            remote(kvbuf.at[m, i, :, columns_of(zz)], upbuf.at[slot, i], out_send, recv, (p, inner)).start()

    def pass_down(slot, m, zz):
        for i, p in enumerate((xs, ys)):
            remote(
                upbuf.at[slot, i], kv.at[m, span(p * rows, rows), columns_of(zz)],
                out_send, out_recv, (s, outer * CORES + c),
            ).start()

    mine_at = chips - 1
    loads[2].wait()
    loads[3].wait()
    before = None
    for core in (c, 1 - c):
        for m in range(2):
            if core is not c:
                got(wbuf.at[m, z, :, sib_lanes], sib_recv.at[m, z])
            columns = product(0, m, z, core * cols, cols)
            if before is not None:
                pl.when(inside)(lambda before=before: send_columns(*before))
            before = (m, columns)

    def vectors():
        loads[4].wait()
        loads[5].wait()
        vector = token[...]
        me_q = jnp.dot(vector, wq[...], preferred_element_type=jnp.float32)
        me_k = jnp.dot(vector, wbuf[0, z, :, lanes], preferred_element_type=jnp.float32)
        me_v = jnp.dot(vector, wbuf[1, z, :, lanes], preferred_element_type=jnp.float32)
        for i, value in enumerate((me_q, me_k, me_v)):
            value = value.astype(jnp.bfloat16).astype(jnp.float32)
            qbuf[t, i * seq_count : (i + 1) * seq_count, :] = value[:seq_count]
    def own_block():
        loads[6].wait()
        far_prompt.wait_recv()

        def some(m, _):
            product(1, m, z, 0, wide)
            keep(m, columns_of(z))
            return 0

        lax.fori_loop(0, 2, some, 0)
        score(mine_at, z)
        new = new_rows(z)
        own_score = jnp.sum(query_of(new) * by_seq(new, seq_count), axis=1, keepdims=True) * scale
        holder = jnp.logical_and(s == 0, c == 0)
        own = (
            jnp.where(holder, by_head(by_seq(new, 2 * seq_count)), 0.0),
            jnp.where(holder, own_score, far_below),
            jnp.where(holder, jnp.ones_like(own_score), 0.0),
        )
        pack(stbuf.at[z, z], 0, state_rows, merged([weigh(mine_at, z), own]))

    def compute(g):
        j, m = group(g)
        zz, _ = source(j)
        multiply(m, zz)

        @pl.when(m == 0)
        def _():
            got(queries_of(zz), pk_recv.at[zz])
            score(j, zz)

        @pl.when(m == 1)
        def _():
            pack(stbuf.at[z, zz], 0, state_rows, weigh(j, zz))

    def results(g):
        j, m = group(g)
        zz, _ = source(j)
        send_columns(m, columns_of(zz))

    def state(g):
        j, m = group(g)
        zz, _ = source(j)
        pl.when(m == 1)(lambda: send_state(zz))

    groups = 2 * (chips - 1)
    own_at = jnp.where(inside, 7, 5)

    def work(e, _):
        arrive(e)

        @pl.when(e == 2)
        def _():
            pl.when(inside)(lambda: send_columns(*before))
            vectors()

        @pl.when(e == 3)
        def _():
            push(qbuf.at[t], pk_send, pk_recv.at[z], (s, sib))

        @pl.when(e == 4)
        def _():
            got(qbuf.at[sib], pk_recv.at[z])
            for p in z_peers:
                push(queries_of(z), pk_send, pk_recv.at[z], p)

            @pl.when(outside)
            def _():
                for m in range(2):
                    view = wbuf.at[m, z, span(sec * half, half), lanes]
                    push(view, line_send.at[jnp.where(z == 0, 1, 0)], sec_recv.at[m, z], (s, inner))
                for m in range(2):
                    send_up(m, m, z, up_recv.at[0])

        pl.when(e == own_at)(own_block)
        pl.when(outside & (e >= 9) & (e < 11))(lambda: arrive_relayed(e - 9))
        pl.when(outside & (e == 9))(lambda: send_up(2, 0, source(1)[0], up_recv.at[1]))
        ready = jnp.where(inside, e - 9, jnp.where(e < 9, e - 6, e - 7))
        pl.when((ready >= 0) & (inside | ((e != 9) & (e < 11))))(lambda: arrive_secondary(ready))
        now = jnp.where(inside, e - 10, jnp.where(e == 8, 2, e - 9))
        pl.when(jnp.where(inside, e >= 10, (e == 8) | (e == 9)))(lambda: compute(now))
        return 0

    events = 2 * groups
    lax.fori_loop(jnp.where(inside, 0, 2), events, work, 0)

    @pl.when(inside)
    def _():
        results(0)
        results(1)

    pl.when(outside)(lambda: send_state(z))

    def rest(i, _):
        @pl.when(inside & (i == 2))
        def _():
            send_state(z)
            state(2)
            state(3)
            got(upbuf.at[pl.ds(0, 2)], up_recv.at[0])
            pass_down(0, 0, outer)

        behind = jnp.where(inside, i + 3, groups - 2)
        pl.when(jnp.where(inside, i < 2, i == 1))(lambda: arrive_secondary(behind))

        @pl.when(i == 2)
        def _():
            last_begin()
            arrive_secondary(groups - 1)

        g = jnp.where(outside & (i == 0), 1, i + 2)
        compute(g)
        pl.when(outside & (i == 0))(lambda: results(0))
        results(g)
        pl.when(outside)(lambda: state(g))
        return 0

    lax.fori_loop(0, 3, rest, 0)

    me = s * CORES + c
    ends = (0, chips - 1)
    middle = tuple(range(1, chips - 1))

    def join_z(k, blocks):
        for i, zz in enumerate(blocks):
            got(stbuf.at[pl.ds(0, chips - 1), zz, pl.ds(0, state_rows + 1)], st_recv.at[zz])
            whole = merged([unpack(stbuf.at[a, zz], 0, state_rows, state_rows) for a in range(chips)])
            pack(finbuf.at[k, me], i * state_rows, len(blocks) * state_rows + i, whole)

    def send_joined(k, blocks):
        view = finbuf.at[k, me, pl.ds(0, len(blocks) * (state_rows + 1))]
        for p in plane_peers + cross_peers + [(s, sib)]:
            push(view, fin_send, fin_recv.at[k], p)

    last_end()
    pack(stbuf.at[z, last_zz], 0, state_rows, weigh(chips - 2, last_zz))
    results(groups - 1)
    state(groups - 1)

    @pl.when(inside)
    def _():
        pass_down(1, 1, outer)
        got(upbuf.at[2], up_recv.at[1])
        pass_down(2, 0, 2 * z - outer)

    join_z(0, middle)
    send_joined(0, middle)
    join_z(1, ends)
    send_joined(1, ends)
    others = sp_count * CORES - 1
    fin_rows = pl.ds(0, 2 * (state_rows + 1))
    for k in range(2):
        got(finbuf.at[k, pl.ds(0, others), fin_rows], fin_recv.at[k])

    def pieces_view(count):
        return wbuf.at[:, 0, pl.ds(0, count * step * cols // (2 * wide)), :]

    others_rows = pl.ds(0, 2)
    far_prompt.wait_send()
    got(kvbuf.at[:, others_rows], out_recv)
    for pieces, on in ((11, inside), (8, outside)):
        pl.when(on)(lambda pieces=pieces: gone(pieces_view(pieces), out_send))
    for pieces, on in ((8, inside), (14, outside)):
        pl.when(on)(lambda pieces=pieces: gone(pieces_view(pieces), xy_send))
    gone(wbuf.at[:, :, :, lanes], sib_send)
    query_rows = qbuf.shape[1] + len(z_peers) * CORES * seq_count
    gone(qbuf.at[pl.ds(0, query_rows // 4), pl.ds(0, 4)], pk_send)
    gone(stbuf.at[pl.ds(0, chips - 1), :, pl.ds(0, state_rows + 1)], st_send)
    gone(finbuf.at[:, pl.ds(0, others), fin_rows], fin_send)
    for direction in (-1, 1):
        for pieces, last in ((10, True), (8, False)):
            @pl.when(jnp.logical_and(has_next(direction), to_end(direction) == last))
            def _(direction=direction, pieces=pieces):
                gone(pieces_view(pieces), line_send.at[(direction + 1) // 2])


def store_kernel(
    blocks, kv, finbuf, balance_hbm, gain_hbm, keys_out, values_out, read_out, read, balance, gain, sem
):
    copies = [
        pltpu.make_async_copy(balance_hbm, balance, sem.at[0]),
        pltpu.make_async_copy(gain_hbm, gain, sem.at[1]),
        pltpu.make_async_copy(kv.at[0], keys_out, sem.at[2]),
        pltpu.make_async_copy(kv.at[1], values_out, sem.at[3]),
        pltpu.make_async_copy(read, read_out, sem.at[4]),
    ]
    for a in copies[:4]:
        a.start()
    devices, state_rows = finbuf.shape[1], CORES * 2 * read.shape[0]
    fold = state_rows // 2
    seq_count = read.shape[0]
    heads = {}
    for k, zz_list in enumerate(blocks):
        for i, zz in enumerate(zz_list):
            at, stat_at = i * state_rows, len(zz_list) * state_rows + i
            weighted, _, total = merged(
                [unpack(finbuf.at[k, a], at, stat_at, state_rows) for a in range(devices)]
            )
            heads[zz] = weighted / total
    copies[0].wait()
    copies[1].wait()
    for zz, heads_out in heads.items():
        lane = lax.broadcasted_iota(jnp.int32, (fold, HEADS), 1)
        chosen = lane == zz * CORES + lax.broadcasted_iota(jnp.int32, (fold, HEADS), 0) % CORES
        second = jnp.sum(jnp.where(chosen, balance[...], 0.0), axis=1, keepdims=True)
        blended = heads_out[:fold] - second * heads_out[fold:]
        normed = (
            blended
            * lax.rsqrt(jnp.mean(blended * blended, axis=1, keepdims=True) + norm_eps)
            * gain[...]
        )
        for b in range(seq_count):
            for h in range(CORES):
                r = b * CORES + h
                read[b : b + 1, (zz * CORES + h) * VD : (zz * CORES + h + 1) * VD] = normed[r : r + 1]
    copies[4].start()
    for a in copies[2:]:
        a.wait()


def fused(prompt, new_token, query_proj_matrix, key_weight, value_weight, map_balance, head_gain):
    seq_count, _, span_count, _, piece_rows, width = prompt.shape
    sp_count, tp_count = lax.axis_size("sp"), lax.axis_size("tp")
    cols = key_weight.shape[1]
    slots = seq_count * span_count
    chips = tp_count // CORES
    key_width = cols * tp_count
    block_rows = sp_count * piece_rows
    state_rows = CORES * 2 * seq_count
    any_space = pl.BlockSpec(memory_space=pltpu.HBM)
    vmem = pl.BlockSpec(memory_space=pltpu.VMEM)
    dma = pltpu.SemaphoreType.DMA
    kv, states = pl.pallas_call(
        functools.partial(step_kernel, (sp_count, tp_count, seq_count)),
        out_shape=[
            pltpu.VMEM((2, block_rows, key_width), jnp.bfloat16),
            pltpu.VMEM((2, sp_count * CORES, 2 * state_rows + 8, VD), jnp.float32),
        ],
        in_specs=[any_space] * 5,
        out_specs=[vmem, vmem],
        scratch_shapes=[
            pltpu.VMEM((slots, piece_rows, width), jnp.bfloat16),
            pltpu.VMEM((2, chips, width, CORES * cols), jnp.bfloat16),
            pltpu.VMEM((2, slots, piece_rows, key_width), jnp.bfloat16),
            pltpu.VMEM((3, 2, piece_rows, CORES * cols), jnp.bfloat16),
            pltpu.VMEM((slots * piece_rows, CORES * cols), jnp.float32),
            pltpu.VMEM((width, cols), jnp.bfloat16),
            pltpu.VMEM((seq_count, width), jnp.bfloat16),
            pltpu.VMEM((tp_count, 8, cols), jnp.float32),
            pltpu.VMEM((chips, 2 * state_rows, slots * piece_rows), jnp.bfloat16),
            pltpu.VMEM((chips, 2, state_rows, VD), jnp.float32),
            pltpu.VMEM((chips, chips, 2 * state_rows, VD), jnp.float32),
            dma((7,)), dma(()), dma(()), dma((2,)), dma((2, chips, PIECES)), dma(()), dma((2, chips)), dma((2,)),
            dma(()), dma((3, chips)),
            dma(()), dma(()), dma((2,)), dma(()), dma((chips,)), dma(()), dma((chips,)), dma(()), dma((2,)),
        ],
        compiler_params=pltpu.CompilerParams(
            collective_id=0, has_side_effects=True, vmem_limit_bytes=61 * 1024 * 1024 + 512 * 1024
        ),
    )(
        prompt.reshape(slots, piece_rows, width),
        new_token, query_proj_matrix, key_weight, value_weight,
    )
    blocks = (tuple(range(1, chips - 1)), (0, chips - 1))
    keys, values, read = pl.pallas_call(
        functools.partial(store_kernel, blocks),
        out_shape=[
            jax.ShapeDtypeStruct((block_rows, key_width), jnp.bfloat16),
            jax.ShapeDtypeStruct((block_rows, key_width), jnp.bfloat16),
            jax.ShapeDtypeStruct((seq_count, HEADS * VD), jnp.float32),
        ],
        in_specs=[vmem, vmem, any_space, any_space],
        out_specs=[any_space] * 3,
        scratch_shapes=[
            pltpu.VMEM((seq_count, HEADS * VD), jnp.float32),
            pltpu.VMEM((1, HEADS), jnp.float32),
            pltpu.VMEM((1, VD), jnp.float32),
            dma((5,)),
        ],
        compiler_params=pltpu.CompilerParams(vmem_limit_bytes=1024 * 1024),
    )(kv, states, map_balance[None, :], head_gain[None, :])
    shape = (1, 1, block_rows, key_width)
    return keys.reshape(shape), values.reshape(shape), read


def fits(mesh, key_weight, value_weight, prompt):
    tp_count, sp_count = mesh.shape["tp"], mesh.shape["sp"]
    seq_count, _, span_count = prompt.shape[:3]
    cols = key_weight.shape[1] // tp_count
    return (
        sp_count == 4
        and seq_count * span_count == sp_count
        and tp_count % CORES == 0
        and tp_count == 4 * CORES
        and cols == VD
        and 3 * seq_count <= 8
        and key_weight.shape == value_weight.shape
    )


def solution(mesh):
    in_specs = (
        P(None, "tp", None, "sp", None, None),
        P(),
        P(None, "tp"),
        P(None, "tp"),
        P(None, "tp"),
        P(),
        P(),
    )
    out_specs = (P("sp", "tp", None, None), P("sp", "tp", None, None), P())

    def step(prompt, new_token, query_proj_matrix, key_weight, value_weight, map_balance, head_gain):
        body = fused if fits(mesh, key_weight, value_weight, prompt) else shards
        mapped = jax.shard_map(
            body, mesh=mesh, in_specs=in_specs, out_specs=out_specs, check_vma=False
        )
        return mapped(
            prompt, new_token, query_proj_matrix, key_weight, value_weight, map_balance, head_gain
        )

    return step
```

```python
import functools

import jax
import jax.numpy as jnp
from jax import lax
from jax.experimental import pallas as pl
from jax.experimental.pallas import tpu as pltpu
from jax.sharding import PartitionSpec as P

HEADS = 8
MAP_HEAD_SIZE = 64
VD = 128


norm_eps = 1e-06
far_below = -1e30


def joined(part, axis, combine):
    gathered = jax.tree.map(lambda a: lax.all_gather(a, axis), part)

    def take(source):
        return jax.tree.map(lambda a: lax.dynamic_index_in_dim(a, source, 0, False), gathered)

    return lax.fori_loop(
        1, lax.axis_size(axis), lambda source, state: combine(state, take(source)), take(0)
    )


def fill_cols(source, w_piece):
    product = jnp.dot(source, w_piece, preferred_element_type=jnp.float32).astype(jnp.bfloat16)
    return product


def local_new(new_token, query_proj_matrix, key_weight, value_weight):
    return (
        jnp.dot(new_token, query_proj_matrix, preferred_element_type=jnp.float32).astype(
            jnp.bfloat16
        ),
        jnp.dot(new_token, key_weight, preferred_element_type=jnp.float32).astype(jnp.bfloat16),
        jnp.dot(new_token, value_weight, preferred_element_type=jnp.float32).astype(jnp.bfloat16),
    )


def partial_read(query_matrix_rows, key_rows, value_rows):
    logit_scores = jnp.einsum(
        "bhmd,bjhmd->bhmj", query_matrix_rows, key_rows, preferred_element_type=jnp.float32
    ) * MAP_HEAD_SIZE ** (-0.5)
    peak = jnp.max(logit_scores, axis=-1)
    weights_exp = jnp.exp(logit_scores - peak[..., None])
    totals = jnp.sum(weights_exp, axis=-1)
    weighted = jnp.einsum("bhmj,bjhe->bhme", weights_exp, value_rows.astype(jnp.float32))
    return (peak, totals, weighted)


def combine(first, second):
    peak_a, totals_a, weighted_a = first
    peak_b, totals_b, weighted_b = second
    peak = jnp.maximum(peak_a, peak_b)
    factor_a = jnp.exp(peak_a - peak)
    factor_b = jnp.exp(peak_b - peak)
    return (
        peak,
        totals_a * factor_a + totals_b * factor_b,
        weighted_a * factor_a[..., None] + weighted_b * factor_b[..., None],
    )


def shards(prompt, new_token, query_proj_matrix, key_weight, value_weight, map_balance, head_gain):
    seq_count, _, span_count, _, piece_rows, model_width = prompt.shape
    token_rows = prompt.reshape(seq_count * span_count * piece_rows, model_width)
    tp_count = lax.axis_size("tp")
    key_width = key_weight.shape[1] * tp_count
    value_width = value_weight.shape[1] * tp_count
    key_piece = lax.all_gather(key_weight, "tp", axis=1, tiled=True)
    value_piece = lax.all_gather(value_weight, "tp", axis=1, tiled=True)
    key_rows = fill_cols(token_rows, key_piece)
    value_rows = fill_cols(token_rows, value_piece)
    own_columns = local_new(new_token, query_proj_matrix, key_weight, value_weight)
    queries, new_keys, new_values = (
        lax.all_gather(own_columns[0], "tp", axis=1, tiled=True),
        lax.all_gather(own_columns[1], "tp", axis=1, tiled=True),
        lax.all_gather(own_columns[2], "tp", axis=1, tiled=True),
    )
    slot_count = seq_count * span_count
    cached_keys, cached_values = (
        lax.all_to_all(
            key_rows.reshape(slot_count, piece_rows, key_width),
            "sp",
            split_axis=0,
            concat_axis=1,
            tiled=True,
        ),
        lax.all_to_all(
            value_rows.reshape(slot_count, piece_rows, value_width),
            "sp",
            split_axis=0,
            concat_axis=1,
            tiled=True,
        ),
    )
    block_rows = cached_keys.shape[1]
    key_cache = cached_keys.reshape(1, 1, block_rows, key_width)
    value_cache = cached_values.reshape(1, 1, block_rows, value_width)
    all_queries = queries.reshape(seq_count, HEADS, 2, MAP_HEAD_SIZE)
    own_seq = lax.axis_index("sp") // span_count
    own_query = lax.dynamic_slice_in_dim(all_queries, own_seq, 1, 0)
    peak, totals, weighted = partial_read(
        own_query,
        cached_keys.reshape(1, block_rows, HEADS, 2, MAP_HEAD_SIZE),
        cached_values.reshape(1, block_rows, HEADS, VD),
    )
    chosen = jnp.arange(seq_count) == own_seq
    chosen_rows = chosen[:, None, None]
    spread = (
        jnp.where(chosen_rows, peak, far_below),
        jnp.where(chosen_rows, totals, 0.0),
        jnp.where(chosen_rows[..., None], weighted, 0.0),
    )
    merged = joined(spread, ("sp", "tp"), combine)
    own_keys = new_keys.reshape(seq_count, HEADS, 2, MAP_HEAD_SIZE)
    own_score = jnp.einsum(
        "bhmd,bhmd->bhm", all_queries, own_keys, preferred_element_type=jnp.float32
    ) * MAP_HEAD_SIZE ** (-0.5)
    own_values = new_values.astype(jnp.float32).reshape(seq_count, HEADS, VD)
    own_weighted = jnp.broadcast_to(own_values[:, :, None, :], (seq_count, HEADS, 2, VD))
    own_state = (own_score, jnp.ones_like(own_score), own_weighted)
    _, totals, weighted = combine(merged, own_state)
    heads_out = weighted / totals[..., None]
    blended = heads_out[:, :, 0] - map_balance[None, :, None] * heads_out[:, :, 1]
    normed = (
        blended
        * lax.rsqrt(jnp.mean(blended * blended, axis=-1, keepdims=True) + norm_eps)
        * head_gain
    )
    return (key_cache, value_cache, normed.reshape(seq_count, HEADS * VD))


MESH = pl.DeviceIdType.MESH
CORES = 2
PIECES = 2


def merged(states):
    peak = functools.reduce(jnp.maximum, [a[1] for a in states])
    factors = [jnp.exp(a[1] - peak) for a in states]
    weighted = functools.reduce(jnp.add, [a[0] * f for a, f in zip(states, factors)])
    total = functools.reduce(jnp.add, [a[2] * f for a, f in zip(states, factors)])
    return weighted, peak, total


def pack(ref, at, stat_at, state):
    weighted, peak, total = state
    rows = weighted.shape[0]
    lane = lax.broadcasted_iota(jnp.int32, weighted.shape, 1)
    row = lax.broadcasted_iota(jnp.int32, weighted.shape, 0)
    stats = jnp.where(lane == row, peak, jnp.where(lane == row + rows, total, 0.0))
    ref[at : at + rows] = weighted
    ref[stat_at : stat_at + 1] = jnp.sum(stats, axis=0, keepdims=True)


def unpack(ref, at, stat_at, rows):
    weighted = ref[at : at + rows]
    lane = lax.broadcasted_iota(jnp.int32, weighted.shape, 1)
    row = lax.broadcasted_iota(jnp.int32, weighted.shape, 0)
    stats = ref[stat_at : stat_at + 1]
    peak = jnp.sum(jnp.where(lane == row, stats, 0.0), axis=1, keepdims=True)
    total = jnp.sum(jnp.where(lane == row + rows, stats, 0.0), axis=1, keepdims=True)
    return weighted, peak, total


def step_kernel(
    dims,
    prompt, token_hbm, wq_hbm, wk_hbm, wv_hbm,
    kv, finbuf,
    xbuf, wbuf, kvbuf, upbuf, partial, wq, token, qbuf, pbuf, pstat, stbuf,
    loc, far_send, far_recv, line_send, prim_recv, xy_send, sec_recv, relay_recv, sib_send, sib_recv,
    out_send, out_recv, up_recv, pk_send, pk_recv, st_send, st_recv, fin_send, fin_recv,
):
    sp_count, tp_count, seq_count = dims
    _, _, depth, wide = wbuf.shape
    cols = wide // CORES
    chips = tp_count // CORES
    rows = xbuf.shape[1]
    state_rows = CORES * 2 * seq_count
    s = lax.axis_index("sp")
    t = lax.axis_index("tp")
    z = t // CORES
    c = t % CORES
    sib = z * CORES + (1 - c)
    xs = s + 1 - 2 * (s % 2)
    ys = (s + 2) % 4
    diag = 3 - s
    prim = (s + s // 2) % 2
    sec = 1 - prim
    turn = s // 2
    near = jnp.minimum(z, chips - 1 - z)
    inside = near > 0
    outside = jnp.logical_not(inside)
    half = depth // 2
    step = half // PIECES
    part_rows = step // 2

    def lanes_of(core):
        return pl.ds(pl.multiple_of(core * cols, cols), cols)

    lanes, sib_lanes = lanes_of(c), lanes_of(1 - c)

    loads = [
        pltpu.make_async_copy(wk_hbm, wbuf.at[0, z, :, lanes], loc.at[0]),
        pltpu.make_async_copy(wv_hbm, wbuf.at[1, z, :, lanes], loc.at[1]),
        pltpu.make_async_copy(prompt.at[xs], xbuf.at[0], loc.at[2]),
        pltpu.make_async_copy(prompt.at[ys], xbuf.at[1], loc.at[3]),
        pltpu.make_async_copy(token_hbm, token, loc.at[4]),
        pltpu.make_async_copy(wq_hbm, wq, loc.at[5]),
        pltpu.make_async_copy(prompt.at[s], xbuf.at[2], loc.at[6]),
    ]
    for a in loads:
        a.start()

    z_peers = [(s, (t + d * CORES) % tp_count) for d in range(1, chips)]
    plane_peers = [((s + d) % sp_count, t) for d in range(1, sp_count)]
    cross_peers = [((s + d) % sp_count, sib) for d in range(1, sp_count)]
    barrier = pltpu.get_barrier_semaphore()
    greeted = plane_peers + [(s, sib)]

    def greet(p):
        pl.semaphore_signal(barrier, inc=1, device_id=p, device_id_type=MESH)

    pl.when(z > 0)(lambda: greet((s, t - CORES)))
    pl.when(z < chips - 1)(lambda: greet((s, t + CORES)))
    for p in greeted:
        greet(p)
    pl.semaphore_wait(barrier, len(greeted) + jnp.where(inside, 2, 1))

    def remote(src, dst, send, recv, dev):
        return pltpu.make_async_remote_copy(
            src_ref=src, dst_ref=dst, send_sem=send, recv_sem=recv, device_id=dev, device_id_type=MESH
        )

    def push(view, send, recv, dev):
        remote(view, view, send, recv, dev).start()

    def got(view, recv):
        remote(view, view, xy_send, recv, (s, sib)).wait_recv()

    def gone(view, send):
        remote(view, view, send, loc.at[0], (s, sib)).wait_send()

    def span(start, size):
        return pl.ds(pl.multiple_of(start, size), size)

    def slot(zz, holder):
        return jnp.where(zz > holder, zz - 1, zz)

    def piece_of(m, zz, p):
        return wbuf.at[m, zz, span(prim * half + p * step, step), lanes]

    def line(direction, m, zz, p):
        view = piece_of(m, zz, p)
        push(view, line_send.at[(direction + 1) // 2], prim_recv.at[m, slot(zz, z + direction), p], (s, t + direction * CORES))

    def has_next(direction):
        return (z > 0) if direction < 0 else (z < chips - 1)

    def to_end(direction):
        return (z == 1) if direction < 0 else (z == chips - 2)

    far_prompt = remote(prompt.at[diag], xbuf.at[3], far_send, far_recv, (diag, t))
    far_prompt.start()
    for m in range(2):
        loads[m].wait()
        for direction in (-1, 1):
            @pl.when(jnp.logical_and(has_next(direction), to_end(direction)))
            def _(direction=direction, m=m):
                line(direction, m, z, turn)

            @pl.when(jnp.logical_and(has_next(direction), jnp.logical_not(to_end(direction))))
            def _(direction=direction, m=m):
                for p in range(PIECES):
                    line(direction, m, z, p)
        push(wbuf.at[m, z, :, lanes], sib_send, sib_recv.at[m * chips + z], (s, sib))
    inner = jnp.where(z == 0, t + CORES, t - CORES)
    outer = jnp.where(z == 1, z - 1, z + 1)

    def source(j):
        j = j + 1
        paired = j <= 2 * near
        dist = jnp.where(paired, (j + 1) // 2, j - near)
        from_left = jnp.where(paired, j % 2 == 1, z > near)
        return jnp.where(from_left, z - dist, z + dist), from_left

    def event(e):
        both = jnp.logical_and(inside, e < 8)
        j = jnp.where(both, e % 2, e // 4)
        m = jnp.where(both, e // 4, (e // 2) % 2)
        p = jnp.where(both, (e // 2) % 2, e % 2)
        single = jnp.logical_and(outside, e < 4)
        return j, jnp.where(single, e % 2, m), jnp.where(single, turn, p)

    def group(g):
        both = jnp.logical_and(inside, g < 4)
        return jnp.where(both, g % 2, g // 2), jnp.where(both, g // 2, g % 2)

    def arrive(e):
        j, m, p = event(e)
        zz, from_left = source(j)
        view = piece_of(m, zz, p)
        got(view, prim_recv.at[m, slot(zz, z), p])
        on_right = jnp.logical_and(from_left, z < chips - 1)
        on_left = jnp.logical_and(jnp.logical_not(from_left), z > 0)
        pl.when(on_right)(lambda: line(1, m, zz, p))
        pl.when(on_left)(lambda: line(-1, m, zz, p))
        single = jnp.logical_and(outside, e < 4)

        @pl.when(single)
        def _():
            for to in (xs, ys):
                push(view, xy_send, sec_recv.at[m, slot(zz, z)], (to, t))

        whole = jnp.logical_and(inside, zz == outer)

        @pl.when(jnp.logical_not(jnp.logical_or(single, whole)))
        def _():
            for h, to in enumerate((xs, ys)):
                part = part_of(prim, m, zz, p, h)
                push(part, xy_send, sec_recv.at[m, slot(zz, z)], (to, t))

        last = jnp.logical_and(j == chips - 2, m == 1)
        push(view, sib_send, sib_recv.at[jnp.where(last, 2 * chips, m * chips + zz)], (s, sib))

    def part_of(which, m, zz, p, h):
        return wbuf.at[m, zz, span(which * half + p * step + h * part_rows, part_rows), lanes]

    def arrive_secondary(g):
        j, m = group(g)
        zz, _ = source(j)
        view = wbuf.at[m, zz, span(sec * half, half), lanes]
        got(view, sec_recv.at[m, slot(zz, z)])

        @pl.when(jnp.logical_and(outside, g < 2))
        def _():
            push(part_of(sec, m, zz, 1 - turn, 0), xy_send, relay_recv.at[m], (xs, t))
            push(part_of(sec, m, zz, turn, 1), xy_send, relay_recv.at[m], (ys, t))

        push(view, sib_send, sib_recv.at[m * chips + zz], (s, sib))

    def arrive_relayed(m):
        zz, _ = source(0)
        view = piece_of(m, zz, 1 - turn)
        got(view, relay_recv.at[m])
        push(view, sib_send, sib_recv.at[m * chips + zz], (s, sib))

    def columns_of(zz):
        return pl.ds(pl.multiple_of(zz * wide, wide), wide)

    def product(pair, m, zz, first, width):
        at = pl.ds(2 * pair, 2)
        columns = span(zz * wide + first, width)
        out = jnp.dot(
            xbuf[at].reshape(-1, depth), wbuf[m, zz, :, span(first, width)],
            preferred_element_type=jnp.float32,
        ).astype(jnp.bfloat16)
        kvbuf[m, at, :, columns] = out.reshape(2, rows, width)
        return columns

    def whole_product(m, zz):
        out = jnp.dot(
            xbuf[...].reshape(-1, depth), wbuf[m, zz], preferred_element_type=jnp.float32
        ).astype(jnp.bfloat16)
        kvbuf[m, :, :, columns_of(zz)] = out.reshape(sp_count, rows, wide)

    def keep(m, columns):
        for i, slot in ((2, s), (3, diag)):
            kv[m, span(slot * rows, rows), columns] = kvbuf[m, i, :, columns]

    def multiply(m, zz):
        got(wbuf.at[m, zz, :, sib_lanes], sib_recv.at[m * chips + zz])

        whole_product(m, zz)
        keep(m, columns_of(zz))

    last_zz = source(chips - 2)[0]

    def halves(which):
        at = span(which * half, half)
        return jnp.dot(
            xbuf[:, :, at].reshape(-1, half), wbuf[1, last_zz, at, :], preferred_element_type=jnp.float32
        )

    def last_begin():
        got(wbuf.at[1, last_zz, span(prim * half, half), sib_lanes], sib_recv.at[2 * chips])
        partial[...] = halves(prim)

    def last_end():
        got(wbuf.at[1, last_zz, span(sec * half, half), sib_lanes], sib_recv.at[chips + last_zz])
        out = (partial[...] + halves(sec)).astype(jnp.bfloat16)
        kvbuf[1, :, :, columns_of(last_zz)] = out.reshape(sp_count, rows, wide)
        keep(1, columns_of(last_zz))

    def send_columns(m, columns):
        for i, p in enumerate((xs, ys)):
            remote(
                kvbuf.at[m, i, :, columns], kv.at[m, span(s * rows, rows), columns],
                out_send, out_recv, (p, t),
            ).start()

    scale = MAP_HEAD_SIZE ** (-0.5)
    row = lax.broadcasted_iota(jnp.int32, (state_rows, 1), 0)
    row_map = row // (CORES * seq_count)
    row_seq = (row // CORES) % seq_count
    row_head = row % CORES

    def by_seq(new, first):
        values = jnp.zeros((state_rows, new.shape[1]), jnp.float32)
        for b in range(seq_count):
            values = jnp.where(row_seq == b, new[first + b : first + b + 1], values)
        return values

    def by_head(values):
        return functools.reduce(
            jnp.add,
            [jnp.where(row_head == i, values[:, i * VD : (i + 1) * VD], 0.0) for i in range(CORES)],
        )

    def queries_of(zz):
        return qbuf.at[span(zz * CORES, CORES), pl.ds(0, seq_count)]

    def new_rows(zz):
        return jnp.concatenate([qbuf[zz * CORES + i] for i in range(CORES)], axis=1)

    def query_of(new):
        lane = lax.broadcasted_iota(jnp.int32, (state_rows, wide), 1)
        mine = lane // MAP_HEAD_SIZE == row_head * 2 + row_map
        return jnp.where(mine, by_seq(new, 0), 0.0)

    def score(j, zz):
        query = query_of(new_rows(zz)).astype(jnp.bfloat16)
        keys = kvbuf[0, :, :, columns_of(zz)].reshape(-1, wide)
        scores = lax.dot_general(
            query, keys, (((1,), (1,)), ((), ())), preferred_element_type=jnp.float32
        ) * scale
        at = lax.broadcasted_iota(jnp.int32, scores.shape, 1) // rows
        spans = sp_count // seq_count
        owner = jnp.where(at == 0, xs, jnp.where(at == 1, ys, s)) // spans
        mine = owner == row_seq
        peak = jnp.max(jnp.where(mine, scores, far_below), axis=1, keepdims=True)
        raised = jnp.where(mine, jnp.exp(scores - peak), 0.0)
        total = jnp.sum(raised, axis=1, keepdims=True)
        high = raised.astype(jnp.bfloat16)
        low = (raised - high.astype(jnp.float32)).astype(jnp.bfloat16)
        pbuf[j, :state_rows] = high
        pbuf[j, state_rows:] = low
        pstat[j, 0] = jnp.broadcast_to(peak, (state_rows, VD))
        pstat[j, 1] = jnp.broadcast_to(total, (state_rows, VD))

    def weigh(j, zz):
        values = kvbuf[1, :, :, columns_of(zz)].reshape(-1, wide)
        both = jnp.dot(pbuf[j], values, preferred_element_type=jnp.float32)
        return by_head(both[:state_rows] + both[state_rows:]), pstat[j, 0][:, :1], pstat[j, 1][:, :1]

    def send_state(zz):
        view = stbuf.at[z, zz, pl.ds(0, state_rows + 1)]
        for p in z_peers:
            push(view, st_send, st_recv.at[zz], p)

    def send_up(slot, m, zz, recv):
        for i, p in enumerate((xs, ys)):
            remote(kvbuf.at[m, i, :, columns_of(zz)], upbuf.at[slot, i], out_send, recv, (p, inner)).start()

    def pass_down(slot, m, zz):
        for i, p in enumerate((xs, ys)):
            remote(
                upbuf.at[slot, i], kv.at[m, span(p * rows, rows), columns_of(zz)],
                out_send, out_recv, (s, outer * CORES + c),
            ).start()

    mine_at = chips - 1
    loads[2].wait()
    loads[3].wait()
    before = None
    for core in (c, 1 - c):
        for m in range(2):
            if core is not c:
                got(wbuf.at[m, z, :, sib_lanes], sib_recv.at[m * chips + z])
            columns = product(0, m, z, core * cols, cols)
            if before is not None:
                pl.when(inside)(lambda before=before: send_columns(*before))
            before = (m, columns)

    def vectors():
        loads[4].wait()
        loads[5].wait()
        vector = token[...]
        me_q = jnp.dot(vector, wq[...], preferred_element_type=jnp.float32)
        me_k = jnp.dot(vector, wbuf[0, z, :, lanes], preferred_element_type=jnp.float32)
        me_v = jnp.dot(vector, wbuf[1, z, :, lanes], preferred_element_type=jnp.float32)
        for i, value in enumerate((me_q, me_k, me_v)):
            value = value.astype(jnp.bfloat16).astype(jnp.float32)
            qbuf[t, i * seq_count : (i + 1) * seq_count, :] = value[:seq_count]
    def own_block():
        loads[6].wait()
        far_prompt.wait_recv()

        def some(m, _):
            product(1, m, z, 0, wide)
            keep(m, columns_of(z))
            return 0

        lax.fori_loop(0, 2, some, 0)
        score(mine_at, z)
        new = new_rows(z)
        own_score = jnp.sum(query_of(new) * by_seq(new, seq_count), axis=1, keepdims=True) * scale
        holder = jnp.logical_and(s == 0, c == 0)
        own = (
            jnp.where(holder, by_head(by_seq(new, 2 * seq_count)), 0.0),
            jnp.where(holder, own_score, far_below),
            jnp.where(holder, jnp.ones_like(own_score), 0.0),
        )
        pack(stbuf.at[z, z], 0, state_rows, merged([weigh(mine_at, z), own]))

    def compute(g):
        j, m = group(g)
        zz, _ = source(j)
        multiply(m, zz)

        @pl.when(m == 0)
        def _():
            got(queries_of(zz), pk_recv.at[zz])
            score(j, zz)

        @pl.when(m == 1)
        def _():
            pack(stbuf.at[z, zz], 0, state_rows, weigh(j, zz))

    def results(g):
        j, m = group(g)
        zz, _ = source(j)
        send_columns(m, columns_of(zz))

    def state(g):
        j, m = group(g)
        zz, _ = source(j)
        pl.when(m == 1)(lambda: send_state(zz))

    groups = 2 * (chips - 1)
    own_at = jnp.where(inside, 7, 5)

    def work(e, _):
        arrive(e)

        @pl.when(e == 2)
        def _():
            pl.when(inside)(lambda: send_columns(*before))
            vectors()

        @pl.when(e == 3)
        def _():
            push(qbuf.at[t], pk_send, pk_recv.at[z], (s, sib))

        @pl.when(e == 4)
        def _():
            got(qbuf.at[sib], pk_recv.at[z])
            for p in z_peers:
                push(queries_of(z), pk_send, pk_recv.at[z], p)

            @pl.when(outside)
            def _():
                for m in range(2):
                    view = wbuf.at[m, z, span(sec * half, half), lanes]
                    push(view, line_send.at[jnp.where(z == 0, 1, 0)], sec_recv.at[m, jnp.where(z == 0, 0, chips - 2)], (s, inner))
                for m in range(2):
                    send_up(m, m, z, up_recv.at[0])

        pl.when(e == own_at)(own_block)
        pl.when(outside & (e >= 9) & (e < 11))(lambda: arrive_relayed(e - 9))
        pl.when(outside & (e == 9))(lambda: send_up(2, 0, source(1)[0], up_recv.at[1]))
        ready = jnp.where(inside, e - 9, jnp.where(e < 9, e - 6, e - 7))
        pl.when((ready >= 0) & (inside | ((e != 9) & (e < 11))))(lambda: arrive_secondary(ready))
        now = jnp.where(inside, e - 10, jnp.where(e == 8, 2, e - 9))
        pl.when(jnp.where(inside, e >= 10, (e == 8) | (e == 9)))(lambda: compute(now))
        return 0

    events = 2 * groups
    lax.fori_loop(jnp.where(inside, 0, 2), events, work, 0)

    @pl.when(inside)
    def _():
        results(0)
        results(1)

    pl.when(outside)(lambda: send_state(z))

    def rest(i, _):
        @pl.when(inside & (i == 2))
        def _():
            send_state(z)
            state(2)
            state(3)
            got(upbuf.at[pl.ds(0, 2)], up_recv.at[0])
            pass_down(0, 0, outer)

        behind = jnp.where(inside, i + 3, groups - 2)
        pl.when(jnp.where(inside, i < 2, i == 1))(lambda: arrive_secondary(behind))

        @pl.when(i == 2)
        def _():
            last_begin()
            arrive_secondary(groups - 1)

        g = jnp.where(outside & (i == 0), 1, i + 2)
        compute(g)
        pl.when(outside & (i == 0))(lambda: results(0))
        results(g)
        pl.when(outside)(lambda: state(g))
        return 0

    lax.fori_loop(0, 3, rest, 0)

    me = s * CORES + c
    ends = (0, chips - 1)
    middle = tuple(range(1, chips - 1))

    def join_z(k, blocks):
        for i, zz in enumerate(blocks):
            got(stbuf.at[pl.ds(0, chips - 1), zz, pl.ds(0, state_rows + 1)], st_recv.at[zz])
            whole = merged([unpack(stbuf.at[a, zz], 0, state_rows, state_rows) for a in range(chips)])
            pack(finbuf.at[k, me], i * state_rows, len(blocks) * state_rows + i, whole)

    def send_joined(k, blocks):
        view = finbuf.at[k, me, pl.ds(0, len(blocks) * (state_rows + 1))]
        for p in plane_peers + cross_peers + [(s, sib)]:
            push(view, fin_send, fin_recv.at[k], p)

    last_end()
    pack(stbuf.at[z, last_zz], 0, state_rows, weigh(chips - 2, last_zz))
    results(groups - 1)
    state(groups - 1)

    @pl.when(inside)
    def _():
        pass_down(1, 1, outer)
        got(upbuf.at[2], up_recv.at[1])
        pass_down(2, 0, 2 * z - outer)

    join_z(0, middle)
    send_joined(0, middle)
    join_z(1, ends)
    send_joined(1, ends)
    others = sp_count * CORES - 1
    fin_rows = pl.ds(0, 2 * (state_rows + 1))
    for k in range(2):
        got(finbuf.at[k, pl.ds(0, others), fin_rows], fin_recv.at[k])

    def pieces_view(count):
        return wbuf.at[:, 0, pl.ds(0, count * step * cols // (2 * wide)), :]

    others_rows = pl.ds(0, 2)
    far_prompt.wait_send()
    got(kvbuf.at[:, others_rows], out_recv)
    for pieces, on in ((11, inside), (8, outside)):
        pl.when(on)(lambda pieces=pieces: gone(pieces_view(pieces), out_send))
    for pieces, on in ((8, inside), (14, outside)):
        pl.when(on)(lambda pieces=pieces: gone(pieces_view(pieces), xy_send))
    gone(wbuf.at[:, :, :, lanes], sib_send)
    query_rows = qbuf.shape[1] + len(z_peers) * CORES * seq_count
    gone(qbuf.at[pl.ds(0, query_rows // 4), pl.ds(0, 4)], pk_send)
    gone(stbuf.at[pl.ds(0, chips - 1), :, pl.ds(0, state_rows + 1)], st_send)
    gone(finbuf.at[:, pl.ds(0, others), fin_rows], fin_send)
    for direction in (-1, 1):
        for pieces, last in ((10, True), (8, False)):
            @pl.when(jnp.logical_and(has_next(direction), to_end(direction) == last))
            def _(direction=direction, pieces=pieces):
                gone(pieces_view(pieces), line_send.at[(direction + 1) // 2])


def store_kernel(
    blocks, kv, finbuf, balance_hbm, gain_hbm, keys_out, values_out, read_out, read, balance, gain, sem
):
    copies = [
        pltpu.make_async_copy(balance_hbm, balance, sem.at[0]),
        pltpu.make_async_copy(gain_hbm, gain, sem.at[1]),
        pltpu.make_async_copy(kv.at[0], keys_out, sem.at[2]),
        pltpu.make_async_copy(kv.at[1], values_out, sem.at[3]),
        pltpu.make_async_copy(read, read_out, sem.at[4]),
    ]
    for a in copies[:4]:
        a.start()
    devices, state_rows = finbuf.shape[1], CORES * 2 * read.shape[0]
    fold = state_rows // 2
    seq_count = read.shape[0]
    heads = {}
    for k, zz_list in enumerate(blocks):
        for i, zz in enumerate(zz_list):
            at, stat_at = i * state_rows, len(zz_list) * state_rows + i
            weighted, _, total = merged(
                [unpack(finbuf.at[k, a], at, stat_at, state_rows) for a in range(devices)]
            )
            heads[zz] = weighted / total
    copies[0].wait()
    copies[1].wait()
    for zz, heads_out in heads.items():
        lane = lax.broadcasted_iota(jnp.int32, (fold, HEADS), 1)
        chosen = lane == zz * CORES + lax.broadcasted_iota(jnp.int32, (fold, HEADS), 0) % CORES
        second = jnp.sum(jnp.where(chosen, balance[...], 0.0), axis=1, keepdims=True)
        blended = heads_out[:fold] - second * heads_out[fold:]
        normed = (
            blended
            * lax.rsqrt(jnp.mean(blended * blended, axis=1, keepdims=True) + norm_eps)
            * gain[...]
        )
        for b in range(seq_count):
            for h in range(CORES):
                r = b * CORES + h
                read[b : b + 1, (zz * CORES + h) * VD : (zz * CORES + h + 1) * VD] = normed[r : r + 1]
    copies[4].start()
    for a in copies[2:]:
        a.wait()


def fused(prompt, new_token, query_proj_matrix, key_weight, value_weight, map_balance, head_gain):
    seq_count, _, span_count, _, piece_rows, width = prompt.shape
    sp_count, tp_count = lax.axis_size("sp"), lax.axis_size("tp")
    cols = key_weight.shape[1]
    slots = seq_count * span_count
    chips = tp_count // CORES
    key_width = cols * tp_count
    block_rows = sp_count * piece_rows
    state_rows = CORES * 2 * seq_count
    any_space = pl.BlockSpec(memory_space=pltpu.HBM)
    vmem = pl.BlockSpec(memory_space=pltpu.VMEM)
    dma = pltpu.SemaphoreType.DMA
    kv, states = pl.pallas_call(
        functools.partial(step_kernel, (sp_count, tp_count, seq_count)),
        out_shape=[
            pltpu.VMEM((2, block_rows, key_width), jnp.bfloat16),
            pltpu.VMEM((2, sp_count * CORES, 2 * state_rows + 8, VD), jnp.float32),
        ],
        in_specs=[any_space] * 5,
        out_specs=[vmem, vmem],
        scratch_shapes=[
            pltpu.VMEM((slots, piece_rows, width), jnp.bfloat16),
            pltpu.VMEM((2, chips, width, CORES * cols), jnp.bfloat16),
            pltpu.VMEM((2, slots, piece_rows, key_width), jnp.bfloat16),
            pltpu.VMEM((3, 2, piece_rows, CORES * cols), jnp.bfloat16),
            pltpu.VMEM((slots * piece_rows, CORES * cols), jnp.float32),
            pltpu.VMEM((width, cols), jnp.bfloat16),
            pltpu.VMEM((seq_count, width), jnp.bfloat16),
            pltpu.VMEM((tp_count, 8, cols), jnp.float32),
            pltpu.VMEM((chips, 2 * state_rows, slots * piece_rows), jnp.bfloat16),
            pltpu.VMEM((chips, 2, state_rows, VD), jnp.float32),
            pltpu.VMEM((chips, chips, 2 * state_rows, VD), jnp.float32),
            dma((7,)), dma(()), dma(()), dma((2,)), dma((2, chips - 1, PIECES)), dma(()), dma((2, chips - 1)), dma((2,)),
            dma(()), dma((2 * chips + 1,)),
            dma(()), dma(()), dma((2,)), dma(()), dma((chips,)), dma(()), dma((chips,)), dma(()), dma((2,)),
        ],
        compiler_params=pltpu.CompilerParams(
            collective_id=0, has_side_effects=True, vmem_limit_bytes=61 * 1024 * 1024 + 512 * 1024
        ),
    )(
        prompt.reshape(slots, piece_rows, width),
        new_token, query_proj_matrix, key_weight, value_weight,
    )
    blocks = (tuple(range(1, chips - 1)), (0, chips - 1))
    keys, values, read = pl.pallas_call(
        functools.partial(store_kernel, blocks),
        out_shape=[
            jax.ShapeDtypeStruct((block_rows, key_width), jnp.bfloat16),
            jax.ShapeDtypeStruct((block_rows, key_width), jnp.bfloat16),
            jax.ShapeDtypeStruct((seq_count, HEADS * VD), jnp.float32),
        ],
        in_specs=[vmem, vmem, any_space, any_space],
        out_specs=[any_space] * 3,
        scratch_shapes=[
            pltpu.VMEM((seq_count, HEADS * VD), jnp.float32),
            pltpu.VMEM((1, HEADS), jnp.float32),
            pltpu.VMEM((1, VD), jnp.float32),
            dma((5,)),
        ],
        compiler_params=pltpu.CompilerParams(vmem_limit_bytes=1024 * 1024),
    )(kv, states, map_balance[None, :], head_gain[None, :])
    shape = (1, 1, block_rows, key_width)
    return keys.reshape(shape), values.reshape(shape), read


def fits(mesh, key_weight, value_weight, prompt):
    tp_count, sp_count = mesh.shape["tp"], mesh.shape["sp"]
    seq_count, _, span_count = prompt.shape[:3]
    cols = key_weight.shape[1] // tp_count
    return (
        sp_count == 4
        and seq_count * span_count == sp_count
        and tp_count % CORES == 0
        and tp_count == 4 * CORES
        and cols == VD
        and 3 * seq_count <= 8
        and key_weight.shape == value_weight.shape
    )


def solution(mesh):
    in_specs = (
        P(None, "tp", None, "sp", None, None),
        P(),
        P(None, "tp"),
        P(None, "tp"),
        P(None, "tp"),
        P(),
        P(),
    )
    out_specs = (P("sp", "tp", None, None), P("sp", "tp", None, None), P())

    def step(prompt, new_token, query_proj_matrix, key_weight, value_weight, map_balance, head_gain):
        body = fused if fits(mesh, key_weight, value_weight, prompt) else shards
        mapped = jax.shard_map(
            body, mesh=mesh, in_specs=in_specs, out_specs=out_specs, check_vma=False
        )
        return mapped(
            prompt, new_token, query_proj_matrix, key_weight, value_weight, map_balance, head_gain
        )

    return step
```
